32 devices in a mesh: ep: 8 (over z, y), tp: 4 (over x, core).
Axes of the slice: x: 2, y: 2, z: 4, core: 2. Of those that a mesh axis runs over, the one named last changes fastest.
Arguments:
- query: bfloat16 [1024, 1536], P('ep', 'tp'), may hold values from -136 to 136
- latent: bfloat16 [1024, 512], P(('ep', 'tp')), may hold values from -6 to 6
- rope_key: bfloat16 [1024, 32], P(('ep', 'tp')), may hold values from -6 to 6
- latent_gain: float32 [512], replicated, may hold values from 0.1 to 1.9
- key_up: bfloat16 [512, 1024], P(None, 'tp'), may hold values from -0.25 to 0.25
- value_up: bfloat16 [512, 1024], P(None, 'tp'), may hold values from -2 to 2
- out_proj: bfloat16 [1024, 2048], replicated, may hold values from -0.1875 to 0.1875
- tokens: bfloat16 [2048, 2048], P(('ep', 'tp')), may hold values from -6 to 6
- moe_gain: float32 [2048], replicated, may hold values from 0.1 to 1.9
- routes: int32 [2048, 2], P(('ep', 'tp')), may hold values from 0 to 7, all different within a row; in each aligned block of 64 rows (0 to 63, 64 to 127, ...) at most 32 rows name the same one
- group_prob: float32 [2048], P(('ep', 'tp')), may hold values from 0.25 to 1
- expert_prob: float32 [2048, 2], P(('ep', 'tp')), may hold values from 0.02 to 1
- w_gate: bfloat16 [8, 2048, 1024], P('ep', None, 'tp'), may hold values from -0.125 to 0.125
- w_up: bfloat16 [8, 2048, 1024], P('ep', None, 'tp'), may hold values from -0.125 to 0.125
- w_down: bfloat16 [8, 1024, 2048], P('ep', 'tp'), may hold values from -0.1875 to 0.1875
Outputs:
- mixed: bfloat16 [1024, 2048], P(('ep', 'tp'))
- moe_out: bfloat16 [2048, 2048], P(('ep', 'tp'))
The draws below stay inside these ranges and needn't reach their ends.
Inputs may be any that keep to these rules, and one draw needn't show every extreme that they name: `routes`: each row names 2 different experts; within the rows of one device no expert is named more than 32 times.
All inputs are finite; a program needn't handle non-finite values.
Results may differ from the reference program's by a relative error of at most 0.025.
Values may be sent and summed in bfloat16 or wider, within the bound.
A program may use at most 128 MiB of HBM per device.

```python
import functools
import math
import jax
import jax.numpy as jnp
import numpy as np
from jax import lax

D = 2048
HEADS = 16
NOPE = 64
ROPE_DIM = 32
V_DIM = 64
LATENT = 512
EXPERT_WIDTH = 1024
TOP = 2
M_ROWS = 64
SEQ = 1024
MOE_TOKENS = 2048
EXPERTS = 8
CAP = 32
N_TP = 4


def draw_query(key, part):
    first_key = jax.random.fold_in(jax.random.fold_in(key, 11), 0)
    full_shape = (SEQ, HEADS * (NOPE + ROPE_DIM))
    values = jnp.clip(2.0 * jax.random.normal(first_key, full_shape, jnp.float32), -8.0, 8.0)
    return values.astype(jnp.bfloat16)


def block_scale(own_key, dims, cuts, smallest, top_value):
    def one(position, blocks):
        draws = jax.random.uniform(jax.random.fold_in(jax.random.fold_in(own_key, 6), position), (blocks,), jnp.float32, smallest / len(cuts), top_value / len(cuts))
        return jnp.repeat(jnp.exp(draws), dims[position] // blocks).reshape((-1,) + (1,) * (len(dims) - position - 1))

    factor_of = one(*cuts[0])
    for cut in cuts[1:]:
        factor_of = factor_of * one(*cut)
    return factor_of


def assign_block(stream_key, own, number, rows, count, top, most, slope):
    order = jax.random.permutation(stream_key, count)
    crowded, usual = portions_of(count, rows * top, most, slope, True), portions_of(count, rows * top, most, slope, False)
    places = jnp.arange(count)

    def named(lengths, turn):
        used = int((lengths > 0).sum())
        fixed = max(1, used // 4)
        shifted = fixed + (places - fixed + turn * (used - fixed)) % max(1, count - fixed)
        return jnp.zeros((count,), jnp.int32).at[order[jnp.where(places < fixed, places, shifted)]].set(jnp.asarray(lengths, jnp.int32))

    lengths = jnp.where(number % 4 == 0, named(crowded, number // 4), named(usual, number - number // 4 - 1))
    mixed = jax.random.permutation(jax.random.fold_in(own, 3), count)
    source_of, taker = mixed[0:count // 2 * 2:2], mixed[1:count // 2 * 2:2]
    room = jnp.minimum(lengths[source_of] - 1, most - lengths[taker]) // 2
    room = jnp.where((source_of == order[0]) | (taker == order[0]) | (lengths[taker] == 0), 0, jnp.maximum(room, 0))
    shifted = jax.random.randint(jax.random.fold_in(own, 4), (count // 2,), 0, 1 << 20) % (room + 1)
    lengths = lengths.at[source_of].add(-shifted).at[taker].add(shifted)
    items = jnp.searchsorted(jnp.cumsum(lengths), jnp.arange(rows * top), side="right").astype(jnp.int32)
    grid = items.reshape(top, rows).T
    grid = grid[jax.random.permutation(jax.random.fold_in(own, 1), rows)]
    turn = jax.random.randint(jax.random.fold_in(own, 2), (rows, 1), 0, top)
    return jnp.take_along_axis(grid, (jnp.arange(top)[None, :] + turn) % top, axis=1)


def portions_of(number_of, total, reach, slope, full):
    portions = [(1 << 20) // math.isqrt(standing ** slope) + 1 for standing in range(1, number_of + 1)]
    largest = reach if full else min(reach, max(-(-total // number_of), total * portions[0] // sum(portions)))
    least = 1 if total - largest >= number_of - 1 else 0
    given, rest = [largest] + [least] * (number_of - 1), total - largest - least * (number_of - 1)
    while rest > 0:
        movable = [i for i in range(1, number_of) if given[i] < largest] or [i for i in range(1, number_of) if given[i] < reach]
        pool, budget = sum([portions[i] for i in movable]), rest
        for i in movable:
            more = min(reach - given[i], max(1, budget * portions[i] // pool), rest)
            given[i] = given[i] + more
            rest = rest - more
    return np.array(given)


def centred(key, shape, spread, bound, cuts=(), kind=jnp.bfloat16):
    array = jax.random.normal(key, shape, jnp.float32) * spread
    if len(cuts) > 0:
        array = block_scale(key, shape, cuts, -0.22, 0.18) * array
    return jnp.clip(array, min=-bound, max=bound).astype(kind)


def setup_inputs(seed: int = 0) -> dict:
    key_list = jax.random.split(jax.random.key(seed), 16)
    query = draw_query(jax.random.fold_in(key_list[15], 71), 0)
    latent = centred(key_list[1], (SEQ, LATENT), 1.0, 6.0, ((0, 32),))
    rope_key = centred(key_list[2], (SEQ, ROPE_DIM), 1.0, 6.0, ((0, 32),))
    latent_gain = jnp.clip(1.0 + 0.18 * jax.random.normal(key_list[3], (LATENT,), jnp.float32), 0.1, 1.9)
    key_up = centred(key_list[4], (LATENT, HEADS * NOPE), LATENT ** -0.5, 0.25, ((1, 4),))
    value_up = centred(key_list[5], (LATENT, HEADS * V_DIM), (LATENT // 64) ** -0.5, 2.0, ((1, 4),))
    out_proj = centred(key_list[6], (HEADS * V_DIM, D), (HEADS * V_DIM) ** -0.5, 0.1875)
    tokens = centred(key_list[7], (MOE_TOKENS, D), 1.0, 6.0, ((0, 32),))
    moe_gain = jnp.clip(1.0 + 0.18 * jax.random.normal(key_list[8], (D,), jnp.float32), 0.1, 1.9)
    routes_keys = jax.random.split(jax.random.fold_in(key_list[9], 1), MOE_TOKENS // M_ROWS)
    routes_turns = jax.random.permutation(jax.random.fold_in(key_list[9], 3), MOE_TOKENS // M_ROWS)
    routes = jax.vmap(lambda own, number: assign_block(jax.random.fold_in(key_list[9], 2), own, number, M_ROWS, EXPERTS, TOP, CAP, 2))(routes_keys, routes_turns).reshape((MOE_TOKENS, TOP))
    group_prob = jnp.clip(jnp.exp(math.log(1.0) - 1.3862944 * jax.random.uniform(key_list[10], (MOE_TOKENS,), jnp.float32) ** block_scale(key_list[10], (MOE_TOKENS,), ((0, 32),), -0.2, 0.2)), 0.25, 1.0)
    expert_prob = jnp.clip(jnp.exp(math.log(1.0) - 3.912023 * jax.random.uniform(key_list[11], (MOE_TOKENS, TOP), jnp.float32) ** block_scale(key_list[11], (MOE_TOKENS, TOP), ((0, 32),), -0.2, 0.2)), 0.02, 1.0)
    w_gate = centred(key_list[12], (EXPERTS, D, EXPERT_WIDTH), D ** -0.5, 0.125, ((0, 8), (2, 4)))
    w_up = centred(key_list[13], (EXPERTS, D, EXPERT_WIDTH), D ** -0.5, 0.125, ((0, 8), (2, 4)))
    w_down = centred(key_list[14], (EXPERTS, EXPERT_WIDTH, D), EXPERT_WIDTH ** -0.5, 0.1875, ((0, 8), (1, 4)))
    return {"query": query, "latent": latent, "rope_key": rope_key, "latent_gain": latent_gain, "key_up": key_up, "value_up": value_up, "out_proj": out_proj, "tokens": tokens, "moe_gain": moe_gain, "routes": routes, "group_prob": group_prob, "expert_prob": expert_prob, "w_gate": w_gate, "w_up": w_up, "w_down": w_down}


epsilon = 1e-06
rope_base = 10000.0
masked_value = -1e+30

def rms_scale(values, gain):
    widened = values.astype(jnp.float32)
    return widened * lax.rsqrt(lax.optimization_barrier(jnp.mean(widened * widened, axis=-1, keepdims=True)) + epsilon) * gain.astype(jnp.float32)

def tables(positions, rope_width):
    half_width = rope_width // 2
    inverse = rope_base ** (-2.0 * jnp.arange(half_width, dtype=jnp.float32) / rope_width)
    angles = positions.astype(jnp.float32)[:, None] * inverse[None, :]
    return (jnp.cos(angles), jnp.sin(angles))

def rotate(values, cosine, sine):
    half_width = values.shape[-1] // 2
    lower = values[..., :half_width]
    upper = values[..., half_width:]
    return jnp.concatenate([lower * cosine - upper * sine, lower * sine + upper * cosine], axis=-1)

def head_attention(rope_prefix, query_pos, parts):
    query_head, key_head, value_head = parts
    full_keys = jnp.concatenate([key_head, rope_prefix], axis=-1)
    scores = jnp.dot(query_head, full_keys.T, preferred_element_type=jnp.float32) * (NOPE + ROPE_DIM) ** (-0.5)
    key_pos = jnp.arange(full_keys.shape[0], dtype=jnp.int32)
    allowed = key_pos[None, :] <= query_pos[:, None]
    scores = jnp.where(allowed, scores, masked_value)
    row_peak = lax.optimization_barrier(jnp.max(scores, axis=-1, keepdims=True))
    raised = jnp.where(allowed, jnp.exp(scores - row_peak), 0.0)
    totals = lax.optimization_barrier(jnp.sum(raised, axis=-1, keepdims=True))
    summed = jnp.dot(raised.astype(jnp.bfloat16), value_head, preferred_element_type=jnp.float32)
    return (summed / totals).astype(jnp.bfloat16)

def mixer_reference(query, latent, rope_key, latent_gain, key_up, value_up, out_proj):
    seq_len = latent.shape[0]
    positions = jnp.arange(seq_len, dtype=jnp.int32)
    cosine, sine = tables(positions, ROPE_DIM)
    normed = rms_scale(latent, latent_gain).astype(jnp.bfloat16)
    rotated_key = rotate(rope_key.astype(jnp.float32), cosine, sine).astype(jnp.bfloat16)
    query_heads = query.reshape(seq_len, HEADS, NOPE + ROPE_DIM)
    turned = rotate(query_heads[..., NOPE:].astype(jnp.float32), cosine[:, None, :], sine[:, None, :]).astype(jnp.bfloat16)
    rotated_query = jnp.concatenate([query_heads[..., :NOPE], turned], axis=-1)
    key_nope = jnp.dot(normed, key_up, preferred_element_type=jnp.float32).astype(jnp.bfloat16).reshape(seq_len, HEADS, NOPE)
    values = jnp.dot(normed, value_up, preferred_element_type=jnp.float32).astype(jnp.bfloat16).reshape(seq_len, HEADS, V_DIM)
    block_len = math.gcd(seq_len, 512)
    pieces = []
    for block_at in range(seq_len // block_len):
        upto = (block_at + 1) * block_len
        query_pos = positions[block_at * block_len:upto]
        parts = (rotated_query[block_at * block_len:upto].transpose(1, 0, 2), key_nope[:upto].transpose(1, 0, 2), values[:upto].transpose(1, 0, 2))
        result = lax.map(functools.partial(head_attention, rotated_key[:upto], query_pos), parts)
        pieces.append(result.transpose(1, 0, 2).reshape(block_len, HEADS * V_DIM))
    attention = jnp.concatenate(pieces, axis=0)
    return jnp.dot(attention, out_proj, preferred_element_type=jnp.float32).astype(jnp.bfloat16)

def expert_reference(tokens, moe_gain, routes, group_prob, expert_prob, w_gate, w_up, w_down):
    amount = tokens.shape[0]
    model_width = tokens.shape[1]
    expert_count = w_gate.shape[0]
    block_count = amount // M_ROWS
    normed = rms_scale(tokens, moe_gain).astype(jnp.bfloat16)
    flat_routes = routes.reshape(block_count, M_ROWS * TOP)
    onehot = (flat_routes[:, :, None] == jnp.arange(expert_count, dtype=jnp.int32)[None, None, :]).astype(jnp.int32)
    earlier = jnp.cumsum(onehot, axis=1) - onehot
    slot_index = lax.optimization_barrier(jnp.sum(earlier * onehot, axis=2))
    block_ids = jnp.arange(block_count, dtype=jnp.int32)[:, None]
    place = block_ids * CAP + slot_index
    source_row = block_ids * M_ROWS + jnp.arange(M_ROWS * TOP, dtype=jnp.int32)[None, :] // TOP
    shares = group_prob[:, None] * expert_prob / lax.optimization_barrier(jnp.sum(expert_prob, axis=1, keepdims=True))
    row_table = jnp.full((expert_count, block_count * CAP), amount, jnp.int32).at[flat_routes, place].set(source_row)
    share_table = jnp.zeros((expert_count, block_count * CAP), jnp.float32).at[flat_routes, place].set(shares.reshape(block_count, M_ROWS * TOP))
    padded = jnp.concatenate([normed, jnp.zeros((1, model_width), jnp.bfloat16)], axis=0)
    group_width = w_down.shape[1] // N_TP

    def per_expert(running, parts):
        row_ids, row_shares, gate_weight, up_weight, down_weight = parts
        rows_here = padded[row_ids]
        gate_values = jnp.dot(rows_here, gate_weight, preferred_element_type=jnp.float32)
        up_values = jnp.dot(rows_here, up_weight, preferred_element_type=jnp.float32)
        hidden = (jax.nn.silu(gate_values) * up_values).astype(jnp.bfloat16)
        summed = jnp.zeros((rows_here.shape[0], model_width), jnp.float32)
        for group_at in range(N_TP):
            lower_edge = group_at * group_width
            partial_low = jnp.dot(hidden[:, lower_edge:lower_edge + group_width], down_weight[lower_edge:lower_edge + group_width], preferred_element_type=jnp.float32).astype(jnp.bfloat16)
            partial_low = lax.optimization_barrier(partial_low)
            summed = summed + partial_low.astype(jnp.float32)
        expert_out = summed.astype(jnp.bfloat16)
        expert_out = lax.optimization_barrier(expert_out)
        running = running.at[row_ids].add(row_shares[:, None] * expert_out.astype(jnp.float32))
        return (running, None)
    running, _ = lax.scan(per_expert, jnp.zeros((amount + 1, model_width), jnp.float32), (row_table, share_table, w_gate, w_up, w_down))
    return running[:amount].astype(jnp.bfloat16)

def reference(query, latent, rope_key, latent_gain, key_up, value_up, out_proj, tokens, moe_gain, routes, group_prob, expert_prob, w_gate, w_up, w_down):
    mixed = mixer_reference(query, latent, rope_key, latent_gain, key_up, value_up, out_proj)
    moe_out = expert_reference(tokens, moe_gain, routes, group_prob, expert_prob, w_gate, w_up, w_down)
    return (mixed, moe_out)
```

```python
import functools
import math

import jax
import jax.numpy as jnp
from jax import lax
from jax.experimental import pallas as pl
from jax.experimental.pallas import tpu as pltpu
from jax.sharding import PartitionSpec as P

NOPE = 64
ROPE_DIM = 32
V_DIM = 64


epsilon = 1e-06
rope_base = 10000.0
masked_value = -1e30


def rms_scale(values, gain):
    widened = values.astype(jnp.float32)
    return widened * lax.rsqrt(jnp.mean(widened * widened, axis=-1, keepdims=True) + epsilon) * gain


def tables(positions, rope_width):
    half_width = rope_width // 2
    inverse = rope_base ** (-2.0 * jnp.arange(half_width, dtype=jnp.float32) / rope_width)
    angles = positions.astype(jnp.float32)[:, None] * inverse[None, :]
    return (jnp.cos(angles), jnp.sin(angles))


def rotate(values, cosine, sine):
    half_width = values.shape[-1] // 2
    lower = values[..., :half_width]
    upper = values[..., half_width:]
    return jnp.concatenate([lower * cosine - upper * sine, lower * sine + upper * cosine], axis=-1)


def keep_state(state_in):
    return state_in


def attend_block(running, query_rot, query_pos, key_part, value_part, rope_part):
    amount = key_part.shape[0]
    span_rows = math.gcd(amount, 1024)
    head_count = query_rot.shape[1]
    scale_factor = query_rot.shape[2] ** (-0.5)
    last_query = query_pos[-1]

    def update(state, block_at):
        row_begin = block_at * span_rows
        keys_here = lax.dynamic_slice_in_dim(key_part, row_begin, span_rows, 0).reshape(
            span_rows, head_count, -1
        )
        values_here = lax.dynamic_slice_in_dim(value_part, row_begin, span_rows, 0).reshape(
            span_rows, head_count, -1
        )
        rope_here = lax.dynamic_slice_in_dim(rope_part, row_begin, span_rows, 0)
        key_pos = row_begin + jnp.arange(span_rows, dtype=jnp.int32)

        def advance(state_in):
            top_old, totals, weighted = state_in
            shared = jnp.broadcast_to(
                rope_here[:, None, :], (span_rows, head_count, rope_here.shape[1])
            )
            full_keys = jnp.concatenate([keys_here, shared], axis=-1)
            scores = (
                jnp.einsum("qhd,khd->hqk", query_rot, full_keys, preferred_element_type=jnp.float32)
                * scale_factor
            )
            allowed = key_pos[None, :] <= query_pos[:, None]
            scores = jnp.where(allowed[None], scores, masked_value)
            top_new = jnp.maximum(top_old, jnp.max(scores, axis=-1))
            raised = jnp.where(allowed[None], jnp.exp(scores - top_new[..., None]), 0.0)
            factor = jnp.exp(top_old - top_new)
            totals = totals * factor + jnp.sum(raised, axis=-1)
            weighted = weighted * factor[..., None] + jnp.einsum(
                "hqk,khd->hqd",
                raised.astype(jnp.bfloat16),
                values_here,
                preferred_element_type=jnp.float32,
            )
            return (top_new, totals, weighted)

        return (lax.cond(key_pos[0] <= last_query, advance, keep_state, state), None)

    running, _ = lax.scan(update, running, jnp.arange(amount // span_rows))
    return running


def mixer_half(query, latent, rope_key, latent_gain, key_up, value_up, out_proj):
    query_rows = query.shape[0]
    own_rows = latent.shape[0]
    query_start = lax.axis_index("ep") * query_rows
    key_start = query_start + lax.axis_index("tp") * own_rows
    head_count = query.shape[1] // (NOPE + ROPE_DIM)
    normed = rms_scale(latent, latent_gain).astype(jnp.bfloat16)
    key_cos, key_sin = tables(key_start + jnp.arange(own_rows, dtype=jnp.int32), ROPE_DIM)
    rotated_key = rotate(rope_key.astype(jnp.float32), key_cos, key_sin).astype(jnp.bfloat16)
    query_pos = query_start + jnp.arange(query_rows, dtype=jnp.int32)
    query_cos, query_sin = tables(query_pos, ROPE_DIM)
    query_heads = query.reshape(query_rows, head_count, NOPE + ROPE_DIM)
    turned = rotate(
        query_heads[..., NOPE:].astype(jnp.float32), query_cos[:, None, :], query_sin[:, None, :]
    ).astype(jnp.bfloat16)
    query_rot = jnp.concatenate([query_heads[..., :NOPE], turned], axis=-1)
    last_query = query_start + query_rows - 1
    initial = (
        jnp.full((head_count, query_rows), masked_value, jnp.float32),
        jnp.zeros((head_count, query_rows), jnp.float32),
        jnp.zeros((head_count, query_rows, V_DIM), jnp.float32),
    )
    shard_rows = (
        lax.all_gather(normed, ("ep", "tp"), axis=0, tiled=True),
        lax.all_gather(rotated_key, ("ep", "tp"), axis=0, tiled=True),
    )

    def compute(state_in):
        key_part = jnp.dot(shard_rows[0], key_up, preferred_element_type=jnp.float32).astype(
            jnp.bfloat16
        )
        value_part = jnp.dot(shard_rows[0], value_up, preferred_element_type=jnp.float32).astype(
            jnp.bfloat16
        )
        return attend_block(state_in, query_rot, query_pos, key_part, value_part, shard_rows[1])

    running = lax.cond(jnp.int32(0) <= last_query, compute, keep_state, initial)
    totals = running[1]
    weighted = running[2]
    attention = (
        (weighted / totals[..., None])
        .transpose(1, 0, 2)
        .reshape(query_rows, head_count * V_DIM)
        .astype(jnp.bfloat16)
    )
    own_attention = lax.all_to_all(attention, "tp", split_axis=0, concat_axis=1, tiled=True)
    return jnp.dot(own_attention, out_proj, preferred_element_type=jnp.float32).astype(jnp.bfloat16)


def expert_half(tokens, moe_gain, routes, group_prob, expert_prob, w_gate, w_up, w_down):
    row_count, model_width = tokens.shape
    top_count = routes.shape[1]
    expert_count = lax.axis_size("ep")
    capacity = 2 * top_count * row_count // expert_count
    normed = rms_scale(tokens, moe_gain).astype(jnp.bfloat16)
    flat_routes = routes.reshape(-1)
    onehot = (flat_routes[:, None] == jnp.arange(expert_count, dtype=jnp.int32)[None, :]).astype(
        jnp.int32
    )
    earlier = jnp.cumsum(onehot, axis=0) - onehot
    slot_index = jnp.sum(earlier * onehot, axis=1)
    target = flat_routes * capacity + slot_index
    owner = target[None, :] == jnp.arange(expert_count * capacity, dtype=jnp.int32)[:, None]
    dispatch_table = jnp.any(
        owner.reshape(expert_count * capacity, row_count, top_count), axis=2
    ).astype(jnp.bfloat16)
    outgoing = jnp.dot(dispatch_table, normed, preferred_element_type=jnp.float32).astype(
        jnp.bfloat16
    )
    outgoing = outgoing.reshape(expert_count, capacity, model_width)
    arrived = lax.all_to_all(outgoing, "ep", split_axis=0, concat_axis=0, tiled=True)
    sources, slots, _ = arrived.shape
    flat_rows = arrived.reshape(sources * slots, model_width)
    shard_rows = lax.all_gather(flat_rows, "tp", axis=0, tiled=True)
    gate_values = jnp.dot(shard_rows, w_gate[0], preferred_element_type=jnp.float32)
    up_values = jnp.dot(shard_rows, w_up[0], preferred_element_type=jnp.float32)
    hidden = (jax.nn.silu(gate_values) * up_values).astype(jnp.bfloat16)

    def lower(offset, amount):
        return jnp.dot(hidden, w_down[0], preferred_element_type=jnp.float32)

    summed = lax.psum_scatter(
        lower(jnp.int32(0), sources * slots * lax.axis_size("tp")).astype(jnp.bfloat16),
        "tp",
        scatter_dimension=0,
        tiled=True,
    )
    result = summed.reshape(sources, slots, model_width)
    returned = lax.all_to_all(result, "ep", split_axis=0, concat_axis=0, tiled=True)
    returned_flat = returned.reshape(expert_count * capacity, model_width)
    picked = returned_flat[target].reshape(row_count, top_count, model_width).astype(jnp.float32)
    shares = group_prob[:, None] * expert_prob / jnp.sum(expert_prob, axis=1, keepdims=True)
    return jnp.sum(shares[:, :, None] * picked, axis=1).astype(jnp.bfloat16)


def body(
    query,
    latent,
    rope_key,
    latent_gain,
    key_up,
    value_up,
    out_proj,
    tokens,
    moe_gain,
    routes,
    group_prob,
    expert_prob,
    w_gate,
    w_up,
    w_down,
):
    mixed = mixer_half(query, latent, rope_key, latent_gain, key_up, value_up, out_proj)
    moe_out = expert_half(tokens, moe_gain, routes, group_prob, expert_prob, w_gate, w_up, w_down)
    return (mixed, moe_out)


def padded(amount):
    return -(-amount // 128) * 128


def line_order(place, depth, spot):
    near = jnp.minimum(place, depth - 1 - place)
    from_low = jnp.where(spot < 2, (spot + near) % 2, spot)
    return jnp.where(place < depth // 2, from_low, depth - 1 - from_low)


def angle_tables(first_row, rows, lanes):
    half_width = ROPE_DIM // 2
    lane = lax.broadcasted_iota(jnp.int32, (rows, lanes), 1) % half_width
    position = first_row + lax.broadcasted_iota(jnp.int32, (rows, lanes), 0)
    inverse = jnp.exp(lane.astype(jnp.float32) * (-2.0 * math.log(rope_base) / ROPE_DIM))
    angles = position.astype(jnp.float32) * inverse
    return (jnp.cos(angles), jnp.sin(angles))


def turn_tables(rows, lanes, first):
    half_width = ROPE_DIM // 2
    row = lax.broadcasted_iota(jnp.int32, (rows, lanes), 0) - first
    lane = lax.broadcasted_iota(jnp.int32, (rows, lanes), 1)
    same = jnp.where((row == lane) & (lane < ROPE_DIM), 1.0, 0.0)
    lower = jnp.where((row == lane + half_width) & (lane < half_width), -1.0, 0.0)
    upper = jnp.where(
        (row == lane - half_width) & (lane >= half_width) & (lane < ROPE_DIM), 1.0, 0.0
    )
    return (same.astype(jnp.bfloat16), (lower + upper).astype(jnp.bfloat16))


def both_halves(
    heads,
    capacity,
    depth_z,
    tokens,
    moe_gain,
    routes,
    group_prob,
    expert_prob,
    latent,
    rope_key,
    latent_gain,
    query_hbm,
    key_up_hbm,
    value_up_hbm,
    out_proj_hbm,
    gate_hbm,
    up_hbm,
    down_hbm,
    mixed,
    moe_out,
    tok,
    info,
    away,
    arrived,
    lat_all,
    partial,
    from_pair,
    pair_sum,
    from_far,
    result,
    returned,
    joined,
    answers,
    passing,
    keys,
    query_big,
    heads_own,
    heads_all,
    query,
    key_up,
    value_up,
    out_proj,
    gate,
    up,
    down,
    load_sem,
    send_sem,
    recv_sem,
):
    row_count, width = tokens.shape
    own_rows, latent_width = latent.shape
    experts = 2 * depth_z
    units = 2 * depth_z
    n_tp = lat_all.shape[2]
    rope_room = lat_all.shape[-1] - latent_width
    bf16 = jnp.bfloat16
    f32 = jnp.float32
    me = lax.axis_index("ep")
    tp = lax.axis_index("tp")
    me_z = me // 2
    me_y = me % 2
    beside = me_z * 2 + 1 - me_y
    inner = (me_z > 0) & (me_z < depth_z - 1)
    inward = jnp.where(me_z < depth_z // 2, me_z + 1, me_z - 1)
    mate = tp + 1 - 2 * (tp % 2)
    far = (tp + 2) % n_tp
    cross = (mate + 2) % n_tp

    barrier = pltpu.get_barrier_semaphore()

    def greet(shift, carry):
        pl.semaphore_signal(
            barrier,
            inc=1,
            device_id={"ep": (me_z + shift) % depth_z * 2 + me_y},
            device_id_type=pl.DeviceIdType.MESH,
        )
        return carry

    lax.fori_loop(1, depth_z, greet, 0)
    pl.semaphore_signal(
        barrier, inc=1, device_id={"ep": beside}, device_id_type=pl.DeviceIdType.MESH
    )
    for peer in (mate, far, cross):
        pl.semaphore_signal(
            barrier, inc=1, device_id={"tp": peer}, device_id_type=pl.DeviceIdType.MESH
        )

    loads = [
        pltpu.make_async_copy(gate_hbm, gate, load_sem.at[0]),
        pltpu.make_async_copy(up_hbm, up, load_sem.at[1]),
        pltpu.make_async_copy(down_hbm, down, load_sem.at[2]),
        pltpu.make_async_copy(query_hbm, query, load_sem.at[3]),
        pltpu.make_async_copy(key_up_hbm, key_up, load_sem.at[4]),
        pltpu.make_async_copy(value_up_hbm, value_up, load_sem.at[5]),
        pltpu.make_async_copy(out_proj_hbm, out_proj, load_sem.at[6]),
    ]
    for load in loads:
        load.start()

    def remote(src, dst, sent, got, device):
        return pltpu.make_async_remote_copy(
            src_ref=src,
            dst_ref=dst,
            send_sem=send_sem.at[sent[0], sent[1]],
            recv_sem=recv_sem.at[got[0], got[1]],
            device_id=device,
            device_id_type=pl.DeviceIdType.MESH,
        )

    def tok_step(origin, step):
        kind = 0 if step > 0 else 1
        target = {"ep": (me_z + step) * 2 + me_y}
        return (
            remote(tok.at[origin], tok.at[origin], (kind, origin), (0, origin), target),
            remote(info.at[origin], info.at[origin], (kind + 2, origin), (2, origin), target),
        )

    def spread_tok(origin, step):
        inside = (me_z < depth_z - 1) if step > 0 else (me_z > 0)
        coming = (origin <= me_z) if step > 0 else (origin >= me_z)
        return inside & coming

    def source_of(unit):
        return line_order(me_z, depth_z, unit // 2) * 2 + (me_y + unit) % 2

    def hop_rows(kind, unit, block, peer):
        place = arrived.at[source_of(unit), block]
        return remote(place, place, (kind, unit), (kind, unit), {"tp": peer})

    def y_rows(spot):
        origin = line_order(me_z, depth_z, spot)
        return remote(
            away.at[origin],
            arrived.at[origin * 2 + me_y, tp],
            (7, spot),
            (7, spot),
            {"ep": beside},
        )

    def to_mate(kind, unit, block, part):
        source = source_of(unit)
        return remote(
            partial.at[source, block],
            from_pair.at[source, part],
            (kind, unit),
            (kind, unit),
            {"tp": mate},
        )

    def to_far(unit):
        source = source_of(unit)
        return remote(
            pair_sum.at[source], from_far.at[source], (10, unit), (10, unit), {"tp": far}
        )

    def y_back(spot):
        origin = line_order(me_z, depth_z, spot)
        return remote(
            result.at[origin * 2 + 1 - me_y],
            returned.at[origin],
            (11, spot),
            (11, spot),
            {"ep": beside},
        )

    def z_back(origin, sender):
        return remote(
            joined.at[origin],
            answers.at[sender],
            (12, origin),
            (12, sender),
            {"ep": origin * 2 + me_y},
        )

    def z_pass():
        return remote(
            joined.at[line_order(me_z, depth_z, 2)],
            passing,
            (18, 0),
            (18, 0),
            {"ep": inward * 2 + me_y},
        )

    def lat_x(block):
        place = lat_all.at[me_z, me_y, block]
        return remote(place, place, (13, 0), (13, 0), {"tp": far})

    def lat_z(shift, part, origin):
        block = (tp + 2 * part) % n_tp
        target = (me_z + shift) % depth_z * 2 + me_y
        number = shift * 2 + part
        return remote(
            lat_all.at[me_z, me_y, block],
            lat_all.at[origin, me_y, block],
            (14, number),
            (14, number),
            {"ep": target},
        )

    def lat_y(part, side):
        place = lat_all.at[:, side, (tp + 2 * part) % n_tp]
        return remote(place, place, (15, part), (15, part), {"ep": beside})

    def lat_mate(part, first):
        place = lat_all.at[:, :, (first + 2 * part) % n_tp]
        return remote(place, place, (16, part), (16, part), {"tp": mate})

    def head_copy(number, peer, slot):
        return remote(
            heads_own.at[peer], heads_all.at[slot], (17, number), (17, number), {"tp": peer}
        )

    first_route = routes[0:1, :]
    second_route = routes[1:2, :]
    lane_expert = lax.broadcasted_iota(jnp.int32, (experts, row_count), 0)
    is_first = lane_expert == first_route
    is_second = lane_expert == second_route
    named = jnp.where(is_first | is_second, 1.0, 0.0).astype(bf16)
    ahead = lax.broadcasted_iota(jnp.int32, (row_count, row_count), 0)
    behind = lax.broadcasted_iota(jnp.int32, (row_count, row_count), 1)
    before = jnp.where(ahead < behind, 1.0, 0.0).astype(bf16)
    earlier = jnp.dot(named, before, preferred_element_type=f32)
    first_slot = jnp.sum(jnp.where(is_first, earlier, 0.0), axis=0, keepdims=True)
    second_slot = jnp.sum(jnp.where(is_second, earlier, 0.0), axis=0, keepdims=True)
    both_prob = expert_prob[0:1, :] + expert_prob[1:2, :]
    info[me_z] = jnp.full(info.shape[1:], -1.0, f32)
    info[me_z, 0:1, 0:row_count] = first_route.astype(f32) * capacity + first_slot
    info[me_z, 1:2, 0:row_count] = second_route.astype(f32) * capacity + second_slot
    info[me_z, 2:3, 0:row_count] = group_prob[...] * expert_prob[0:1, :] / both_prob
    info[me_z, 3:4, 0:row_count] = group_prob[...] * expert_prob[1:2, :] / both_prob
    tok[me_z] = rms_scale(tokens[...], moe_gain[...]).astype(bf16)

    pl.semaphore_wait(barrier, depth_z + 3)

    for step in (1, -1):

        @pl.when(spread_tok(me_z, step))
        def _(step=step):
            for copy in tok_step(me_z, step):
                copy.start()

    def wanted():
        row = lax.broadcasted_iota(jnp.int32, (2 * capacity, info.shape[2]), 0)
        own = me * capacity + row
        other = (beside - 1) * capacity + row
        return jnp.where(row < capacity, own, other).astype(f32)

    def take_tok(spot):
        origin = line_order(me_z, depth_z, spot)
        for copy in tok_step(origin, 1):
            copy.wait_recv()
        for step in (1, -1):

            @pl.when(spread_tok(origin, step))
            def _(step=step):
                for copy in tok_step(origin, step):
                    copy.start()

    def gather_spot(spot):
        origin = line_order(me_z, depth_z, spot)

        @pl.when((spot > 0) & jnp.logical_not(inner))
        def _():
            take_tok(spot)

        want = wanted()
        table = jnp.where(
            (want == info[origin, 0:1, :]) | (want == info[origin, 1:2, :]), 1.0, 0.0
        )
        packed = jnp.dot(
            table[:, :row_count].astype(bf16), tok[origin], preferred_element_type=f32
        ).astype(bf16)
        arrived[origin * 2 + me_y, tp] = packed[:capacity]
        away[origin] = packed[capacity:]
        y_rows(spot).start()

    def forward(unit):
        spot = unit // 2

        @pl.when(unit % 2 == 0)
        def _():
            gather_spot(spot)

        @pl.when(unit % 2 == 1)
        def _():
            y_rows(spot).wait_recv()

        hop_rows(4, unit, tp, far).start()
        hop_rows(5, unit, tp, mate).start()

    def relay(unit):
        hop_rows(4, unit, far, far).wait_recv()
        hop_rows(6, unit, far, mate).start()

    def compute(unit):
        source = source_of(unit)
        hop_rows(5, unit, mate, mate).wait_recv()
        hop_rows(6, unit, cross, mate).wait_recv()

        @pl.when(unit == 0)
        def _():
            for load in loads[:3]:
                load.wait()

        rows = arrived[source].reshape(n_tp * capacity, width)
        gate_values = jnp.dot(rows, gate[...], preferred_element_type=f32)
        up_values = jnp.dot(rows, up[...], preferred_element_type=f32)
        hidden = (gate_values / (1.0 + jnp.exp(-gate_values)) * up_values).astype(bf16)
        product = jnp.dot(hidden, down[...], preferred_element_type=f32)
        partial[source] = product.astype(bf16).reshape(n_tp, capacity, width)
        to_mate(9, unit, cross, 1).start()
        to_mate(8, unit, mate, 0).start()

    def reduce_pair(unit):
        source = source_of(unit)
        to_mate(9, unit, cross, 1).wait_recv()
        pair_sum[source] = (
            partial[source, far].astype(f32) + from_pair[source, 1].astype(f32)
        ).astype(bf16)

    def reduce_far(unit):
        source = source_of(unit)
        to_mate(8, unit, mate, 0).wait_recv()
        to_far(unit).wait_recv()
        result[source] = (
            partial[source, tp].astype(f32)
            + from_pair[source, 0].astype(f32)
            + from_far[source].astype(f32)
        ).astype(bf16)

        @pl.when(unit % 2 == 1)
        def _():
            y_back(unit // 2).start()

    def weighted(spot):
        origin = line_order(me_z, depth_z, spot)
        y_back(spot).wait_recv()
        want = wanted()
        weights = jnp.where(want == info[origin, 0:1, :], info[origin, 2:3, :], 0.0) + jnp.where(
            want == info[origin, 1:2, :], info[origin, 3:4, :], 0.0
        )
        weights = weights[:, :row_count]
        high = weights.astype(bf16)
        low = (weights - high.astype(f32)).astype(bf16)
        rows = jnp.concatenate([result[origin * 2 + me_y], returned[origin]], axis=0)
        over_slots = (((0,), (0,)), ((), ()))
        return lax.dot_general(
            high, rows, over_slots, preferred_element_type=f32
        ) + lax.dot_general(low, rows, over_slots, preferred_element_type=f32)

    def join(spot):
        origin = line_order(me_z, depth_z, spot)
        joined[origin] = weighted(spot).astype(bf16)
        z_back(origin, me_z).start()

    def join_pass():
        origin = line_order(me_z, depth_z, 2)
        joined[origin] = weighted(2).astype(bf16)
        z_pass().start()

    def join_passed():
        origin = line_order(me_z, depth_z, 2)
        own = weighted(2)
        z_pass().wait_recv()
        joined[origin] = (own + passing[...].astype(f32)).astype(bf16)
        z_back(origin, me_z).start()

    def own_latent():
        same, swapped = turn_tables(ROPE_DIM, rope_room, 0)
        first_row = (me * n_tp + tp) * own_rows
        cosine, sine = angle_tables(first_row, own_rows, rope_room)
        turned = jnp.dot(rope_key[...], same, preferred_element_type=f32) * cosine + (
            jnp.dot(rope_key[...], swapped, preferred_element_type=f32) * sine
        )
        lat_all[me_z, me_y, tp, :, :latent_width] = rms_scale(
            latent[...], latent_gain[...]
        ).astype(bf16)
        lat_all[me_z, me_y, tp, :, latent_width:] = turned.astype(bf16)
        lat_x(tp).start()

    def spread_query():
        loads[3].wait()
        rows, packed_width = query.shape
        head_width = packed_width // heads
        nope_width = heads * NOPE
        cosine, sine = angle_tables(me * rows, rows, rope_room)
        row = lax.broadcasted_iota(jnp.int32, (packed_width, nope_width), 0)
        lane = lax.broadcasted_iota(jnp.int32, (packed_width, nope_width), 1)
        out_lane = lax.broadcasted_iota(jnp.int32, (rows, nope_width), 1)
        plain = jnp.zeros((packed_width, nope_width), f32)
        for head in range(heads):
            inside = (lane >= head * NOPE) & (lane < (head + 1) * NOPE)
            plain = jnp.where(inside & (row - lane == head * ROPE_DIM), 1.0, plain)
        nope = jnp.dot(query[...], plain.astype(bf16), preferred_element_type=f32)
        for head in range(heads):
            inside = (out_lane >= head * NOPE) & (out_lane < (head + 1) * NOPE)
            query_big[head, :, :nope_width] = jnp.where(inside, nope, 0.0).astype(bf16)
            same, swapped = turn_tables(packed_width, rope_room, head * head_width + NOPE)
            turned = jnp.dot(query[...], same, preferred_element_type=f32) * cosine + (
                jnp.dot(query[...], swapped, preferred_element_type=f32) * sine
            )
            query_big[head, :, nope_width:] = turned.astype(bf16)

    def attend():
        rows = query_big.shape[1]
        nope_width = key_up.shape[1]
        value_width = value_up.shape[1] // heads
        packed = lat_all[...].reshape(-1, lat_all.shape[-1])
        normed = packed[:, :latent_width]
        seq = packed.shape[0]
        loads[4].wait()
        loads[5].wait()
        keys[:, :nope_width] = jnp.dot(normed, key_up[...], preferred_element_type=f32).astype(bf16)
        keys[:, nope_width:] = packed[:, latent_width:]
        values = jnp.dot(normed, value_up[...], preferred_element_type=f32).astype(bf16)
        query_pos = me * rows + lax.broadcasted_iota(jnp.int32, (rows, seq), 0)
        allowed = lax.broadcasted_iota(jnp.int32, (rows, seq), 1) <= query_pos
        lane = lax.broadcasted_iota(jnp.int32, (rows, heads * value_width), 1)
        scale = (nope_width // heads + ROPE_DIM) ** (-0.5)
        gathered = jnp.zeros((rows, heads * value_width), f32)
        for head in range(heads):
            scores = (
                lax.dot_general(
                    query_big[head],
                    keys[...],
                    (((1,), (1,)), ((), ())),
                    preferred_element_type=f32,
                )
                * scale
            )
            scores = jnp.where(allowed, scores, masked_value)
            raised = jnp.exp(scores - jnp.max(scores, axis=1, keepdims=True))
            totals = jnp.sum(raised, axis=1, keepdims=True)
            summed = jnp.dot(raised.astype(bf16), values, preferred_element_type=f32)
            inside = (lane >= head * value_width) & (lane < (head + 1) * value_width)
            gathered = jnp.where(inside, summed / totals, gathered)
        heads_own[...] = gathered.astype(bf16).reshape(heads_own.shape)

    peers = (mate, far, cross)

    @pl.when(inner)
    def _():
        answers[line_order(me_z, depth_z, 3)] = jnp.zeros(answers.shape[1:], bf16)

    def stage(turn, carry):
        @pl.when((turn == 2) & inner)
        def _():
            take_tok(1)
            take_tok(2)

        @pl.when((turn == 4) & inner)
        def _():
            take_tok(3)

        @pl.when(turn < units)
        def _():
            forward(turn)

        @pl.when(turn == 0)
        def _():
            own_latent()

        @pl.when(turn == 5)
        def _():
            lat_x(far).wait_recv()

            def spread(shift, inside):
                lat_z(shift, 0, me_z).start()
                lat_z(shift, 1, me_z).start()
                return inside

            lax.fori_loop(1, depth_z, spread, 0)

        @pl.when((turn >= 1) & (turn < units + 1))
        def _():
            relay(turn - 1)

        @pl.when(turn >= 3)
        def _():
            reduce_pair(turn - 3)

            @pl.when((turn - 3 >= units - 4) & (turn - 3 < units - 2))
            def _():
                to_far(turn - 3).start()

        @pl.when((turn >= 2) & (turn < units + 2))
        def _():
            compute(turn - 2)

        @pl.when(turn == 2)
        def _():
            spread_query()

        @pl.when(turn == units)
        def _():
            def collect(shift, inside):
                origin = (me_z + depth_z - shift) % depth_z
                lat_z(shift, 0, origin).wait_recv()
                lat_z(shift, 1, origin).wait_recv()
                return inside

            lax.fori_loop(1, depth_z, collect, 0)
            lat_y(0, me_y).start()
            lat_y(1, me_y).start()

        return carry

    lax.fori_loop(0, units + 3, stage, 0)

    for unit in (7, 6, 3, 2, 1, 0):
        to_far(unit).start()

    reduce_far(4)
    reduce_far(5)
    reduce_far(7)

    @pl.when(jnp.logical_not(inner))
    def _():
        join_pass()

    lat_y(0, 1 - me_y).wait_recv()
    lat_y(1, 1 - me_y).wait_recv()
    lat_mate(0, tp).start()
    lat_mate(1, tp).start()
    reduce_far(6)
    join(3)
    lat_mate(0, mate).wait_recv()
    lat_mate(1, mate).wait_recv()
    attend()
    for number, peer in enumerate(peers):
        head_copy(number, peer, tp).start()
    heads_all[tp] = heads_own[tp]
    reduce_far(3)

    @pl.when(inner)
    def _():
        join_passed()

    reduce_far(2)
    join(1)
    reduce_far(1)
    loads[6].wait()
    for number, peer in enumerate(peers):
        head_copy(number, peer, peer).wait_recv()
    depth = heads_all.shape[2]
    total = jnp.zeros(mixed.shape, f32)
    for part in range(n_tp):
        total = total + jnp.dot(
            heads_all[part],
            out_proj[part * depth : (part + 1) * depth, :],
            preferred_element_type=f32,
        )
    mixed[...] = total.astype(mixed.dtype)
    reduce_far(0)
    chosen = weighted(0)
    for shift in range(1, depth_z):
        sender = (me_z + shift) % depth_z

        @pl.when(jnp.logical_not(inner & (sender == line_order(me_z, depth_z, 3))))
        def _(sender=sender):
            z_back(me_z, sender).wait_recv()

        chosen = chosen + answers[sender].astype(f32)
    moe_out[...] = chosen.astype(moe_out.dtype)

    def finish_line(origin, carry):
        for step in (1, -1):

            @pl.when(spread_tok(origin, step))
            def _(step=step):
                for copy in tok_step(origin, step):
                    copy.wait_send()

        y_rows(origin).wait_send()
        y_back(origin).wait_send()

        @pl.when((origin != me_z) & (inner | (origin != line_order(me_z, depth_z, 2))))
        def _():
            z_back(origin, me_z).wait_send()

        return carry

    lax.fori_loop(0, depth_z, finish_line, 0)

    @pl.when(jnp.logical_not(inner))
    def _():
        z_pass().wait_send()

    lat_x(tp).wait_send()

    def finish_lat(shift, carry):
        lat_z(shift, 0, me_z).wait_send()
        lat_z(shift, 1, me_z).wait_send()
        return carry

    lax.fori_loop(1, depth_z, finish_lat, 0)
    for part in range(2):
        lat_y(part, me_y).wait_send()
        lat_mate(part, tp).wait_send()

    def finish_tp(unit, carry):
        hop_rows(4, unit, tp, far).wait_send()
        hop_rows(5, unit, tp, mate).wait_send()
        hop_rows(6, unit, far, mate).wait_send()
        to_mate(9, unit, cross, 1).wait_send()
        to_mate(8, unit, mate, 0).wait_send()
        to_far(unit).wait_send()
        return carry

    lax.fori_loop(0, units, finish_tp, 0)
    for number, peer in enumerate(peers):
        head_copy(number, peer, tp).wait_send()


def hand_over(mixed_in, moe_in, mixed_out, moe_out):
    mixed_out[...] = mixed_in[...]
    moe_out[...] = moe_in[...]


def fused_body(
    query,
    latent,
    rope_key,
    latent_gain,
    key_up,
    value_up,
    out_proj,
    tokens,
    moe_gain,
    routes,
    group_prob,
    expert_prob,
    w_gate,
    w_up,
    w_down,
):
    n_ep = lax.axis_size("ep")
    n_tp = lax.axis_size("tp")
    depth_z = n_ep // 2
    query_rows = query.shape[0]
    own_rows, latent_width = latent.shape
    heads = query.shape[1] // (NOPE + ROPE_DIM)
    rope_room = padded(ROPE_DIM)
    row_count, width = tokens.shape
    capacity = 2 * routes.shape[1] * row_count // n_ep
    bf16 = jnp.bfloat16
    lat_width = latent_width + rope_room
    key_width = key_up.shape[1] + rope_room
    vmem = pl.BlockSpec(memory_space=pltpu.VMEM)
    anywhere = pl.BlockSpec(memory_space=pl.ANY)
    results = pl.pallas_call(
        functools.partial(both_halves, heads, capacity, depth_z),
        out_shape=(
            jax.ShapeDtypeStruct((own_rows, out_proj.shape[1]), bf16),
            jax.ShapeDtypeStruct((row_count, width), bf16),
        ),
        in_specs=[vmem] * 8 + [anywhere] * 7,
        out_specs=(vmem, vmem),
        scratch_shapes=[
            pltpu.VMEM((depth_z, row_count, width), bf16),
            pltpu.VMEM((depth_z, 8, padded(row_count)), jnp.float32),
            pltpu.VMEM((depth_z, capacity, width), bf16),
            pltpu.VMEM((n_ep, n_tp, capacity, width), bf16),
            pltpu.VMEM((depth_z, 2, n_tp, own_rows, lat_width), bf16),
            pltpu.VMEM((n_ep, n_tp, capacity, width), bf16),
            pltpu.VMEM((n_ep, 2, capacity, width), bf16),
            pltpu.VMEM((n_ep, capacity, width), bf16),
            pltpu.VMEM((n_ep, capacity, width), bf16),
            pltpu.VMEM((n_ep, capacity, width), bf16),
            pltpu.VMEM((depth_z, capacity, width), bf16),
            pltpu.VMEM((depth_z, row_count, width), bf16),
            pltpu.VMEM((depth_z, row_count, width), bf16),
            pltpu.VMEM((row_count, width), bf16),
            pltpu.VMEM((n_ep * n_tp * own_rows, key_width), bf16),
            pltpu.VMEM((heads, query_rows, key_width), bf16),
            pltpu.VMEM((n_tp, own_rows, value_up.shape[1]), bf16),
            pltpu.VMEM((n_tp, own_rows, value_up.shape[1]), bf16),
            pltpu.VMEM(query.shape, bf16),
            pltpu.VMEM(key_up.shape, bf16),
            pltpu.VMEM(value_up.shape, bf16),
            pltpu.VMEM(out_proj.shape, bf16),
            pltpu.VMEM(w_gate.shape[1:], bf16),
            pltpu.VMEM(w_up.shape[1:], bf16),
            pltpu.VMEM(w_down.shape[1:], bf16),
            pltpu.SemaphoreType.DMA((7,)),
            pltpu.SemaphoreType.DMA((19, n_ep)),
            pltpu.SemaphoreType.DMA((19, n_ep)),
        ],
        compiler_params=pltpu.CompilerParams(
            collective_id=0, has_side_effects=True, vmem_limit_bytes=60 * 1024 * 1024
        ),
        name="both_halves",
    )(
        tokens,
        moe_gain.reshape(1, -1),
        routes.T,
        group_prob.reshape(1, -1),
        expert_prob.T,
        latent,
        rope_key,
        latent_gain.reshape(1, -1),
        query,
        key_up,
        value_up,
        out_proj,
        w_gate[0],
        w_up[0],
        w_down[0],
    )
    return pl.pallas_call(
        hand_over,
        out_shape=tuple(jax.ShapeDtypeStruct(part.shape, part.dtype) for part in results),
        in_specs=[vmem] * 2,
        out_specs=(vmem, vmem),
        name="hand_over",
    )(*results)


def fits_kernel(mesh, *arrays):
    n_ep, n_tp = mesh.shape["ep"], mesh.shape["tp"]
    tokens, routes, latent = arrays[7], arrays[9], arrays[1]
    row_count = tokens.shape[0] // (n_ep * n_tp)
    capacity = 2 * routes.shape[1] * row_count // n_ep
    own_rows = latent.shape[0] // (n_ep * n_tp)
    shaped = n_tp == 4 and n_ep == 8 and routes.shape[1] == 2
    aligned = capacity % 16 == 0 and own_rows % 16 == 0 and row_count % 16 == 0
    return shaped and aligned and latent.shape[0] <= 2048


def mapped(mesh, chosen):
    return jax.shard_map(
        chosen,
        mesh=mesh,
        in_specs=(
            P("ep", "tp"),
            P(("ep", "tp"), None),
            P(("ep", "tp"), None),
            P(),
            P(None, "tp"),
            P(None, "tp"),
            P(),
            P(("ep", "tp"), None),
            P(),
            P(("ep", "tp"), None),
            P(("ep", "tp")),
            P(("ep", "tp"), None),
            P("ep", None, "tp"),
            P("ep", None, "tp"),
            P("ep", "tp", None),
        ),
        out_specs=(P(("ep", "tp"), None), P(("ep", "tp"), None)),
        check_vma=False,
    )


def solution(mesh):
    def whole(*arrays):
        chosen = fused_body if fits_kernel(mesh, *arrays) else body
        return mapped(mesh, chosen)(*arrays)

    return whole
```

```python
import functools
import math

import jax
import jax.numpy as jnp
from jax import lax
from jax.experimental import pallas as pl
from jax.experimental.pallas import tpu as pltpu
from jax.sharding import PartitionSpec as P

NOPE = 64
ROPE_DIM = 32
V_DIM = 64


epsilon = 1e-06
rope_base = 10000.0
masked_value = -1e30


def rms_scale(values, gain):
    widened = values.astype(jnp.float32)
    return widened * lax.rsqrt(jnp.mean(widened * widened, axis=-1, keepdims=True) + epsilon) * gain


def tables(positions, rope_width):
    half_width = rope_width // 2
    inverse = rope_base ** (-2.0 * jnp.arange(half_width, dtype=jnp.float32) / rope_width)
    angles = positions.astype(jnp.float32)[:, None] * inverse[None, :]
    return (jnp.cos(angles), jnp.sin(angles))


def rotate(values, cosine, sine):
    half_width = values.shape[-1] // 2
    lower = values[..., :half_width]
    upper = values[..., half_width:]
    return jnp.concatenate([lower * cosine - upper * sine, lower * sine + upper * cosine], axis=-1)


def keep_state(state_in):
    return state_in


def attend_block(running, query_rot, query_pos, key_part, value_part, rope_part):
    amount = key_part.shape[0]
    span_rows = math.gcd(amount, 1024)
    head_count = query_rot.shape[1]
    scale_factor = query_rot.shape[2] ** (-0.5)
    last_query = query_pos[-1]

    def update(state, block_at):
        row_begin = block_at * span_rows
        keys_here = lax.dynamic_slice_in_dim(key_part, row_begin, span_rows, 0).reshape(
            span_rows, head_count, -1
        )
        values_here = lax.dynamic_slice_in_dim(value_part, row_begin, span_rows, 0).reshape(
            span_rows, head_count, -1
        )
        rope_here = lax.dynamic_slice_in_dim(rope_part, row_begin, span_rows, 0)
        key_pos = row_begin + jnp.arange(span_rows, dtype=jnp.int32)

        def advance(state_in):
            top_old, totals, weighted = state_in
            shared = jnp.broadcast_to(
                rope_here[:, None, :], (span_rows, head_count, rope_here.shape[1])
            )
            full_keys = jnp.concatenate([keys_here, shared], axis=-1)
            scores = (
                jnp.einsum("qhd,khd->hqk", query_rot, full_keys, preferred_element_type=jnp.float32)
                * scale_factor
            )
            allowed = key_pos[None, :] <= query_pos[:, None]
            scores = jnp.where(allowed[None], scores, masked_value)
            top_new = jnp.maximum(top_old, jnp.max(scores, axis=-1))
            raised = jnp.where(allowed[None], jnp.exp(scores - top_new[..., None]), 0.0)
            factor = jnp.exp(top_old - top_new)
            totals = totals * factor + jnp.sum(raised, axis=-1)
            weighted = weighted * factor[..., None] + jnp.einsum(
                "hqk,khd->hqd",
                raised.astype(jnp.bfloat16),
                values_here,
                preferred_element_type=jnp.float32,
            )
            return (top_new, totals, weighted)

        return (lax.cond(key_pos[0] <= last_query, advance, keep_state, state), None)

    running, _ = lax.scan(update, running, jnp.arange(amount // span_rows))
    return running


def mixer_half(query, latent, rope_key, latent_gain, key_up, value_up, out_proj):
    query_rows = query.shape[0]
    own_rows = latent.shape[0]
    query_start = lax.axis_index("ep") * query_rows
    key_start = query_start + lax.axis_index("tp") * own_rows
    head_count = query.shape[1] // (NOPE + ROPE_DIM)
    normed = rms_scale(latent, latent_gain).astype(jnp.bfloat16)
    key_cos, key_sin = tables(key_start + jnp.arange(own_rows, dtype=jnp.int32), ROPE_DIM)
    rotated_key = rotate(rope_key.astype(jnp.float32), key_cos, key_sin).astype(jnp.bfloat16)
    query_pos = query_start + jnp.arange(query_rows, dtype=jnp.int32)
    query_cos, query_sin = tables(query_pos, ROPE_DIM)
    query_heads = query.reshape(query_rows, head_count, NOPE + ROPE_DIM)
    turned = rotate(
        query_heads[..., NOPE:].astype(jnp.float32), query_cos[:, None, :], query_sin[:, None, :]
    ).astype(jnp.bfloat16)
    query_rot = jnp.concatenate([query_heads[..., :NOPE], turned], axis=-1)
    last_query = query_start + query_rows - 1
    initial = (
        jnp.full((head_count, query_rows), masked_value, jnp.float32),
        jnp.zeros((head_count, query_rows), jnp.float32),
        jnp.zeros((head_count, query_rows, V_DIM), jnp.float32),
    )
    shard_rows = (
        lax.all_gather(normed, ("ep", "tp"), axis=0, tiled=True),
        lax.all_gather(rotated_key, ("ep", "tp"), axis=0, tiled=True),
    )

    def compute(state_in):
        key_part = jnp.dot(shard_rows[0], key_up, preferred_element_type=jnp.float32).astype(
            jnp.bfloat16
        )
        value_part = jnp.dot(shard_rows[0], value_up, preferred_element_type=jnp.float32).astype(
            jnp.bfloat16
        )
        return attend_block(state_in, query_rot, query_pos, key_part, value_part, shard_rows[1])

    running = lax.cond(jnp.int32(0) <= last_query, compute, keep_state, initial)
    totals = running[1]
    weighted = running[2]
    attention = (
        (weighted / totals[..., None])
        .transpose(1, 0, 2)
        .reshape(query_rows, head_count * V_DIM)
        .astype(jnp.bfloat16)
    )
    own_attention = lax.all_to_all(attention, "tp", split_axis=0, concat_axis=1, tiled=True)
    return jnp.dot(own_attention, out_proj, preferred_element_type=jnp.float32).astype(jnp.bfloat16)


def expert_half(tokens, moe_gain, routes, group_prob, expert_prob, w_gate, w_up, w_down):
    row_count, model_width = tokens.shape
    top_count = routes.shape[1]
    expert_count = lax.axis_size("ep")
    capacity = 2 * top_count * row_count // expert_count
    normed = rms_scale(tokens, moe_gain).astype(jnp.bfloat16)
    flat_routes = routes.reshape(-1)
    onehot = (flat_routes[:, None] == jnp.arange(expert_count, dtype=jnp.int32)[None, :]).astype(
        jnp.int32
    )
    earlier = jnp.cumsum(onehot, axis=0) - onehot
    slot_index = jnp.sum(earlier * onehot, axis=1)
    target = flat_routes * capacity + slot_index
    owner = target[None, :] == jnp.arange(expert_count * capacity, dtype=jnp.int32)[:, None]
    dispatch_table = jnp.any(
        owner.reshape(expert_count * capacity, row_count, top_count), axis=2
    ).astype(jnp.bfloat16)
    outgoing = jnp.dot(dispatch_table, normed, preferred_element_type=jnp.float32).astype(
        jnp.bfloat16
    )
    outgoing = outgoing.reshape(expert_count, capacity, model_width)
    arrived = lax.all_to_all(outgoing, "ep", split_axis=0, concat_axis=0, tiled=True)
    sources, slots, _ = arrived.shape
    flat_rows = arrived.reshape(sources * slots, model_width)
    shard_rows = lax.all_gather(flat_rows, "tp", axis=0, tiled=True)
    gate_values = jnp.dot(shard_rows, w_gate[0], preferred_element_type=jnp.float32)
    up_values = jnp.dot(shard_rows, w_up[0], preferred_element_type=jnp.float32)
    hidden = (jax.nn.silu(gate_values) * up_values).astype(jnp.bfloat16)

    def lower(offset, amount):
        return jnp.dot(hidden, w_down[0], preferred_element_type=jnp.float32)

    summed = lax.psum_scatter(
        lower(jnp.int32(0), sources * slots * lax.axis_size("tp")).astype(jnp.bfloat16),
        "tp",
        scatter_dimension=0,
        tiled=True,
    )
    result = summed.reshape(sources, slots, model_width)
    returned = lax.all_to_all(result, "ep", split_axis=0, concat_axis=0, tiled=True)
    returned_flat = returned.reshape(expert_count * capacity, model_width)
    picked = returned_flat[target].reshape(row_count, top_count, model_width).astype(jnp.float32)
    shares = group_prob[:, None] * expert_prob / jnp.sum(expert_prob, axis=1, keepdims=True)
    return jnp.sum(shares[:, :, None] * picked, axis=1).astype(jnp.bfloat16)


def body(
    query,
    latent,
    rope_key,
    latent_gain,
    key_up,
    value_up,
    out_proj,
    tokens,
    moe_gain,
    routes,
    group_prob,
    expert_prob,
    w_gate,
    w_up,
    w_down,
):
    mixed = mixer_half(query, latent, rope_key, latent_gain, key_up, value_up, out_proj)
    moe_out = expert_half(tokens, moe_gain, routes, group_prob, expert_prob, w_gate, w_up, w_down)
    return (mixed, moe_out)


def padded(amount):
    return -(-amount // 128) * 128


def send_kinds(depth):
    line = 2 * depth
    return (line, line, depth, depth, 1, 1, 1, 1, 1, 1, 1, 1, depth, 1, line, 2, 2, 3, 2, 2)


def recv_kinds(depth):
    line = 2 * depth
    units = (2 * depth,) * 3
    return (line, 0, depth, 0, *units, depth, *units, depth, depth, 1, line, 2, 2, 3, 2, 2)


def line_order(place, depth, spot):
    mirrored = depth - 1 - place
    from_low = (place + spot) % depth
    from_high = depth - 1 - (mirrored + spot) % depth
    return jnp.where(place < depth // 2, from_low, from_high)


def angle_tables(first_row, rows, lanes):
    half_width = ROPE_DIM // 2
    lane = lax.broadcasted_iota(jnp.int32, (rows, lanes), 1) % half_width
    position = first_row + lax.broadcasted_iota(jnp.int32, (rows, lanes), 0)
    inverse = jnp.exp(lane.astype(jnp.float32) * (-2.0 * math.log(rope_base) / ROPE_DIM))
    angles = position.astype(jnp.float32) * inverse
    return (jnp.cos(angles), jnp.sin(angles))


def turn_tables(rows, lanes, first):
    half_width = ROPE_DIM // 2
    row = lax.broadcasted_iota(jnp.int32, (rows, lanes), 0) - first
    lane = lax.broadcasted_iota(jnp.int32, (rows, lanes), 1)
    same = jnp.where((row == lane) & (lane < ROPE_DIM), 1.0, 0.0)
    lower = jnp.where((row == lane + half_width) & (lane < half_width), -1.0, 0.0)
    upper = jnp.where(
        (row == lane - half_width) & (lane >= half_width) & (lane < ROPE_DIM), 1.0, 0.0
    )
    return (same.astype(jnp.bfloat16), (lower + upper).astype(jnp.bfloat16))


def both_halves(
    heads,
    capacity,
    depth_z,
    tokens,
    moe_gain,
    routes,
    group_prob,
    expert_prob,
    latent,
    rope_key,
    latent_gain,
    query_hbm,
    key_up_hbm,
    value_up_hbm,
    out_proj_hbm,
    gate_hbm,
    up_hbm,
    down_hbm,
    mixed,
    moe_out,
    tok,
    info,
    away,
    arrived,
    lat_all,
    partial,
    from_pair,
    pair_sum,
    from_far,
    result,
    returned,
    joined,
    answers,
    passing,
    keys,
    values,
    query_big,
    heads_own,
    heads_all,
    query,
    key_up,
    value_up,
    out_proj,
    gate,
    up,
    down,
    load_sem,
    send_sem,
    recv_sem,
):
    row_count, width = tokens.shape
    own_rows, latent_width = latent.shape
    experts = 2 * depth_z
    units = 2 * depth_z
    n_tp = lat_all.shape[2]
    rope_room = lat_all.shape[-1] - latent_width
    bf16 = jnp.bfloat16
    f32 = jnp.float32
    me = lax.axis_index("ep")
    tp = lax.axis_index("tp")
    me_z = me // 2
    me_y = me % 2
    beside = me_z * 2 + 1 - me_y
    inner = (me_z > 0) & (me_z < depth_z - 1)
    inward = jnp.where(me_z < depth_z // 2, me_z + 1, me_z - 1)
    mate = tp + 1 - 2 * (tp % 2)
    far = (tp + 2) % n_tp
    cross = (mate + 2) % n_tp

    barrier = pltpu.get_barrier_semaphore()

    for step in (1, -1):

        @pl.when((me_z + step >= 0) & (me_z + step < depth_z))
        def _(step=step):
            pl.semaphore_signal(
                barrier,
                inc=1,
                device_id={"ep": (me_z + step) * 2 + me_y},
                device_id_type=pl.DeviceIdType.MESH,
            )

    pl.semaphore_signal(
        barrier, inc=1, device_id={"ep": beside}, device_id_type=pl.DeviceIdType.MESH
    )
    for peer in (mate, far, cross):
        pl.semaphore_signal(
            barrier, inc=1, device_id={"tp": peer}, device_id_type=pl.DeviceIdType.MESH
        )

    loads = [
        pltpu.make_async_copy(gate_hbm, gate, load_sem.at[0]),
        pltpu.make_async_copy(up_hbm, up, load_sem.at[1]),
        pltpu.make_async_copy(down_hbm, down, load_sem.at[2]),
        pltpu.make_async_copy(query_hbm, query, load_sem.at[3]),
        pltpu.make_async_copy(key_up_hbm, key_up, load_sem.at[4]),
        pltpu.make_async_copy(value_up_hbm, value_up, load_sem.at[5]),
        pltpu.make_async_copy(out_proj_hbm, out_proj, load_sem.at[6]),
    ]
    for load in loads:
        load.start()

    def remote(src, dst, sent, got, device):
        return pltpu.make_async_remote_copy(
            src_ref=src,
            dst_ref=dst,
            send_sem=send_sem.at[sum(send_kinds(depth_z)[: sent[0]]) + sent[1]],
            recv_sem=recv_sem.at[sum(recv_kinds(depth_z)[: got[0]]) + got[1]],
            device_id=device,
            device_id_type=pl.DeviceIdType.MESH,
        )

    def tok_step(origin, step, half):
        kind = 0 if step > 0 else 1
        target = {"ep": (me_z + step) * 2 + me_y}
        number = origin * 2 + half
        place = tok.at[origin, pl.ds(half * (row_count // 2), row_count // 2)]
        copies = [remote(place, place, (kind, number), (0, number), target)]
        if half == 0:
            place = info.at[origin]
            copies.append(remote(place, place, (kind + 2, origin), (2, origin), target))
        return copies

    def spread_tok(origin, step):
        inside = (me_z < depth_z - 1) if step > 0 else (me_z > 0)
        coming = (origin <= me_z) if step > 0 else (origin >= me_z)
        return inside & coming

    def source_of(unit):
        return line_order(me_z, depth_z, unit // 2) * 2 + (me_y + unit) % 2

    def hop_rows(kind, unit, block, peer):
        place = arrived.at[source_of(unit), block]
        return remote(place, place, (kind, 0), (kind, unit), {"tp": peer})

    def y_rows(spot):
        origin = line_order(me_z, depth_z, spot)
        return remote(
            away.at[origin],
            arrived.at[origin * 2 + me_y, tp],
            (7, 0),
            (7, spot),
            {"ep": beside},
        )

    def to_mate(kind, unit, block, part):
        source = source_of(unit)
        return remote(
            partial.at[source, block],
            from_pair.at[source, part],
            (kind, 0),
            (kind, unit),
            {"tp": mate},
        )

    def to_far(unit):
        source = source_of(unit)
        return remote(
            pair_sum.at[source], from_far.at[source], (10, 0), (10, unit), {"tp": far}
        )

    def y_back(spot):
        origin = line_order(me_z, depth_z, spot)
        return remote(
            result.at[origin * 2 + 1 - me_y],
            returned.at[origin],
            (11, 0),
            (11, spot),
            {"ep": beside},
        )

    def z_back(origin, sender):
        return remote(
            joined.at[origin],
            answers.at[sender],
            (12, origin),
            (12, sender),
            {"ep": origin * 2 + me_y},
        )

    def z_pass(half):
        rows = pl.ds(half * (row_count // 2), row_count // 2)
        return remote(
            joined.at[line_order(me_z, depth_z, 2), rows],
            passing.at[rows],
            (18, half),
            (18, half),
            {"ep": inward * 2 + me_y},
        )

    def z_half(origin, sender, half):
        rows = pl.ds(half * (row_count // 2), row_count // 2)
        return remote(
            joined.at[origin, rows],
            answers.at[sender, rows],
            (19, half),
            (19, half),
            {"ep": origin * 2 + me_y},
        )

    def lat_x(block):
        place = lat_all.at[me_z, me_y, block]
        return remote(place, place, (13, 0), (13, 0), {"tp": far})

    def lat_up(origin):
        copies = []
        for part in range(2):
            place = lat_all.at[origin, :, (tp + 2 * part) % n_tp]
            number = (14, origin * 2 + part)
            copies.append(remote(place, place, number, number, {"ep": (me_z + 1) * 2 + me_y}))
        return copies

    def lat_y(part, side):
        place = lat_all.at[me_z, side, (tp + 2 * part) % n_tp]
        return remote(place, place, (15, part), (15, part), {"ep": beside})

    def lat_mate(part, first):
        place = lat_all.at[:, :, (first + 2 * part) % n_tp]
        return remote(place, place, (16, part), (16, part), {"tp": mate})

    def head_copy(number, peer, slot):
        return remote(
            heads_own.at[peer], heads_all.at[slot], (17, number), (17, number), {"tp": peer}
        )

    first_route = routes[0:1, :]
    second_route = routes[1:2, :]
    lane_expert = lax.broadcasted_iota(jnp.int32, (experts, row_count), 0)
    is_first = lane_expert == first_route
    is_second = lane_expert == second_route
    named = jnp.where(is_first | is_second, 1.0, 0.0).astype(bf16)
    ahead = lax.broadcasted_iota(jnp.int32, (row_count, row_count), 0)
    behind = lax.broadcasted_iota(jnp.int32, (row_count, row_count), 1)
    before = jnp.where(ahead < behind, 1.0, 0.0).astype(bf16)
    earlier = jnp.dot(named, before, preferred_element_type=f32)
    first_slot = jnp.sum(jnp.where(is_first, earlier, 0.0), axis=0, keepdims=True)
    second_slot = jnp.sum(jnp.where(is_second, earlier, 0.0), axis=0, keepdims=True)
    both_prob = expert_prob[0:1, :] + expert_prob[1:2, :]
    info[me_z] = jnp.full(info.shape[1:], -1.0, f32)
    info[me_z, 0:1, 0:row_count] = first_route.astype(f32) * capacity + first_slot
    info[me_z, 1:2, 0:row_count] = second_route.astype(f32) * capacity + second_slot
    info[me_z, 2:3, 0:row_count] = group_prob[...] * expert_prob[0:1, :] / both_prob
    info[me_z, 3:4, 0:row_count] = group_prob[...] * expert_prob[1:2, :] / both_prob
    tok[me_z] = rms_scale(tokens[...], moe_gain[...]).astype(bf16)

    pl.semaphore_wait(barrier, jnp.where(inner, 6, 5))

    for step in (1, -1):

        @pl.when(spread_tok(me_z, step))
        def _(step=step):
            for half in range(2):
                for copy in tok_step(me_z, step, half):
                    copy.start()

    def wanted():
        row = lax.broadcasted_iota(jnp.int32, (2 * capacity, info.shape[2]), 0)
        own = me * capacity + row
        other = (beside - 1) * capacity + row
        return jnp.where(row < capacity, own, other).astype(f32)

    def take_tok(spot, half):
        origin = line_order(me_z, depth_z, spot)
        for copy in tok_step(origin, 1, half):
            copy.wait_recv()
        for step in (1, -1):

            @pl.when(spread_tok(origin, step))
            def _(step=step):
                for copy in tok_step(origin, step, half):
                    copy.start()

    def raise_lat(origin):
        @pl.when(spread_tok(origin, 1))
        def _():
            for copy in lat_up(origin):
                copy.start()

    def take_lat(below):
        @pl.when(me_z >= below)
        def _():
            for copy in lat_up(me_z - below):
                copy.wait_recv()
            raise_lat(me_z - below)

    def gather_spot(spot):
        origin = line_order(me_z, depth_z, spot)

        @pl.when((spot > 0) & jnp.logical_not(inner))
        def _():
            take_tok(spot, 0)
            take_tok(spot, 1)

        want = wanted()
        table = jnp.where(
            (want == info[origin, 0:1, :]) | (want == info[origin, 1:2, :]), 1.0, 0.0
        )
        packed = jnp.dot(
            table[:, :row_count].astype(bf16), tok[origin], preferred_element_type=f32
        ).astype(bf16)
        arrived[origin * 2 + me_y, tp] = packed[:capacity]
        away[origin] = packed[capacity:]
        y_rows(spot).start()

    def forward(unit):
        spot = unit // 2

        @pl.when(unit % 2 == 0)
        def _():
            gather_spot(spot)

        @pl.when(unit % 2 == 1)
        def _():
            y_rows(spot).wait_recv()

        hop_rows(4, unit, tp, far).start()
        hop_rows(5, unit, tp, mate).start()

    def relay(unit):
        hop_rows(4, unit, far, far).wait_recv()
        hop_rows(6, unit, far, mate).start()

    def compute(unit):
        source = source_of(unit)
        hop_rows(5, unit, mate, mate).wait_recv()
        hop_rows(6, unit, cross, mate).wait_recv()

        @pl.when(unit == 0)
        def _():
            for load in loads[:3]:
                load.wait()

        rows = arrived[source].reshape(n_tp * capacity, width)
        gate_values = jnp.dot(rows, gate[...], preferred_element_type=f32)
        up_values = jnp.dot(rows, up[...], preferred_element_type=f32)
        hidden = (gate_values / (1.0 + jnp.exp(-gate_values)) * up_values).astype(bf16)
        product = jnp.dot(hidden, down[...], preferred_element_type=f32)
        partial[source] = product.astype(bf16).reshape(n_tp, capacity, width)
        to_mate(9, unit, cross, 1).start()
        to_mate(8, unit, mate, 0).start()

    def reduce_pair(unit):
        source = source_of(unit)
        to_mate(9, unit, cross, 1).wait_recv()
        pair_sum[source] = (
            partial[source, far].astype(f32) + from_pair[source, 1].astype(f32)
        ).astype(bf16)

    def reduce_far(unit):
        source = source_of(unit)
        to_mate(8, unit, mate, 0).wait_recv()
        to_far(unit).wait_recv()
        result[source] = (
            partial[source, tp].astype(f32)
            + from_pair[source, 0].astype(f32)
            + from_far[source].astype(f32)
        ).astype(bf16)

        @pl.when(unit % 2 == 1)
        def _():
            y_back(unit // 2).start()

    def weighted(spot):
        origin = line_order(me_z, depth_z, spot)
        y_back(spot).wait_recv()
        want = wanted()
        weights = jnp.where(want == info[origin, 0:1, :], info[origin, 2:3, :], 0.0) + jnp.where(
            want == info[origin, 1:2, :], info[origin, 3:4, :], 0.0
        )
        weights = weights[:, :row_count]
        high = weights.astype(bf16)
        low = (weights - high.astype(f32)).astype(bf16)
        rows = jnp.concatenate([result[origin * 2 + me_y], returned[origin]], axis=0)
        over_slots = (((0,), (0,)), ((), ()))
        return lax.dot_general(
            high, rows, over_slots, preferred_element_type=f32
        ) + lax.dot_general(low, rows, over_slots, preferred_element_type=f32)

    def join(spot):
        origin = line_order(me_z, depth_z, spot)
        joined[origin] = weighted(spot).astype(bf16)
        z_back(origin, me_z).start()

    def join_pass():
        origin = line_order(me_z, depth_z, 2)
        joined[origin] = weighted(2).astype(bf16)
        for half in range(2):
            z_pass(half).start()

    def join_passed():
        origin = line_order(me_z, depth_z, 1)
        own = weighted(1)
        for half in range(2):
            first = half * (row_count // 2)
            rows = pl.ds(first, row_count // 2)
            z_pass(half).wait_recv()
            part = own[first : first + row_count // 2]
            joined[origin, rows] = (part + passing[rows].astype(f32)).astype(bf16)
            z_half(origin, me_z, half).start()

    def own_latent():
        same, swapped = turn_tables(ROPE_DIM, rope_room, 0)
        first_row = (me * n_tp + tp) * own_rows
        cosine, sine = angle_tables(first_row, own_rows, rope_room)
        turned = jnp.dot(rope_key[...], same, preferred_element_type=f32) * cosine + (
            jnp.dot(rope_key[...], swapped, preferred_element_type=f32) * sine
        )
        lat_all[me_z, me_y, tp, :, :latent_width] = rms_scale(
            latent[...], latent_gain[...]
        ).astype(bf16)
        lat_all[me_z, me_y, tp, :, latent_width:] = turned.astype(bf16)
        lat_x(tp).start()

    def spread_query():
        loads[3].wait()
        rows, packed_width = query.shape
        head_width = packed_width // heads
        nope_width = heads * NOPE
        cosine, sine = angle_tables(me * rows, rows, rope_room)
        row = lax.broadcasted_iota(jnp.int32, (packed_width, nope_width), 0)
        lane = lax.broadcasted_iota(jnp.int32, (packed_width, nope_width), 1)
        out_lane = lax.broadcasted_iota(jnp.int32, (rows, nope_width), 1)
        plain = jnp.zeros((packed_width, nope_width), f32)
        for head in range(heads):
            inside = (lane >= head * NOPE) & (lane < (head + 1) * NOPE)
            plain = jnp.where(inside & (row - lane == head * ROPE_DIM), 1.0, plain)
        nope = jnp.dot(query[...], plain.astype(bf16), preferred_element_type=f32)
        for head in range(heads):
            inside = (out_lane >= head * NOPE) & (out_lane < (head + 1) * NOPE)
            query_big[head, :, :nope_width] = jnp.where(inside, nope, 0.0).astype(bf16)
            same, swapped = turn_tables(packed_width, rope_room, head * head_width + NOPE)
            turned = jnp.dot(query[...], same, preferred_element_type=f32) * cosine + (
                jnp.dot(query[...], swapped, preferred_element_type=f32) * sine
            )
            query_big[head, :, nope_width:] = turned.astype(bf16)

    def fill_keys():
        nope_width = key_up.shape[1]
        packed = lat_all[...].reshape(-1, lat_all.shape[-1])
        normed = packed[:, :latent_width]
        loads[4].wait()
        loads[5].wait()
        keys[:, :nope_width] = jnp.dot(normed, key_up[...], preferred_element_type=f32).astype(bf16)
        keys[:, nope_width:] = packed[:, latent_width:]
        values[...] = jnp.dot(normed, value_up[...], preferred_element_type=f32).astype(bf16)

    def attend(first_head, last_head):
        rows = query_big.shape[1]
        seq = keys.shape[0]
        value_width = values.shape[1] // heads
        query_pos = me * rows + lax.broadcasted_iota(jnp.int32, (rows, seq), 0)
        allowed = lax.broadcasted_iota(jnp.int32, (rows, seq), 1) <= query_pos
        lane = lax.broadcasted_iota(jnp.int32, (rows, heads * value_width), 1)
        scale = (NOPE + ROPE_DIM) ** (-0.5)
        gathered = jnp.zeros((rows, heads * value_width), f32)
        if first_head > 0:
            gathered = heads_own[...].reshape(rows, -1).astype(f32)
        for head in range(first_head, last_head):
            scores = (
                lax.dot_general(
                    query_big[head],
                    keys[...],
                    (((1,), (1,)), ((), ())),
                    preferred_element_type=f32,
                )
                * scale
            )
            scores = jnp.where(allowed, scores, masked_value)
            raised = jnp.exp(scores - jnp.max(scores, axis=1, keepdims=True))
            totals = jnp.sum(raised, axis=1, keepdims=True)
            summed = jnp.dot(raised.astype(bf16), values[...], preferred_element_type=f32)
            inside = (lane >= head * value_width) & (lane < (head + 1) * value_width)
            gathered = jnp.where(inside, summed / totals, gathered)
        heads_own[...] = gathered.astype(bf16).reshape(heads_own.shape)

    peers = (mate, far, cross)

    @pl.when(inner)
    def _():
        answers[line_order(me_z, depth_z, 2)] = jnp.zeros(answers.shape[1:], bf16)

    def clear(above, carry):
        @pl.when(me_z + above < depth_z)
        def _():
            lat_all[me_z + above] = jnp.zeros(lat_all.shape[1:], bf16)

        return carry

    def stage(turn, carry):
        @pl.when((turn == 2) & inner)
        def _():
            take_tok(1, 1)
            take_tok(3, 1)

        @pl.when((turn == 4) & inner)
        def _():
            take_tok(2, 1)

        forward(turn)

        @pl.when((turn == 1) & inner)
        def _():
            take_tok(1, 0)
            take_tok(3, 0)

        @pl.when((turn == 3) & inner)
        def _():
            take_tok(2, 0)

        @pl.when(turn == 0)
        def _():
            own_latent()
            lax.fori_loop(1, depth_z, clear, 0)

        @pl.when(turn == 2)
        def _():
            lat_x(far).wait_recv()
            lat_y(0, me_y).start()
            lat_y(1, me_y).start()

        @pl.when(turn == 4)
        def _():
            lat_y(0, 1 - me_y).wait_recv()
            lat_y(1, 1 - me_y).wait_recv()
            raise_lat(me_z)

        @pl.when(turn == 6)
        def _():
            take_lat(1)

        @pl.when(turn >= 3)
        def _():
            reduce_pair(turn - 3)

        @pl.when(turn >= 2)
        def _():
            compute(turn - 2)

        @pl.when(turn >= 1)
        def _():
            relay(turn - 1)

        @pl.when(turn == 2)
        def _():
            spread_query()

        return carry

    lax.fori_loop(0, units - 1, stage, 0)

    reduce_pair(4)
    to_far(4).start()
    take_lat(2)
    compute(5)
    relay(6)
    reduce_pair(5)
    to_far(5).start()
    forward(7)
    to_far(3).start()
    to_far(2).start()
    compute(6)
    reduce_far(4)
    reduce_pair(6)
    take_lat(3)
    lat_mate(0, tp).start()
    lat_mate(1, tp).start()
    reduce_far(5)
    lat_mate(0, mate).wait_recv()
    lat_mate(1, mate).wait_recv()
    fill_keys()
    relay(7)

    @pl.when(inner)
    def _():
        join(2)

    @pl.when(jnp.logical_not(inner))
    def _():
        join_pass()

    compute(7)
    reduce_pair(7)
    to_far(7).start()
    to_far(6).start()
    reduce_far(3)
    attend(0, heads // 2)
    reduce_far(2)
    attend(heads // 2, heads)
    for number, peer in enumerate(peers):
        head_copy(number, peer, tp).start()
    to_far(1).start()
    to_far(0).start()
    heads_all[tp] = heads_own[tp]
    reduce_far(7)

    @pl.when(inner)
    def _():
        join_passed()

    @pl.when(jnp.logical_not(inner))
    def _():
        join(1)

    reduce_far(6)
    join(3)
    reduce_far(1)
    loads[6].wait()
    for number, peer in enumerate(peers):
        head_copy(number, peer, peer).wait_recv()
    depth = heads_all.shape[2]
    total = jnp.zeros(mixed.shape, f32)
    for part in range(n_tp):
        total = total + jnp.dot(
            heads_all[part],
            out_proj[part * depth : (part + 1) * depth, :],
            preferred_element_type=f32,
        )
    mixed[...] = total.astype(mixed.dtype)
    reduce_far(0)
    chosen = weighted(0)

    def finish_line(origin, carry):
        for step in (1, -1):

            @pl.when(spread_tok(origin, step))
            def _(step=step):
                for copy in (*tok_step(origin, step, 0), *tok_step(origin, step, 1)):
                    copy.wait_send()

        @pl.when(spread_tok(origin, 1))
        def _():
            for copy in lat_up(origin):
                copy.wait_send()

        halved = jnp.where(inner, line_order(me_z, depth_z, 1), line_order(me_z, depth_z, 2))

        @pl.when((origin != me_z) & (origin != halved))
        def _():
            z_back(origin, me_z).wait_send()

        return carry

    lax.fori_loop(0, depth_z, finish_line, 0)

    @pl.when(jnp.logical_not(inner))
    def _():
        for half in range(2):
            z_pass(half).wait_send()

    @pl.when(inner)
    def _():
        for half in range(2):
            z_half(line_order(me_z, depth_z, 1), me_z, half).wait_send()

    lat_x(tp).wait_send()
    for part in range(2):
        lat_y(part, me_y).wait_send()
        lat_mate(part, tp).wait_send()
    for number, peer in enumerate(peers):
        head_copy(number, peer, tp).wait_send()

    def all_sent(kind, src, device):
        remote(src, src, (kind, 0), (4, 0), device).wait_send()

    all_sent(4, arrived.at[:, tp], {"tp": far})
    all_sent(5, arrived.at[:, tp], {"tp": mate})
    all_sent(6, arrived.at[:, far], {"tp": mate})
    all_sent(7, away, {"ep": beside})
    all_sent(8, partial.at[:, mate], {"tp": mate})
    all_sent(9, partial.at[:, cross], {"tp": mate})
    all_sent(10, pair_sum, {"tp": far})
    all_sent(11, returned, {"ep": beside})

    for shift in range(1, depth_z):
        sender = (me_z + shift) % depth_z

        near = line_order(me_z, depth_z, 1)
        none = line_order(me_z, depth_z, 2)

        @pl.when(jnp.logical_not(inner & ((sender == none) | (sender == near))))
        def _(sender=sender):
            z_back(me_z, sender).wait_recv()

        @pl.when(inner & (sender == near))
        def _(sender=sender):
            for half in range(2):
                z_half(me_z, sender, half).wait_recv()

        chosen = chosen + answers[sender].astype(f32)
    moe_out[...] = chosen.astype(moe_out.dtype)


def hand_over(mixed_in, moe_in, mixed_out, moe_out, sem):
    copies = [
        pltpu.make_async_copy(mixed_in, mixed_out, sem.at[0]),
        pltpu.make_async_copy(moe_in, moe_out, sem.at[1]),
    ]
    for copy in copies:
        copy.start()
    for copy in copies:
        copy.wait()


def fused_body(
    query,
    latent,
    rope_key,
    latent_gain,
    key_up,
    value_up,
    out_proj,
    tokens,
    moe_gain,
    routes,
    group_prob,
    expert_prob,
    w_gate,
    w_up,
    w_down,
):
    n_ep = lax.axis_size("ep")
    n_tp = lax.axis_size("tp")
    depth_z = n_ep // 2
    query_rows = query.shape[0]
    own_rows, latent_width = latent.shape
    heads = query.shape[1] // (NOPE + ROPE_DIM)
    rope_room = padded(ROPE_DIM)
    row_count, width = tokens.shape
    capacity = 2 * routes.shape[1] * row_count // n_ep
    bf16 = jnp.bfloat16
    lat_width = latent_width + rope_room
    key_width = key_up.shape[1] + rope_room
    vmem = pl.BlockSpec(memory_space=pltpu.VMEM)
    anywhere = pl.BlockSpec(memory_space=pl.ANY)
    results = pl.pallas_call(
        functools.partial(both_halves, heads, capacity, depth_z),
        out_shape=(
            pltpu.VMEM((own_rows, out_proj.shape[1]), bf16),
            pltpu.VMEM((row_count, width), bf16),
        ),
        in_specs=[vmem] * 8 + [anywhere] * 7,
        out_specs=(vmem, vmem),
        scratch_shapes=[
            pltpu.VMEM((depth_z, row_count, width), bf16),
            pltpu.VMEM((depth_z, 8, padded(row_count)), jnp.float32),
            pltpu.VMEM((depth_z, capacity, width), bf16),
            pltpu.VMEM((n_ep, n_tp, capacity, width), bf16),
            pltpu.VMEM((depth_z, 2, n_tp, own_rows, lat_width), bf16),
            pltpu.VMEM((n_ep, n_tp, capacity, width), bf16),
            pltpu.VMEM((n_ep, 2, capacity, width), bf16),
            pltpu.VMEM((n_ep, capacity, width), bf16),
            pltpu.VMEM((n_ep, capacity, width), bf16),
            pltpu.VMEM((n_ep, capacity, width), bf16),
            pltpu.VMEM((depth_z, capacity, width), bf16),
            pltpu.VMEM((depth_z, row_count, width), bf16),
            pltpu.VMEM((depth_z, row_count, width), bf16),
            pltpu.VMEM((row_count, width), bf16),
            pltpu.VMEM((n_ep * n_tp * own_rows, key_width), bf16),
            pltpu.VMEM((n_ep * n_tp * own_rows, value_up.shape[1]), bf16),
            pltpu.VMEM((heads, query_rows, key_width), bf16),
            pltpu.VMEM((n_tp, own_rows, value_up.shape[1]), bf16),
            pltpu.VMEM((n_tp, own_rows, value_up.shape[1]), bf16),
            pltpu.VMEM(query.shape, bf16),
            pltpu.VMEM(key_up.shape, bf16),
            pltpu.VMEM(value_up.shape, bf16),
            pltpu.VMEM(out_proj.shape, bf16),
            pltpu.VMEM(w_gate.shape[1:], bf16),
            pltpu.VMEM(w_up.shape[1:], bf16),
            pltpu.VMEM(w_down.shape[1:], bf16),
            pltpu.SemaphoreType.DMA((7,)),
            pltpu.SemaphoreType.DMA((sum(send_kinds(depth_z)),)),
            pltpu.SemaphoreType.DMA((sum(recv_kinds(depth_z)),)),
        ],
        compiler_params=pltpu.CompilerParams(
            collective_id=0, has_side_effects=True, vmem_limit_bytes=60 * 1024 * 1024
        ),
        name="both_halves",
    )(
        tokens,
        moe_gain.reshape(1, -1),
        routes.T,
        group_prob.reshape(1, -1),
        expert_prob.T,
        latent,
        rope_key,
        latent_gain.reshape(1, -1),
        query,
        key_up,
        value_up,
        out_proj,
        w_gate[0],
        w_up[0],
        w_down[0],
    )
    return pl.pallas_call(
        hand_over,
        out_shape=tuple(jax.ShapeDtypeStruct(part.shape, part.dtype) for part in results),
        in_specs=[vmem] * 2,
        out_specs=(anywhere, anywhere),
        scratch_shapes=[pltpu.SemaphoreType.DMA((2,))],
        compiler_params=pltpu.CompilerParams(vmem_limit_bytes=4 * 1024 * 1024),
        name="hand_over",
    )(*results)


def fits_kernel(mesh, *arrays):
    n_ep, n_tp = mesh.shape["ep"], mesh.shape["tp"]
    tokens, routes, latent = arrays[7], arrays[9], arrays[1]
    row_count = tokens.shape[0] // (n_ep * n_tp)
    capacity = 2 * routes.shape[1] * row_count // n_ep
    own_rows = latent.shape[0] // (n_ep * n_tp)
    shaped = n_tp == 4 and n_ep == 8 and routes.shape[1] == 2
    aligned = capacity % 16 == 0 and own_rows % 16 == 0 and row_count % 16 == 0
    return shaped and aligned and latent.shape[0] <= 2048


def mapped(mesh, chosen):
    return jax.shard_map(
        chosen,
        mesh=mesh,
        in_specs=(
            P("ep", "tp"),
            P(("ep", "tp"), None),
            P(("ep", "tp"), None),
            P(),
            P(None, "tp"),
            P(None, "tp"),
            P(),
            P(("ep", "tp"), None),
            P(),
            P(("ep", "tp"), None),
            P(("ep", "tp")),
            P(("ep", "tp"), None),
            P("ep", None, "tp"),
            P("ep", None, "tp"),
            P("ep", "tp", None),
        ),
        out_specs=(P(("ep", "tp"), None), P(("ep", "tp"), None)),
        check_vma=False,
    )


def solution(mesh):
    def whole(*arrays):
        chosen = fused_body if fits_kernel(mesh, *arrays) else body
        return mapped(mesh, chosen)(*arrays)

    return whole
```

```python
import functools
import math

import jax
import jax.numpy as jnp
from jax import lax
from jax.experimental import pallas as pl
from jax.experimental.pallas import tpu as pltpu
from jax.sharding import PartitionSpec as P

NOPE = 64
ROPE_DIM = 32
V_DIM = 64


epsilon = 1e-06
rope_base = 10000.0
masked_value = -1e30


def rms_scale(values, gain):
    widened = values.astype(jnp.float32)
    return widened * lax.rsqrt(jnp.mean(widened * widened, axis=-1, keepdims=True) + epsilon) * gain


def tables(positions, rope_width):
    half_width = rope_width // 2
    inverse = rope_base ** (-2.0 * jnp.arange(half_width, dtype=jnp.float32) / rope_width)
    angles = positions.astype(jnp.float32)[:, None] * inverse[None, :]
    return (jnp.cos(angles), jnp.sin(angles))


def rotate(values, cosine, sine):
    half_width = values.shape[-1] // 2
    lower = values[..., :half_width]
    upper = values[..., half_width:]
    return jnp.concatenate([lower * cosine - upper * sine, lower * sine + upper * cosine], axis=-1)


def keep_state(state_in):
    return state_in


def attend_block(running, query_rot, query_pos, key_part, value_part, rope_part):
    amount = key_part.shape[0]
    span_rows = math.gcd(amount, 1024)
    head_count = query_rot.shape[1]
    scale_factor = query_rot.shape[2] ** (-0.5)
    last_query = query_pos[-1]

    def update(state, block_at):
        row_begin = block_at * span_rows
        keys_here = lax.dynamic_slice_in_dim(key_part, row_begin, span_rows, 0).reshape(
            span_rows, head_count, -1
        )
        values_here = lax.dynamic_slice_in_dim(value_part, row_begin, span_rows, 0).reshape(
            span_rows, head_count, -1
        )
        rope_here = lax.dynamic_slice_in_dim(rope_part, row_begin, span_rows, 0)
        key_pos = row_begin + jnp.arange(span_rows, dtype=jnp.int32)

        def advance(state_in):
            top_old, totals, weighted = state_in
            shared = jnp.broadcast_to(
                rope_here[:, None, :], (span_rows, head_count, rope_here.shape[1])
            )
            full_keys = jnp.concatenate([keys_here, shared], axis=-1)
            scores = (
                jnp.einsum("qhd,khd->hqk", query_rot, full_keys, preferred_element_type=jnp.float32)
                * scale_factor
            )
            allowed = key_pos[None, :] <= query_pos[:, None]
            scores = jnp.where(allowed[None], scores, masked_value)
            top_new = jnp.maximum(top_old, jnp.max(scores, axis=-1))
            raised = jnp.where(allowed[None], jnp.exp(scores - top_new[..., None]), 0.0)
            factor = jnp.exp(top_old - top_new)
            totals = totals * factor + jnp.sum(raised, axis=-1)
            weighted = weighted * factor[..., None] + jnp.einsum(
                "hqk,khd->hqd",
                raised.astype(jnp.bfloat16),
                values_here,
                preferred_element_type=jnp.float32,
            )
            return (top_new, totals, weighted)

        return (lax.cond(key_pos[0] <= last_query, advance, keep_state, state), None)

    running, _ = lax.scan(update, running, jnp.arange(amount // span_rows))
    return running


def mixer_half(query, latent, rope_key, latent_gain, key_up, value_up, out_proj):
    query_rows = query.shape[0]
    own_rows = latent.shape[0]
    query_start = lax.axis_index("ep") * query_rows
    key_start = query_start + lax.axis_index("tp") * own_rows
    head_count = query.shape[1] // (NOPE + ROPE_DIM)
    normed = rms_scale(latent, latent_gain).astype(jnp.bfloat16)
    key_cos, key_sin = tables(key_start + jnp.arange(own_rows, dtype=jnp.int32), ROPE_DIM)
    rotated_key = rotate(rope_key.astype(jnp.float32), key_cos, key_sin).astype(jnp.bfloat16)
    query_pos = query_start + jnp.arange(query_rows, dtype=jnp.int32)
    query_cos, query_sin = tables(query_pos, ROPE_DIM)
    query_heads = query.reshape(query_rows, head_count, NOPE + ROPE_DIM)
    turned = rotate(
        query_heads[..., NOPE:].astype(jnp.float32), query_cos[:, None, :], query_sin[:, None, :]
    ).astype(jnp.bfloat16)
    query_rot = jnp.concatenate([query_heads[..., :NOPE], turned], axis=-1)
    last_query = query_start + query_rows - 1
    initial = (
        jnp.full((head_count, query_rows), masked_value, jnp.float32),
        jnp.zeros((head_count, query_rows), jnp.float32),
        jnp.zeros((head_count, query_rows, V_DIM), jnp.float32),
    )
    shard_rows = (
        lax.all_gather(normed, ("ep", "tp"), axis=0, tiled=True),
        lax.all_gather(rotated_key, ("ep", "tp"), axis=0, tiled=True),
    )

    def compute(state_in):
        key_part = jnp.dot(shard_rows[0], key_up, preferred_element_type=jnp.float32).astype(
            jnp.bfloat16
        )
        value_part = jnp.dot(shard_rows[0], value_up, preferred_element_type=jnp.float32).astype(
            jnp.bfloat16
        )
        return attend_block(state_in, query_rot, query_pos, key_part, value_part, shard_rows[1])

    running = lax.cond(jnp.int32(0) <= last_query, compute, keep_state, initial)
    totals = running[1]
    weighted = running[2]
    attention = (
        (weighted / totals[..., None])
        .transpose(1, 0, 2)
        .reshape(query_rows, head_count * V_DIM)
        .astype(jnp.bfloat16)
    )
    own_attention = lax.all_to_all(attention, "tp", split_axis=0, concat_axis=1, tiled=True)
    return jnp.dot(own_attention, out_proj, preferred_element_type=jnp.float32).astype(jnp.bfloat16)


def expert_half(tokens, moe_gain, routes, group_prob, expert_prob, w_gate, w_up, w_down):
    row_count, model_width = tokens.shape
    top_count = routes.shape[1]
    expert_count = lax.axis_size("ep")
    capacity = 2 * top_count * row_count // expert_count
    normed = rms_scale(tokens, moe_gain).astype(jnp.bfloat16)
    flat_routes = routes.reshape(-1)
    onehot = (flat_routes[:, None] == jnp.arange(expert_count, dtype=jnp.int32)[None, :]).astype(
        jnp.int32
    )
    earlier = jnp.cumsum(onehot, axis=0) - onehot
    slot_index = jnp.sum(earlier * onehot, axis=1)
    target = flat_routes * capacity + slot_index
    owner = target[None, :] == jnp.arange(expert_count * capacity, dtype=jnp.int32)[:, None]
    dispatch_table = jnp.any(
        owner.reshape(expert_count * capacity, row_count, top_count), axis=2
    ).astype(jnp.bfloat16)
    outgoing = jnp.dot(dispatch_table, normed, preferred_element_type=jnp.float32).astype(
        jnp.bfloat16
    )
    outgoing = outgoing.reshape(expert_count, capacity, model_width)
    arrived = lax.all_to_all(outgoing, "ep", split_axis=0, concat_axis=0, tiled=True)
    sources, slots, _ = arrived.shape
    flat_rows = arrived.reshape(sources * slots, model_width)
    shard_rows = lax.all_gather(flat_rows, "tp", axis=0, tiled=True)
    gate_values = jnp.dot(shard_rows, w_gate[0], preferred_element_type=jnp.float32)
    up_values = jnp.dot(shard_rows, w_up[0], preferred_element_type=jnp.float32)
    hidden = (jax.nn.silu(gate_values) * up_values).astype(jnp.bfloat16)

    def lower(offset, amount):
        return jnp.dot(hidden, w_down[0], preferred_element_type=jnp.float32)

    summed = lax.psum_scatter(
        lower(jnp.int32(0), sources * slots * lax.axis_size("tp")).astype(jnp.bfloat16),
        "tp",
        scatter_dimension=0,
        tiled=True,
    )
    result = summed.reshape(sources, slots, model_width)
    returned = lax.all_to_all(result, "ep", split_axis=0, concat_axis=0, tiled=True)
    returned_flat = returned.reshape(expert_count * capacity, model_width)
    picked = returned_flat[target].reshape(row_count, top_count, model_width).astype(jnp.float32)
    shares = group_prob[:, None] * expert_prob / jnp.sum(expert_prob, axis=1, keepdims=True)
    return jnp.sum(shares[:, :, None] * picked, axis=1).astype(jnp.bfloat16)


def body(
    query,
    latent,
    rope_key,
    latent_gain,
    key_up,
    value_up,
    out_proj,
    tokens,
    moe_gain,
    routes,
    group_prob,
    expert_prob,
    w_gate,
    w_up,
    w_down,
):
    mixed = mixer_half(query, latent, rope_key, latent_gain, key_up, value_up, out_proj)
    moe_out = expert_half(tokens, moe_gain, routes, group_prob, expert_prob, w_gate, w_up, w_down)
    return (mixed, moe_out)


def padded(amount):
    return -(-amount // 128) * 128


def send_kinds(depth):
    line = 2 * depth
    return (line, line, depth, depth, 1, 1, 1, 1, 1, 1, 1, 1, line, 1, line, 2, 2, 3, 2)


def recv_kinds(depth):
    line = 2 * depth
    wide = 2 * line
    gather = (wide, line, line, line, line, line, wide)
    return (line, 0, depth, 0, *gather, line, line, 1, line, 2, 2, 3, 2)


def line_order(place, depth, spot):
    mirrored = depth - 1 - place
    from_low = (place + spot) % depth
    from_high = depth - 1 - (mirrored + spot) % depth
    return jnp.where(place < depth // 2, from_low, from_high)


def angle_tables(first_row, rows, lanes):
    half_width = ROPE_DIM // 2
    lane = lax.broadcasted_iota(jnp.int32, (rows, lanes), 1) % half_width
    position = first_row + lax.broadcasted_iota(jnp.int32, (rows, lanes), 0)
    inverse = jnp.exp(lane.astype(jnp.float32) * (-2.0 * math.log(rope_base) / ROPE_DIM))
    angles = position.astype(jnp.float32) * inverse
    return (jnp.cos(angles), jnp.sin(angles))


def turn_tables(rows, lanes, first):
    half_width = ROPE_DIM // 2
    row = lax.broadcasted_iota(jnp.int32, (rows, lanes), 0) - first
    lane = lax.broadcasted_iota(jnp.int32, (rows, lanes), 1)
    same = jnp.where((row == lane) & (lane < ROPE_DIM), 1.0, 0.0)
    lower = jnp.where((row == lane + half_width) & (lane < half_width), -1.0, 0.0)
    upper = jnp.where(
        (row == lane - half_width) & (lane >= half_width) & (lane < ROPE_DIM), 1.0, 0.0
    )
    return (same.astype(jnp.bfloat16), (lower + upper).astype(jnp.bfloat16))


def both_halves(
    heads,
    capacity,
    depth_z,
    tokens,
    moe_gain,
    routes,
    group_prob,
    expert_prob,
    latent,
    rope_key,
    latent_gain,
    query_hbm,
    key_up_hbm,
    value_up_hbm,
    out_proj_hbm,
    gate_hbm,
    up_hbm,
    down_hbm,
    mixed,
    moe_out,
    tok,
    info,
    away,
    arrived,
    lat_all,
    partial,
    from_pair,
    pair_sum,
    from_far,
    result,
    returned,
    joined,
    answers,
    passing,
    keys,
    values,
    query_big,
    heads_own,
    heads_all,
    query,
    key_up,
    value_up,
    out_proj,
    gate,
    up,
    down,
    load_sem,
    send_sem,
    recv_sem,
):
    row_count, width = tokens.shape
    own_rows, latent_width = latent.shape
    experts = 2 * depth_z
    units = 2 * depth_z
    n_tp = lat_all.shape[2]
    rope_room = lat_all.shape[-1] - latent_width
    bf16 = jnp.bfloat16
    f32 = jnp.float32
    me = lax.axis_index("ep")
    tp = lax.axis_index("tp")
    me_z = me // 2
    me_y = me % 2
    beside = me_z * 2 + 1 - me_y
    inner = (me_z > 0) & (me_z < depth_z - 1)
    inward = jnp.where(me_z < depth_z // 2, me_z + 1, me_z - 1)
    mate = tp + 1 - 2 * (tp % 2)
    far = (tp + 2) % n_tp
    cross = (mate + 2) % n_tp

    barrier = pltpu.get_barrier_semaphore()

    for step in (1, -1):

        @pl.when((me_z + step >= 0) & (me_z + step < depth_z))
        def _(step=step):
            pl.semaphore_signal(
                barrier,
                inc=1,
                device_id={"ep": (me_z + step) * 2 + me_y},
                device_id_type=pl.DeviceIdType.MESH,
            )

    pl.semaphore_signal(
        barrier, inc=1, device_id={"ep": beside}, device_id_type=pl.DeviceIdType.MESH
    )
    for peer in (mate, far, cross):
        pl.semaphore_signal(
            barrier, inc=1, device_id={"tp": peer}, device_id_type=pl.DeviceIdType.MESH
        )

    loads = [
        pltpu.make_async_copy(gate_hbm, gate, load_sem.at[0]),
        pltpu.make_async_copy(up_hbm, up, load_sem.at[1]),
        pltpu.make_async_copy(down_hbm, down, load_sem.at[2]),
        pltpu.make_async_copy(query_hbm, query, load_sem.at[3]),
        pltpu.make_async_copy(key_up_hbm, key_up, load_sem.at[4]),
        pltpu.make_async_copy(value_up_hbm, value_up, load_sem.at[5]),
        pltpu.make_async_copy(out_proj_hbm, out_proj, load_sem.at[6]),
    ]
    for load in loads:
        load.start()

    def remote(src, dst, sent, got, device):
        return pltpu.make_async_remote_copy(
            src_ref=src,
            dst_ref=dst,
            send_sem=send_sem.at[sum(send_kinds(depth_z)[: sent[0]]) + sent[1]],
            recv_sem=recv_sem.at[sum(recv_kinds(depth_z)[: got[0]]) + got[1]],
            device_id=device,
            device_id_type=pl.DeviceIdType.MESH,
        )

    def columns(half):
        return pl.ds(half * (width // 2), width // 2)

    def tok_step(origin, step, half):
        kind = 0 if step > 0 else 1
        target = {"ep": (me_z + step) * 2 + me_y}
        number = origin * 2 + half
        place = tok.at[origin, :, columns(half)]
        copies = [remote(place, place, (kind, number), (0, number), target)]
        if half == 0:
            place = info.at[origin]
            copies.append(remote(place, place, (kind + 2, origin), (2, origin), target))
        return copies

    def spread_tok(origin, step):
        inside = (me_z < depth_z - 1) if step > 0 else (me_z > 0)
        coming = (origin <= me_z) if step > 0 else (origin >= me_z)
        return inside & coming

    def source_of(unit):
        return line_order(me_z, depth_z, unit // 2) * 2 + (me_y + unit) % 2

    def hop_rows(kind, unit, block, peer):
        place = arrived.at[source_of(unit), block]
        return remote(place, place, (kind, 0), (kind, unit), {"tp": peer})

    def far_rows(unit, half, block):
        place = arrived.at[source_of(unit), block, :, columns(half)]
        return remote(place, place, (4, 0), (4, unit * 2 + half), {"tp": far})

    def y_rows(spot, half):
        origin = line_order(me_z, depth_z, spot)
        return remote(
            away.at[origin, :, columns(half)],
            arrived.at[origin * 2 + me_y, tp, :, columns(half)],
            (7, 0),
            (7, spot * 2 + half),
            {"ep": beside},
        )

    def to_mate(kind, unit, block, part):
        source = source_of(unit)
        return remote(
            partial.at[source, block],
            from_pair.at[source, part],
            (kind, 0),
            (kind, unit),
            {"tp": mate},
        )

    def to_far(unit, half):
        source = source_of(unit)
        return remote(
            pair_sum.at[source, :, columns(half)],
            from_far.at[source, :, columns(half)],
            (10, 0),
            (10, unit * 2 + half),
            {"tp": far},
        )

    def send_far(unit):
        for half in range(2):
            to_far(unit, half).start()

    def y_back(spot, half):
        origin = line_order(me_z, depth_z, spot)
        return remote(
            result.at[origin * 2 + 1 - me_y, :, columns(half)],
            returned.at[origin, :, columns(half)],
            (11, 0),
            (11, spot * 2 + half),
            {"ep": beside},
        )

    def z_back(origin, sender, half):
        return remote(
            joined.at[origin, :, columns(half)],
            answers.at[sender, :, columns(half)],
            (12, origin * 2 + half),
            (12, sender * 2 + half),
            {"ep": origin * 2 + me_y},
        )

    def z_pass(half):
        return remote(
            joined.at[line_order(me_z, depth_z, 2), :, columns(half)],
            passing.at[:, columns(half)],
            (18, half),
            (18, half),
            {"ep": inward * 2 + me_y},
        )

    def lat_x(block):
        place = lat_all.at[me_z, me_y, block]
        return remote(place, place, (13, 0), (13, 0), {"tp": far})

    def lat_up(origin):
        copies = []
        for part in range(2):
            place = lat_all.at[origin, :, (tp + 2 * part) % n_tp]
            number = (14, origin * 2 + part)
            copies.append(remote(place, place, number, number, {"ep": (me_z + 1) * 2 + me_y}))
        return copies

    def lat_y(part, side):
        place = lat_all.at[me_z, side, (tp + 2 * part) % n_tp]
        return remote(place, place, (15, part), (15, part), {"ep": beside})

    def lat_mate(part, first):
        place = lat_all.at[:, :, (first + 2 * part) % n_tp]
        return remote(place, place, (16, part), (16, part), {"tp": mate})

    def head_copy(number, peer, slot):
        return remote(
            heads_own.at[peer], heads_all.at[slot], (17, number), (17, number), {"tp": peer}
        )

    first_route = routes[0:1, :]
    second_route = routes[1:2, :]
    lane_expert = lax.broadcasted_iota(jnp.int32, (experts, row_count), 0)
    is_first = lane_expert == first_route
    is_second = lane_expert == second_route
    named = jnp.where(is_first | is_second, 1.0, 0.0).astype(bf16)
    ahead = lax.broadcasted_iota(jnp.int32, (row_count, row_count), 0)
    behind = lax.broadcasted_iota(jnp.int32, (row_count, row_count), 1)
    before = jnp.where(ahead < behind, 1.0, 0.0).astype(bf16)
    earlier = jnp.dot(named, before, preferred_element_type=f32)
    first_slot = jnp.sum(jnp.where(is_first, earlier, 0.0), axis=0, keepdims=True)
    second_slot = jnp.sum(jnp.where(is_second, earlier, 0.0), axis=0, keepdims=True)
    both_prob = expert_prob[0:1, :] + expert_prob[1:2, :]
    info[me_z] = jnp.full(info.shape[1:], -1.0, f32)
    info[me_z, 0:1, 0:row_count] = first_route.astype(f32) * capacity + first_slot
    info[me_z, 1:2, 0:row_count] = second_route.astype(f32) * capacity + second_slot
    info[me_z, 2:3, 0:row_count] = group_prob[...] * expert_prob[0:1, :] / both_prob
    info[me_z, 3:4, 0:row_count] = group_prob[...] * expert_prob[1:2, :] / both_prob
    tok[me_z] = rms_scale(tokens[...], moe_gain[...]).astype(bf16)

    pl.semaphore_wait(barrier, jnp.where(inner, 6, 5))

    for step in (1, -1):

        @pl.when(spread_tok(me_z, step))
        def _(step=step):
            for half in range(2):
                for copy in tok_step(me_z, step, half):
                    copy.start()

    def wanted():
        row = lax.broadcasted_iota(jnp.int32, (2 * capacity, info.shape[2]), 0)
        own = me * capacity + row
        other = (beside - 1) * capacity + row
        return jnp.where(row < capacity, own, other).astype(f32)

    def take_tok(spot, half):
        origin = line_order(me_z, depth_z, spot)
        for copy in tok_step(origin, 1, half):
            copy.wait_recv()
        for step in (1, -1):

            @pl.when(spread_tok(origin, step))
            def _(step=step):
                for copy in tok_step(origin, step, half):
                    copy.start()

    def raise_lat(origin):
        @pl.when(spread_tok(origin, 1))
        def _():
            for copy in lat_up(origin):
                copy.start()

    def take_lat(below):
        @pl.when(me_z >= below)
        def _():
            for copy in lat_up(me_z - below):
                copy.wait_recv()
            raise_lat(me_z - below)

    def gather_spot(spot, half):
        origin = line_order(me_z, depth_z, spot)

        @pl.when((spot > 0) & jnp.logical_not(inner))
        def _():
            take_tok(spot, half)

        want = wanted()
        table = jnp.where(
            (want == info[origin, 0:1, :]) | (want == info[origin, 1:2, :]), 1.0, 0.0
        )
        packed = jnp.dot(
            table[:, :row_count].astype(bf16),
            tok[origin, :, columns(half)],
            preferred_element_type=f32,
        ).astype(bf16)
        arrived[origin * 2 + me_y, tp, :, columns(half)] = packed[:capacity]
        away[origin, :, columns(half)] = packed[capacity:]
        y_rows(spot, half).start()
        far_rows(spot * 2, half, tp).start()

    def pass_y(spot, half):
        y_rows(spot, half).wait_recv()
        far_rows(spot * 2 + 1, half, tp).start()

    def share(unit):
        hop_rows(5, unit, tp, mate).start()

    def relay(unit):
        for half in range(2):
            far_rows(unit, half, far).wait_recv()
        hop_rows(6, unit, far, mate).start()

    def compute(unit):
        source = source_of(unit)
        hop_rows(5, unit, mate, mate).wait_recv()
        hop_rows(6, unit, cross, mate).wait_recv()

        @pl.when(unit == 0)
        def _():
            for load in loads[:3]:
                load.wait()

        rows = arrived[source].reshape(n_tp * capacity, width)
        gate_values = jnp.dot(rows, gate[...], preferred_element_type=f32)
        up_values = jnp.dot(rows, up[...], preferred_element_type=f32)
        hidden = (gate_values / (1.0 + jnp.exp(-gate_values)) * up_values).astype(bf16)
        product = jnp.dot(hidden, down[...], preferred_element_type=f32)
        partial[source] = product.astype(bf16).reshape(n_tp, capacity, width)
        to_mate(9, unit, cross, 1).start()
        to_mate(8, unit, mate, 0).start()

    def reduce_pair(unit):
        source = source_of(unit)
        to_mate(9, unit, cross, 1).wait_recv()
        pair_sum[source] = (
            partial[source, far].astype(f32) + from_pair[source, 1].astype(f32)
        ).astype(bf16)

    def reduce_far(unit):
        source = source_of(unit)
        to_mate(8, unit, mate, 0).wait_recv()
        for half in range(2):
            to_far(unit, half).wait_recv()
            result[source, :, columns(half)] = (
                partial[source, tp, :, columns(half)].astype(f32)
                + from_pair[source, 0, :, columns(half)].astype(f32)
                + from_far[source, :, columns(half)].astype(f32)
            ).astype(bf16)
            if unit % 2 == 1:
                y_back(unit // 2, half).start()

    def weighted(spot, half):
        origin = line_order(me_z, depth_z, spot)
        y_back(spot, half).wait_recv()
        want = wanted()
        weights = jnp.where(want == info[origin, 0:1, :], info[origin, 2:3, :], 0.0) + jnp.where(
            want == info[origin, 1:2, :], info[origin, 3:4, :], 0.0
        )
        weights = weights[:, :row_count]
        high = weights.astype(bf16)
        low = (weights - high.astype(f32)).astype(bf16)
        rows = jnp.concatenate(
            [result[origin * 2 + me_y, :, columns(half)], returned[origin, :, columns(half)]],
            axis=0,
        )
        over_slots = (((0,), (0,)), ((), ()))
        return lax.dot_general(
            high, rows, over_slots, preferred_element_type=f32
        ) + lax.dot_general(low, rows, over_slots, preferred_element_type=f32)

    def join(spot):
        origin = line_order(me_z, depth_z, spot)
        for half in range(2):
            joined[origin, :, columns(half)] = weighted(spot, half).astype(bf16)
            z_back(origin, me_z, half).start()

    def join_pass():
        origin = line_order(me_z, depth_z, 2)
        for half in range(2):
            joined[origin, :, columns(half)] = weighted(2, half).astype(bf16)
            z_pass(half).start()

    def join_passed():
        origin = line_order(me_z, depth_z, 1)
        for half in range(2):
            own = weighted(1, half)
            z_pass(half).wait_recv()
            joined[origin, :, columns(half)] = (
                own + passing[:, columns(half)].astype(f32)
            ).astype(bf16)
            z_back(origin, me_z, half).start()

    def own_latent():
        same, swapped = turn_tables(ROPE_DIM, rope_room, 0)
        first_row = (me * n_tp + tp) * own_rows
        cosine, sine = angle_tables(first_row, own_rows, rope_room)
        turned = jnp.dot(rope_key[...], same, preferred_element_type=f32) * cosine + (
            jnp.dot(rope_key[...], swapped, preferred_element_type=f32) * sine
        )
        lat_all[me_z, me_y, tp, :, :latent_width] = rms_scale(
            latent[...], latent_gain[...]
        ).astype(bf16)
        lat_all[me_z, me_y, tp, :, latent_width:] = turned.astype(bf16)
        lat_x(tp).start()

    def spread_query():
        loads[3].wait()
        rows, packed_width = query.shape
        head_width = packed_width // heads
        nope_width = heads * NOPE
        cosine, sine = angle_tables(me * rows, rows, rope_room)
        row = lax.broadcasted_iota(jnp.int32, (packed_width, nope_width), 0)
        lane = lax.broadcasted_iota(jnp.int32, (packed_width, nope_width), 1)
        out_lane = lax.broadcasted_iota(jnp.int32, (rows, nope_width), 1)
        plain = jnp.zeros((packed_width, nope_width), f32)
        for head in range(heads):
            inside = (lane >= head * NOPE) & (lane < (head + 1) * NOPE)
            plain = jnp.where(inside & (row - lane == head * ROPE_DIM), 1.0, plain)
        nope = jnp.dot(query[...], plain.astype(bf16), preferred_element_type=f32)
        for head in range(heads):
            inside = (out_lane >= head * NOPE) & (out_lane < (head + 1) * NOPE)
            query_big[head, :, :nope_width] = jnp.where(inside, nope, 0.0).astype(bf16)
            same, swapped = turn_tables(packed_width, rope_room, head * head_width + NOPE)
            turned = jnp.dot(query[...], same, preferred_element_type=f32) * cosine + (
                jnp.dot(query[...], swapped, preferred_element_type=f32) * sine
            )
            query_big[head, :, nope_width:] = turned.astype(bf16)

    def fill_keys():
        nope_width = key_up.shape[1]
        packed = lat_all[...].reshape(-1, lat_all.shape[-1])
        normed = packed[:, :latent_width]
        loads[4].wait()
        loads[5].wait()
        keys[:, :nope_width] = jnp.dot(normed, key_up[...], preferred_element_type=f32).astype(bf16)
        keys[:, nope_width:] = packed[:, latent_width:]
        values[...] = jnp.dot(normed, value_up[...], preferred_element_type=f32).astype(bf16)

    def attend(first_head, last_head):
        rows = query_big.shape[1]
        seq = keys.shape[0]
        value_width = values.shape[1] // heads
        query_pos = me * rows + lax.broadcasted_iota(jnp.int32, (rows, seq), 0)
        allowed = lax.broadcasted_iota(jnp.int32, (rows, seq), 1) <= query_pos
        lane = lax.broadcasted_iota(jnp.int32, (rows, heads * value_width), 1)
        scale = (NOPE + ROPE_DIM) ** (-0.5)
        gathered = jnp.zeros((rows, heads * value_width), f32)
        if first_head > 0:
            gathered = heads_own[...].reshape(rows, -1).astype(f32)
        for head in range(first_head, last_head):
            scores = (
                lax.dot_general(
                    query_big[head],
                    keys[...],
                    (((1,), (1,)), ((), ())),
                    preferred_element_type=f32,
                )
                * scale
            )
            scores = jnp.where(allowed, scores, masked_value)
            raised = jnp.exp(scores - jnp.max(scores, axis=1, keepdims=True))
            totals = jnp.sum(raised, axis=1, keepdims=True)
            summed = jnp.dot(raised.astype(bf16), values[...], preferred_element_type=f32)
            inside = (lane >= head * value_width) & (lane < (head + 1) * value_width)
            gathered = jnp.where(inside, summed / totals, gathered)
        heads_own[...] = gathered.astype(bf16).reshape(heads_own.shape)

    peers = (mate, far, cross)

    @pl.when(inner)
    def _():
        answers[line_order(me_z, depth_z, 2)] = jnp.zeros(answers.shape[1:], bf16)

    def clear(above, carry):
        @pl.when(me_z + above < depth_z)
        def _():
            lat_all[me_z + above] = jnp.zeros(lat_all.shape[1:], bf16)

        return carry

    def stage(turn, carry):
        spot = turn // 2

        @pl.when(turn == 0)
        def _():
            gather_spot(0, 0)

        @pl.when(turn == 1)
        def _():
            pass_y(0, 1)

        @pl.when((turn == 1) & inner)
        def _():
            take_tok(1, 0)
            take_tok(3, 0)

        @pl.when((turn == 2) & inner)
        def _():
            take_tok(1, 1)
            take_tok(3, 1)

        @pl.when((turn == 3) & inner)
        def _():
            take_tok(2, 0)

        @pl.when((turn == 4) & inner)
        def _():
            take_tok(2, 1)

        @pl.when(turn % 2 == 0)
        def _():
            gather_spot(spot, 1)
            share(turn)

            @pl.when(turn > 0)
            def _():
                pass_y(spot, 0)

        @pl.when(turn % 2 == 1)
        def _():
            gather_spot(spot + 1, 0)

            @pl.when(turn > 1)
            def _():
                pass_y(spot, 1)

            share(turn)

        @pl.when(turn == 0)
        def _():
            own_latent()
            lax.fori_loop(1, depth_z, clear, 0)
            pass_y(0, 0)

        @pl.when(turn == 2)
        def _():
            lat_x(far).wait_recv()
            lat_y(0, me_y).start()
            lat_y(1, me_y).start()

        @pl.when(turn == 4)
        def _():
            lat_y(0, 1 - me_y).wait_recv()
            lat_y(1, 1 - me_y).wait_recv()
            raise_lat(me_z)

        @pl.when(turn == 6)
        def _():
            take_lat(1)

        @pl.when(turn >= 4)
        def _():
            reduce_pair(turn - 4)

        @pl.when(turn >= 2)
        def _():
            compute(turn - 2)

        @pl.when(turn >= 1)
        def _():
            relay(turn - 1)

        @pl.when(turn == 2)
        def _():
            spread_query()

        return carry

    lax.fori_loop(0, units - 1, stage, 0)

    pass_y(depth_z - 1, 1)
    share(7)
    reduce_pair(4)
    send_far(4)
    take_lat(2)
    compute(5)
    relay(6)
    reduce_pair(3)
    reduce_pair(5)
    send_far(5)
    compute(6)
    take_lat(3)
    lat_mate(0, tp).start()
    lat_mate(1, tp).start()
    reduce_pair(6)
    relay(7)
    lat_mate(0, mate).wait_recv()
    lat_mate(1, mate).wait_recv()
    fill_keys()
    compute(7)
    send_far(3)
    reduce_far(4)
    reduce_far(5)
    reduce_pair(7)
    send_far(7)
    send_far(6)
    attend(0, heads // 2)
    attend(heads // 2, heads)
    for number, peer in enumerate(peers):
        head_copy(number, peer, tp).start()
    send_far(2)
    send_far(1)
    send_far(0)
    heads_all[tp] = heads_own[tp]
    reduce_far(3)

    @pl.when(inner)
    def _():
        join(2)

    @pl.when(jnp.logical_not(inner))
    def _():
        join_pass()

    reduce_far(7)
    reduce_far(6)

    join(3)
    reduce_far(2)

    @pl.when(inner)
    def _():
        join_passed()

    @pl.when(jnp.logical_not(inner))
    def _():
        join(1)

    loads[6].wait()
    for number, peer in enumerate(peers):
        head_copy(number, peer, peer).wait_recv()
    depth = heads_all.shape[2]
    total = jnp.zeros(mixed.shape, f32)
    for part in range(n_tp):
        total = total + jnp.dot(
            heads_all[part],
            out_proj[part * depth : (part + 1) * depth, :],
            preferred_element_type=f32,
        )
    mixed[...] = total.astype(mixed.dtype)
    reduce_far(1)
    reduce_far(0)
    chosen = [weighted(0, half) for half in range(2)]

    def finish_line(origin, carry):
        for step in (1, -1):

            @pl.when(spread_tok(origin, step))
            def _(step=step):
                for copy in (*tok_step(origin, step, 0), *tok_step(origin, step, 1)):
                    copy.wait_send()

        @pl.when(spread_tok(origin, 1))
        def _():
            for copy in lat_up(origin):
                copy.wait_send()

        passed = jnp.logical_not(inner) & (origin == line_order(me_z, depth_z, 2))

        @pl.when((origin != me_z) & jnp.logical_not(passed))
        def _():
            for half in range(2):
                z_back(origin, me_z, half).wait_send()

        return carry

    lax.fori_loop(0, depth_z, finish_line, 0)

    @pl.when(jnp.logical_not(inner))
    def _():
        for half in range(2):
            z_pass(half).wait_send()

    lat_x(tp).wait_send()
    for part in range(2):
        lat_y(part, me_y).wait_send()
        lat_mate(part, tp).wait_send()
    for number, peer in enumerate(peers):
        head_copy(number, peer, tp).wait_send()

    def all_sent(kind, src, device):
        remote(src, src, (kind, 0), (4, 0), device).wait_send()

    all_sent(4, arrived.at[:, tp], {"tp": far})
    all_sent(5, arrived.at[:, tp], {"tp": mate})
    all_sent(6, arrived.at[:, far], {"tp": mate})
    all_sent(7, away, {"ep": beside})
    all_sent(8, partial.at[:, mate], {"tp": mate})
    all_sent(9, partial.at[:, cross], {"tp": mate})
    all_sent(10, pair_sum, {"tp": far})
    all_sent(11, returned, {"ep": beside})

    none = line_order(me_z, depth_z, 2)
    for half in range(2):
        total = chosen[half]
        for shift in range(1, depth_z):
            sender = (me_z + shift) % depth_z

            @pl.when(jnp.logical_not(inner & (sender == none)))
            def _(sender=sender, half=half):
                z_back(me_z, sender, half).wait_recv()

            total = total + answers[sender, :, columns(half)].astype(f32)
        moe_out[:, columns(half)] = total.astype(moe_out.dtype)


def hand_over(mixed_in, moe_in, mixed_out, moe_out, sem):
    copies = [
        pltpu.make_async_copy(mixed_in, mixed_out, sem.at[0]),
        pltpu.make_async_copy(moe_in, moe_out, sem.at[1]),
    ]
    for copy in copies:
        copy.start()
    for copy in copies:
        copy.wait()


def fused_body(
    query,
    latent,
    rope_key,
    latent_gain,
    key_up,
    value_up,
    out_proj,
    tokens,
    moe_gain,
    routes,
    group_prob,
    expert_prob,
    w_gate,
    w_up,
    w_down,
):
    n_ep = lax.axis_size("ep")
    n_tp = lax.axis_size("tp")
    depth_z = n_ep // 2
    query_rows = query.shape[0]
    own_rows, latent_width = latent.shape
    heads = query.shape[1] // (NOPE + ROPE_DIM)
    rope_room = padded(ROPE_DIM)
    row_count, width = tokens.shape
    capacity = 2 * routes.shape[1] * row_count // n_ep
    bf16 = jnp.bfloat16
    lat_width = latent_width + rope_room
    key_width = key_up.shape[1] + rope_room
    vmem = pl.BlockSpec(memory_space=pltpu.VMEM)
    anywhere = pl.BlockSpec(memory_space=pl.ANY)
    results = pl.pallas_call(
        functools.partial(both_halves, heads, capacity, depth_z),
        out_shape=(
            pltpu.VMEM((own_rows, out_proj.shape[1]), bf16),
            pltpu.VMEM((row_count, width), bf16),
        ),
        in_specs=[vmem] * 8 + [anywhere] * 7,
        out_specs=(vmem, vmem),
        scratch_shapes=[
            pltpu.VMEM((depth_z, row_count, width), bf16),
            pltpu.VMEM((depth_z, 8, padded(row_count)), jnp.float32),
            pltpu.VMEM((depth_z, capacity, width), bf16),
            pltpu.VMEM((n_ep, n_tp, capacity, width), bf16),
            pltpu.VMEM((depth_z, 2, n_tp, own_rows, lat_width), bf16),
            pltpu.VMEM((n_ep, n_tp, capacity, width), bf16),
            pltpu.VMEM((n_ep, 2, capacity, width), bf16),
            pltpu.VMEM((n_ep, capacity, width), bf16),
            pltpu.VMEM((n_ep, capacity, width), bf16),
            pltpu.VMEM((n_ep, capacity, width), bf16),
            pltpu.VMEM((depth_z, capacity, width), bf16),
            pltpu.VMEM((depth_z, row_count, width), bf16),
            pltpu.VMEM((depth_z, row_count, width), bf16),
            pltpu.VMEM((row_count, width), bf16),
            pltpu.VMEM((n_ep * n_tp * own_rows, key_width), bf16),
            pltpu.VMEM((n_ep * n_tp * own_rows, value_up.shape[1]), bf16),
            pltpu.VMEM((heads, query_rows, key_width), bf16),
            pltpu.VMEM((n_tp, own_rows, value_up.shape[1]), bf16),
            pltpu.VMEM((n_tp, own_rows, value_up.shape[1]), bf16),
            pltpu.VMEM(query.shape, bf16),
            pltpu.VMEM(key_up.shape, bf16),
            pltpu.VMEM(value_up.shape, bf16),
            pltpu.VMEM(out_proj.shape, bf16),
            pltpu.VMEM(w_gate.shape[1:], bf16),
            pltpu.VMEM(w_up.shape[1:], bf16),
            pltpu.VMEM(w_down.shape[1:], bf16),
            pltpu.SemaphoreType.DMA((7,)),
            pltpu.SemaphoreType.DMA((sum(send_kinds(depth_z)),)),
            pltpu.SemaphoreType.DMA((sum(recv_kinds(depth_z)),)),
        ],
        compiler_params=pltpu.CompilerParams(
            collective_id=0, has_side_effects=True, vmem_limit_bytes=60 * 1024 * 1024
        ),
        name="both_halves",
    )(
        tokens,
        moe_gain.reshape(1, -1),
        routes.T,
        group_prob.reshape(1, -1),
        expert_prob.T,
        latent,
        rope_key,
        latent_gain.reshape(1, -1),
        query,
        key_up,
        value_up,
        out_proj,
        w_gate[0],
        w_up[0],
        w_down[0],
    )
    return pl.pallas_call(
        hand_over,
        out_shape=tuple(jax.ShapeDtypeStruct(part.shape, part.dtype) for part in results),
        in_specs=[vmem] * 2,
        out_specs=(anywhere, anywhere),
        scratch_shapes=[pltpu.SemaphoreType.DMA((2,))],
        compiler_params=pltpu.CompilerParams(vmem_limit_bytes=4 * 1024 * 1024),
        name="hand_over",
    )(*results)


def fits_kernel(mesh, *arrays):
    n_ep, n_tp = mesh.shape["ep"], mesh.shape["tp"]
    tokens, routes, latent = arrays[7], arrays[9], arrays[1]
    row_count = tokens.shape[0] // (n_ep * n_tp)
    capacity = 2 * routes.shape[1] * row_count // n_ep
    own_rows = latent.shape[0] // (n_ep * n_tp)
    shaped = n_tp == 4 and n_ep == 8 and routes.shape[1] == 2
    aligned = capacity % 16 == 0 and own_rows % 16 == 0 and row_count % 16 == 0
    return shaped and aligned and latent.shape[0] <= 2048


def mapped(mesh, chosen):
    return jax.shard_map(
        chosen,
        mesh=mesh,
        in_specs=(
            P("ep", "tp"),
            P(("ep", "tp"), None),
            P(("ep", "tp"), None),
            P(),
            P(None, "tp"),
            P(None, "tp"),
            P(),
            P(("ep", "tp"), None),
            P(),
            P(("ep", "tp"), None),
            P(("ep", "tp")),
            P(("ep", "tp"), None),
            P("ep", None, "tp"),
            P("ep", None, "tp"),
            P("ep", "tp", None),
        ),
        out_specs=(P(("ep", "tp"), None), P(("ep", "tp"), None)),
        check_vma=False,
    )


def solution(mesh):
    def whole(*arrays):
        chosen = fused_body if fits_kernel(mesh, *arrays) else body
        return mapped(mesh, chosen)(*arrays)

    return whole
```

```python
import functools
import math

import jax
import jax.numpy as jnp
from jax import lax
from jax.experimental import pallas as pl
from jax.experimental.pallas import tpu as pltpu
from jax.sharding import PartitionSpec as P

NOPE = 64
ROPE_DIM = 32
V_DIM = 64


epsilon = 1e-06
rope_base = 10000.0
masked_value = -1e30


def rms_scale(values, gain):
    widened = values.astype(jnp.float32)
    return widened * lax.rsqrt(jnp.mean(widened * widened, axis=-1, keepdims=True) + epsilon) * gain


def tables(positions, rope_width):
    half_width = rope_width // 2
    inverse = rope_base ** (-2.0 * jnp.arange(half_width, dtype=jnp.float32) / rope_width)
    angles = positions.astype(jnp.float32)[:, None] * inverse[None, :]
    return (jnp.cos(angles), jnp.sin(angles))


def rotate(values, cosine, sine):
    half_width = values.shape[-1] // 2
    lower = values[..., :half_width]
    upper = values[..., half_width:]
    return jnp.concatenate([lower * cosine - upper * sine, lower * sine + upper * cosine], axis=-1)


def keep_state(state_in):
    return state_in


def attend_block(running, query_rot, query_pos, key_part, value_part, rope_part):
    amount = key_part.shape[0]
    span_rows = math.gcd(amount, 1024)
    head_count = query_rot.shape[1]
    scale_factor = query_rot.shape[2] ** (-0.5)
    last_query = query_pos[-1]

    def update(state, block_at):
        row_begin = block_at * span_rows
        keys_here = lax.dynamic_slice_in_dim(key_part, row_begin, span_rows, 0).reshape(
            span_rows, head_count, -1
        )
        values_here = lax.dynamic_slice_in_dim(value_part, row_begin, span_rows, 0).reshape(
            span_rows, head_count, -1
        )
        rope_here = lax.dynamic_slice_in_dim(rope_part, row_begin, span_rows, 0)
        key_pos = row_begin + jnp.arange(span_rows, dtype=jnp.int32)

        def advance(state_in):
            top_old, totals, weighted = state_in
            shared = jnp.broadcast_to(
                rope_here[:, None, :], (span_rows, head_count, rope_here.shape[1])
            )
            full_keys = jnp.concatenate([keys_here, shared], axis=-1)
            scores = (
                jnp.einsum("qhd,khd->hqk", query_rot, full_keys, preferred_element_type=jnp.float32)
                * scale_factor
            )
            allowed = key_pos[None, :] <= query_pos[:, None]
            scores = jnp.where(allowed[None], scores, masked_value)
            top_new = jnp.maximum(top_old, jnp.max(scores, axis=-1))
            raised = jnp.where(allowed[None], jnp.exp(scores - top_new[..., None]), 0.0)
            factor = jnp.exp(top_old - top_new)
            totals = totals * factor + jnp.sum(raised, axis=-1)
            weighted = weighted * factor[..., None] + jnp.einsum(
                "hqk,khd->hqd",
                raised.astype(jnp.bfloat16),
                values_here,
                preferred_element_type=jnp.float32,
            )
            return (top_new, totals, weighted)

        return (lax.cond(key_pos[0] <= last_query, advance, keep_state, state), None)

    running, _ = lax.scan(update, running, jnp.arange(amount // span_rows))
    return running


def mixer_half(query, latent, rope_key, latent_gain, key_up, value_up, out_proj):
    query_rows = query.shape[0]
    own_rows = latent.shape[0]
    query_start = lax.axis_index("ep") * query_rows
    key_start = query_start + lax.axis_index("tp") * own_rows
    head_count = query.shape[1] // (NOPE + ROPE_DIM)
    normed = rms_scale(latent, latent_gain).astype(jnp.bfloat16)
    key_cos, key_sin = tables(key_start + jnp.arange(own_rows, dtype=jnp.int32), ROPE_DIM)
    rotated_key = rotate(rope_key.astype(jnp.float32), key_cos, key_sin).astype(jnp.bfloat16)
    query_pos = query_start + jnp.arange(query_rows, dtype=jnp.int32)
    query_cos, query_sin = tables(query_pos, ROPE_DIM)
    query_heads = query.reshape(query_rows, head_count, NOPE + ROPE_DIM)
    turned = rotate(
        query_heads[..., NOPE:].astype(jnp.float32), query_cos[:, None, :], query_sin[:, None, :]
    ).astype(jnp.bfloat16)
    query_rot = jnp.concatenate([query_heads[..., :NOPE], turned], axis=-1)
    last_query = query_start + query_rows - 1
    initial = (
        jnp.full((head_count, query_rows), masked_value, jnp.float32),
        jnp.zeros((head_count, query_rows), jnp.float32),
        jnp.zeros((head_count, query_rows, V_DIM), jnp.float32),
    )
    shard_rows = (
        lax.all_gather(normed, ("ep", "tp"), axis=0, tiled=True),
        lax.all_gather(rotated_key, ("ep", "tp"), axis=0, tiled=True),
    )

    def compute(state_in):
        key_part = jnp.dot(shard_rows[0], key_up, preferred_element_type=jnp.float32).astype(
            jnp.bfloat16
        )
        value_part = jnp.dot(shard_rows[0], value_up, preferred_element_type=jnp.float32).astype(
            jnp.bfloat16
        )
        return attend_block(state_in, query_rot, query_pos, key_part, value_part, shard_rows[1])

    running = lax.cond(jnp.int32(0) <= last_query, compute, keep_state, initial)
    totals = running[1]
    weighted = running[2]
    attention = (
        (weighted / totals[..., None])
        .transpose(1, 0, 2)
        .reshape(query_rows, head_count * V_DIM)
        .astype(jnp.bfloat16)
    )
    own_attention = lax.all_to_all(attention, "tp", split_axis=0, concat_axis=1, tiled=True)
    return jnp.dot(own_attention, out_proj, preferred_element_type=jnp.float32).astype(jnp.bfloat16)


def expert_half(tokens, moe_gain, routes, group_prob, expert_prob, w_gate, w_up, w_down):
    row_count, model_width = tokens.shape
    top_count = routes.shape[1]
    expert_count = lax.axis_size("ep")
    capacity = 2 * top_count * row_count // expert_count
    normed = rms_scale(tokens, moe_gain).astype(jnp.bfloat16)
    flat_routes = routes.reshape(-1)
    onehot = (flat_routes[:, None] == jnp.arange(expert_count, dtype=jnp.int32)[None, :]).astype(
        jnp.int32
    )
    earlier = jnp.cumsum(onehot, axis=0) - onehot
    slot_index = jnp.sum(earlier * onehot, axis=1)
    target = flat_routes * capacity + slot_index
    owner = target[None, :] == jnp.arange(expert_count * capacity, dtype=jnp.int32)[:, None]
    dispatch_table = jnp.any(
        owner.reshape(expert_count * capacity, row_count, top_count), axis=2
    ).astype(jnp.bfloat16)
    outgoing = jnp.dot(dispatch_table, normed, preferred_element_type=jnp.float32).astype(
        jnp.bfloat16
    )
    outgoing = outgoing.reshape(expert_count, capacity, model_width)
    arrived = lax.all_to_all(outgoing, "ep", split_axis=0, concat_axis=0, tiled=True)
    sources, slots, _ = arrived.shape
    flat_rows = arrived.reshape(sources * slots, model_width)
    shard_rows = lax.all_gather(flat_rows, "tp", axis=0, tiled=True)
    gate_values = jnp.dot(shard_rows, w_gate[0], preferred_element_type=jnp.float32)
    up_values = jnp.dot(shard_rows, w_up[0], preferred_element_type=jnp.float32)
    hidden = (jax.nn.silu(gate_values) * up_values).astype(jnp.bfloat16)

    def lower(offset, amount):
        return jnp.dot(hidden, w_down[0], preferred_element_type=jnp.float32)

    summed = lax.psum_scatter(
        lower(jnp.int32(0), sources * slots * lax.axis_size("tp")).astype(jnp.bfloat16),
        "tp",
        scatter_dimension=0,
        tiled=True,
    )
    result = summed.reshape(sources, slots, model_width)
    returned = lax.all_to_all(result, "ep", split_axis=0, concat_axis=0, tiled=True)
    returned_flat = returned.reshape(expert_count * capacity, model_width)
    picked = returned_flat[target].reshape(row_count, top_count, model_width).astype(jnp.float32)
    shares = group_prob[:, None] * expert_prob / jnp.sum(expert_prob, axis=1, keepdims=True)
    return jnp.sum(shares[:, :, None] * picked, axis=1).astype(jnp.bfloat16)


def body(
    query,
    latent,
    rope_key,
    latent_gain,
    key_up,
    value_up,
    out_proj,
    tokens,
    moe_gain,
    routes,
    group_prob,
    expert_prob,
    w_gate,
    w_up,
    w_down,
):
    mixed = mixer_half(query, latent, rope_key, latent_gain, key_up, value_up, out_proj)
    moe_out = expert_half(tokens, moe_gain, routes, group_prob, expert_prob, w_gate, w_up, w_down)
    return (mixed, moe_out)


def padded(amount):
    return -(-amount // 128) * 128


def send_kinds(depth):
    line = 2 * depth
    return (line, line, depth, depth, 1, 1, 1, 1, 1, 1, 1, 1, line, 1, line, 2, 2, 3, 2)


def recv_kinds(depth):
    line = 2 * depth
    wide = 2 * line
    gather = (wide, line, line, line, line, line, wide)
    return (line, 0, depth, 0, *gather, line, line, 1, line, 2, 2, 3, 2)


def line_order(place, depth, spot):
    mirrored = depth - 1 - place
    from_low = (place + spot) % depth
    from_high = depth - 1 - (mirrored + spot) % depth
    return jnp.where(place < depth // 2, from_low, from_high)


def angle_tables(first_row, rows, lanes):
    half_width = ROPE_DIM // 2
    lane = lax.broadcasted_iota(jnp.int32, (rows, lanes), 1) % half_width
    position = first_row + lax.broadcasted_iota(jnp.int32, (rows, lanes), 0)
    inverse = jnp.exp(lane.astype(jnp.float32) * (-2.0 * math.log(rope_base) / ROPE_DIM))
    angles = position.astype(jnp.float32) * inverse
    return (jnp.cos(angles), jnp.sin(angles))


def turn_tables(rows, lanes, first):
    half_width = ROPE_DIM // 2
    row = lax.broadcasted_iota(jnp.int32, (rows, lanes), 0) - first
    lane = lax.broadcasted_iota(jnp.int32, (rows, lanes), 1)
    same = jnp.where((row == lane) & (lane < ROPE_DIM), 1.0, 0.0)
    lower = jnp.where((row == lane + half_width) & (lane < half_width), -1.0, 0.0)
    upper = jnp.where(
        (row == lane - half_width) & (lane >= half_width) & (lane < ROPE_DIM), 1.0, 0.0
    )
    return (same.astype(jnp.bfloat16), (lower + upper).astype(jnp.bfloat16))


def both_halves(
    heads,
    capacity,
    depth_z,
    tokens_hbm,
    moe_gain_hbm,
    routes_hbm,
    group_prob_hbm,
    expert_prob_hbm,
    latent_hbm,
    rope_key_hbm,
    latent_gain_hbm,
    query_hbm,
    key_up_hbm,
    value_up_hbm,
    out_proj_hbm,
    gate_hbm,
    up_hbm,
    down_hbm,
    mixed,
    moe_out,
    tok,
    info,
    away,
    arrived,
    lat_all,
    partial,
    from_pair,
    pair_sum,
    from_far,
    result,
    returned,
    joined,
    answers,
    passing,
    keys,
    values,
    query_big,
    heads_own,
    heads_all,
    tokens,
    moe_gain,
    routes,
    group_prob,
    expert_prob,
    latent,
    rope_key,
    latent_gain,
    query,
    key_up,
    value_up,
    out_proj,
    gate,
    up,
    down,
    load_sem,
    send_sem,
    recv_sem,
):
    row_count, width = tokens.shape
    own_rows, latent_width = latent.shape
    experts = 2 * depth_z
    units = 2 * depth_z
    n_tp = lat_all.shape[2]
    rope_room = lat_all.shape[-1] - latent_width
    bf16 = jnp.bfloat16
    f32 = jnp.float32
    me = lax.axis_index("ep")
    tp = lax.axis_index("tp")
    me_z = me // 2
    me_y = me % 2
    beside = me_z * 2 + 1 - me_y
    inner = (me_z > 0) & (me_z < depth_z - 1)
    inward = jnp.where(me_z < depth_z // 2, me_z + 1, me_z - 1)
    mate = tp + 1 - 2 * (tp % 2)
    far = (tp + 2) % n_tp
    cross = (mate + 2) % n_tp

    barrier = pltpu.get_barrier_semaphore()

    for step in (1, -1):

        @pl.when((me_z + step >= 0) & (me_z + step < depth_z))
        def _(step=step):
            pl.semaphore_signal(
                barrier,
                inc=1,
                device_id={"ep": (me_z + step) * 2 + me_y},
                device_id_type=pl.DeviceIdType.MESH,
            )

    pl.semaphore_signal(
        barrier, inc=1, device_id={"ep": beside}, device_id_type=pl.DeviceIdType.MESH
    )
    for peer in (mate, far, cross):
        pl.semaphore_signal(
            barrier, inc=1, device_id={"tp": peer}, device_id_type=pl.DeviceIdType.MESH
        )

    loads = [
        pltpu.make_async_copy(gate_hbm, gate, load_sem.at[0]),
        pltpu.make_async_copy(up_hbm, up, load_sem.at[1]),
        pltpu.make_async_copy(down_hbm, down, load_sem.at[2]),
        pltpu.make_async_copy(query_hbm, query, load_sem.at[3]),
        pltpu.make_async_copy(key_up_hbm, key_up, load_sem.at[4]),
        pltpu.make_async_copy(value_up_hbm, value_up, load_sem.at[5]),
        pltpu.make_async_copy(out_proj_hbm, out_proj, load_sem.at[6]),
    ]
    small = (
        (routes_hbm, routes),
        (expert_prob_hbm, expert_prob),
        (group_prob_hbm, group_prob),
        (tokens_hbm, tokens),
        (moe_gain_hbm, moe_gain),
        (latent_hbm, latent),
        (rope_key_hbm, rope_key),
        (latent_gain_hbm, latent_gain),
    )
    early = [
        pltpu.make_async_copy(src, dst, load_sem.at[7 + number])
        for number, (src, dst) in enumerate(small)
    ]
    for load in early + loads:
        load.start()

    def remote(src, dst, sent, got, device):
        return pltpu.make_async_remote_copy(
            src_ref=src,
            dst_ref=dst,
            send_sem=send_sem.at[sum(send_kinds(depth_z)[: sent[0]]) + sent[1]],
            recv_sem=recv_sem.at[sum(recv_kinds(depth_z)[: got[0]]) + got[1]],
            device_id=device,
            device_id_type=pl.DeviceIdType.MESH,
        )

    def columns(half):
        return pl.ds(half * (width // 2), width // 2)

    def tok_step(origin, step, half):
        kind = 0 if step > 0 else 1
        target = {"ep": (me_z + step) * 2 + me_y}
        number = origin * 2 + half
        place = tok.at[origin, :, columns(half)]
        copies = [remote(place, place, (kind, number), (0, number), target)]
        if half == 0:
            place = info.at[origin]
            copies.append(remote(place, place, (kind + 2, origin), (2, origin), target))
        return copies

    def spread_tok(origin, step):
        inside = (me_z < depth_z - 1) if step > 0 else (me_z > 0)
        coming = (origin <= me_z) if step > 0 else (origin >= me_z)
        return inside & coming

    def source_of(unit):
        return line_order(me_z, depth_z, unit // 2) * 2 + (me_y + unit) % 2

    def hop_rows(kind, unit, block, peer):
        place = arrived.at[source_of(unit), block]
        return remote(place, place, (kind, 0), (kind, unit), {"tp": peer})

    def far_rows(unit, half, block):
        place = arrived.at[source_of(unit), block, :, columns(half)]
        return remote(place, place, (4, 0), (4, unit * 2 + half), {"tp": far})

    def y_rows(spot, half):
        origin = line_order(me_z, depth_z, spot)
        return remote(
            away.at[origin, :, columns(half)],
            arrived.at[origin * 2 + me_y, tp, :, columns(half)],
            (7, 0),
            (7, spot * 2 + half),
            {"ep": beside},
        )

    def to_mate(kind, unit, block, part):
        source = source_of(unit)
        return remote(
            partial.at[source, block],
            from_pair.at[source, part],
            (kind, 0),
            (kind, unit),
            {"tp": mate},
        )

    def to_far(unit, half):
        source = source_of(unit)
        return remote(
            pair_sum.at[source, :, columns(half)],
            from_far.at[source, :, columns(half)],
            (10, 0),
            (10, unit * 2 + half),
            {"tp": far},
        )

    def send_far(unit):
        for half in range(2):
            to_far(unit, half).start()

    def y_back(spot, half):
        origin = line_order(me_z, depth_z, spot)
        return remote(
            result.at[origin * 2 + 1 - me_y, :, columns(half)],
            returned.at[origin, :, columns(half)],
            (11, 0),
            (11, spot * 2 + half),
            {"ep": beside},
        )

    def z_back(origin, sender, half):
        return remote(
            joined.at[origin, :, columns(half)],
            answers.at[sender, :, columns(half)],
            (12, origin * 2 + half),
            (12, sender * 2 + half),
            {"ep": origin * 2 + me_y},
        )

    def z_pass(half):
        return remote(
            joined.at[line_order(me_z, depth_z, 2), :, columns(half)],
            passing.at[:, columns(half)],
            (18, half),
            (18, half),
            {"ep": inward * 2 + me_y},
        )

    def lat_x(block):
        place = lat_all.at[me_z, me_y, block]
        return remote(place, place, (13, 0), (13, 0), {"tp": far})

    def lat_up(origin):
        copies = []
        for part in range(2):
            place = lat_all.at[origin, :, (tp + 2 * part) % n_tp]
            number = (14, origin * 2 + part)
            copies.append(remote(place, place, number, number, {"ep": (me_z + 1) * 2 + me_y}))
        return copies

    def lat_y(part, side):
        place = lat_all.at[me_z, side, (tp + 2 * part) % n_tp]
        return remote(place, place, (15, part), (15, part), {"ep": beside})

    def lat_mate(part, first):
        place = lat_all.at[:, :, (first + 2 * part) % n_tp]
        return remote(place, place, (16, part), (16, part), {"tp": mate})

    def head_copy(number, peer, slot):
        return remote(
            heads_own.at[peer], heads_all.at[slot], (17, number), (17, number), {"tp": peer}
        )

    for load in early:
        load.wait()
    first_route = routes[0:1, :]
    second_route = routes[1:2, :]
    lane_expert = lax.broadcasted_iota(jnp.int32, (experts, row_count), 0)
    is_first = lane_expert == first_route
    is_second = lane_expert == second_route
    named = jnp.where(is_first | is_second, 1.0, 0.0).astype(bf16)
    ahead = lax.broadcasted_iota(jnp.int32, (row_count, row_count), 0)
    behind = lax.broadcasted_iota(jnp.int32, (row_count, row_count), 1)
    before = jnp.where(ahead < behind, 1.0, 0.0).astype(bf16)
    earlier = jnp.dot(named, before, preferred_element_type=f32)
    first_slot = jnp.sum(jnp.where(is_first, earlier, 0.0), axis=0, keepdims=True)
    second_slot = jnp.sum(jnp.where(is_second, earlier, 0.0), axis=0, keepdims=True)
    both_prob = expert_prob[0:1, :] + expert_prob[1:2, :]
    info[me_z] = jnp.full(info.shape[1:], -1.0, f32)
    info[me_z, 0:1, 0:row_count] = first_route.astype(f32) * capacity + first_slot
    info[me_z, 1:2, 0:row_count] = second_route.astype(f32) * capacity + second_slot
    info[me_z, 2:3, 0:row_count] = group_prob[...] * expert_prob[0:1, :] / both_prob
    info[me_z, 3:4, 0:row_count] = group_prob[...] * expert_prob[1:2, :] / both_prob
    tok[me_z] = rms_scale(tokens[...], moe_gain[...]).astype(bf16)

    pl.semaphore_wait(barrier, jnp.where(inner, 6, 5))

    for step in (1, -1):

        @pl.when(spread_tok(me_z, step))
        def _(step=step):
            for half in range(2):
                for copy in tok_step(me_z, step, half):
                    copy.start()

    def wanted():
        row = lax.broadcasted_iota(jnp.int32, (2 * capacity, info.shape[2]), 0)
        own = me * capacity + row
        other = (beside - 1) * capacity + row
        return jnp.where(row < capacity, own, other).astype(f32)

    def take_tok(spot, half):
        origin = line_order(me_z, depth_z, spot)
        for copy in tok_step(origin, 1, half):
            copy.wait_recv()
        for step in (1, -1):

            @pl.when(spread_tok(origin, step))
            def _(step=step):
                for copy in tok_step(origin, step, half):
                    copy.start()

    def raise_lat(origin):
        @pl.when(spread_tok(origin, 1))
        def _():
            for copy in lat_up(origin):
                copy.start()

    def take_lat(below):
        @pl.when(me_z >= below)
        def _():
            for copy in lat_up(me_z - below):
                copy.wait_recv()
            raise_lat(me_z - below)

    def gather_spot(spot, half):
        origin = line_order(me_z, depth_z, spot)

        @pl.when((spot > 0) & jnp.logical_not(inner))
        def _():
            take_tok(spot, half)

        want = wanted()
        table = jnp.where(
            (want == info[origin, 0:1, :]) | (want == info[origin, 1:2, :]), 1.0, 0.0
        )
        packed = jnp.dot(
            table[:, :row_count].astype(bf16),
            tok[origin, :, columns(half)],
            preferred_element_type=f32,
        ).astype(bf16)
        arrived[origin * 2 + me_y, tp, :, columns(half)] = packed[:capacity]
        away[origin, :, columns(half)] = packed[capacity:]
        y_rows(spot, half).start()
        far_rows(spot * 2, half, tp).start()

    def pass_y(spot, half):
        y_rows(spot, half).wait_recv()
        far_rows(spot * 2 + 1, half, tp).start()

    def share(unit):
        hop_rows(5, unit, tp, mate).start()

    def relay(unit):
        for half in range(2):
            far_rows(unit, half, far).wait_recv()
        hop_rows(6, unit, far, mate).start()

    def compute(unit):
        source = source_of(unit)
        hop_rows(5, unit, mate, mate).wait_recv()
        hop_rows(6, unit, cross, mate).wait_recv()

        @pl.when(unit == 0)
        def _():
            for load in loads[:3]:
                load.wait()

        rows = arrived[source].reshape(n_tp * capacity, width)
        gate_values = jnp.dot(rows, gate[...], preferred_element_type=f32)
        up_values = jnp.dot(rows, up[...], preferred_element_type=f32)
        hidden = (gate_values / (1.0 + jnp.exp(-gate_values)) * up_values).astype(bf16)
        product = jnp.dot(hidden, down[...], preferred_element_type=f32)
        partial[source] = product.astype(bf16).reshape(n_tp, capacity, width)
        to_mate(9, unit, cross, 1).start()
        to_mate(8, unit, mate, 0).start()

    def reduce_pair(unit):
        source = source_of(unit)
        to_mate(9, unit, cross, 1).wait_recv()
        pair_sum[source] = (
            partial[source, far].astype(f32) + from_pair[source, 1].astype(f32)
        ).astype(bf16)

    def reduce_far(unit):
        source = source_of(unit)
        to_mate(8, unit, mate, 0).wait_recv()
        for half in range(2):
            to_far(unit, half).wait_recv()
            result[source, :, columns(half)] = (
                partial[source, tp, :, columns(half)].astype(f32)
                + from_pair[source, 0, :, columns(half)].astype(f32)
                + from_far[source, :, columns(half)].astype(f32)
            ).astype(bf16)
            if unit % 2 == 1:
                y_back(unit // 2, half).start()

    def weighted(spot, half):
        origin = line_order(me_z, depth_z, spot)
        y_back(spot, half).wait_recv()
        want = wanted()
        weights = jnp.where(want == info[origin, 0:1, :], info[origin, 2:3, :], 0.0) + jnp.where(
            want == info[origin, 1:2, :], info[origin, 3:4, :], 0.0
        )
        weights = weights[:, :row_count]
        high = weights.astype(bf16)
        low = (weights - high.astype(f32)).astype(bf16)
        rows = jnp.concatenate(
            [result[origin * 2 + me_y, :, columns(half)], returned[origin, :, columns(half)]],
            axis=0,
        )
        over_slots = (((0,), (0,)), ((), ()))
        return lax.dot_general(
            high, rows, over_slots, preferred_element_type=f32
        ) + lax.dot_general(low, rows, over_slots, preferred_element_type=f32)

    def join(spot):
        origin = line_order(me_z, depth_z, spot)
        for half in range(2):
            joined[origin, :, columns(half)] = weighted(spot, half).astype(bf16)
            z_back(origin, me_z, half).start()

    def join_pass():
        origin = line_order(me_z, depth_z, 2)
        for half in range(2):
            joined[origin, :, columns(half)] = weighted(2, half).astype(bf16)
            z_pass(half).start()

    def join_passed():
        origin = line_order(me_z, depth_z, 1)
        for half in range(2):
            own = weighted(1, half)
            z_pass(half).wait_recv()
            joined[origin, :, columns(half)] = (
                own + passing[:, columns(half)].astype(f32)
            ).astype(bf16)
            z_back(origin, me_z, half).start()

    def own_latent():
        same, swapped = turn_tables(ROPE_DIM, rope_room, 0)
        first_row = (me * n_tp + tp) * own_rows
        cosine, sine = angle_tables(first_row, own_rows, rope_room)
        turned = jnp.dot(rope_key[...], same, preferred_element_type=f32) * cosine + (
            jnp.dot(rope_key[...], swapped, preferred_element_type=f32) * sine
        )
        lat_all[me_z, me_y, tp, :, :latent_width] = rms_scale(
            latent[...], latent_gain[...]
        ).astype(bf16)
        lat_all[me_z, me_y, tp, :, latent_width:] = turned.astype(bf16)
        lat_x(tp).start()

    def spread_query():
        loads[3].wait()
        rows, packed_width = query.shape
        head_width = packed_width // heads
        nope_width = heads * NOPE
        cosine, sine = angle_tables(me * rows, rows, rope_room)
        row = lax.broadcasted_iota(jnp.int32, (packed_width, nope_width), 0)
        lane = lax.broadcasted_iota(jnp.int32, (packed_width, nope_width), 1)
        out_lane = lax.broadcasted_iota(jnp.int32, (rows, nope_width), 1)
        plain = jnp.zeros((packed_width, nope_width), f32)
        for head in range(heads):
            inside = (lane >= head * NOPE) & (lane < (head + 1) * NOPE)
            plain = jnp.where(inside & (row - lane == head * ROPE_DIM), 1.0, plain)
        nope = jnp.dot(query[...], plain.astype(bf16), preferred_element_type=f32)
        for head in range(heads):
            inside = (out_lane >= head * NOPE) & (out_lane < (head + 1) * NOPE)
            query_big[head, :, :nope_width] = jnp.where(inside, nope, 0.0).astype(bf16)
            same, swapped = turn_tables(packed_width, rope_room, head * head_width + NOPE)
            turned = jnp.dot(query[...], same, preferred_element_type=f32) * cosine + (
                jnp.dot(query[...], swapped, preferred_element_type=f32) * sine
            )
            query_big[head, :, nope_width:] = turned.astype(bf16)

    def fill_keys():
        nope_width = key_up.shape[1]
        packed = lat_all[...].reshape(-1, lat_all.shape[-1])
        normed = packed[:, :latent_width]
        loads[4].wait()
        loads[5].wait()
        keys[:, :nope_width] = jnp.dot(normed, key_up[...], preferred_element_type=f32).astype(bf16)
        keys[:, nope_width:] = packed[:, latent_width:]
        values[...] = jnp.dot(normed, value_up[...], preferred_element_type=f32).astype(bf16)

    def attend(first_head, last_head):
        rows = query_big.shape[1]
        seq = keys.shape[0]
        value_width = values.shape[1] // heads
        query_pos = me * rows + lax.broadcasted_iota(jnp.int32, (rows, seq), 0)
        allowed = lax.broadcasted_iota(jnp.int32, (rows, seq), 1) <= query_pos
        lane = lax.broadcasted_iota(jnp.int32, (rows, heads * value_width), 1)
        scale = (NOPE + ROPE_DIM) ** (-0.5)
        gathered = jnp.zeros((rows, heads * value_width), f32)
        if first_head > 0:
            gathered = heads_own[...].reshape(rows, -1).astype(f32)
        for head in range(first_head, last_head):
            scores = (
                lax.dot_general(
                    query_big[head],
                    keys[...],
                    (((1,), (1,)), ((), ())),
                    preferred_element_type=f32,
                )
                * scale
            )
            scores = jnp.where(allowed, scores, masked_value)
            raised = jnp.exp(scores - jnp.max(scores, axis=1, keepdims=True))
            totals = jnp.sum(raised, axis=1, keepdims=True)
            summed = jnp.dot(raised.astype(bf16), values[...], preferred_element_type=f32)
            inside = (lane >= head * value_width) & (lane < (head + 1) * value_width)
            gathered = jnp.where(inside, summed / totals, gathered)
        heads_own[...] = gathered.astype(bf16).reshape(heads_own.shape)

    peers = (mate, far, cross)

    @pl.when(inner)
    def _():
        answers[line_order(me_z, depth_z, 2)] = jnp.zeros(answers.shape[1:], bf16)

    def clear(above, carry):
        @pl.when(me_z + above < depth_z)
        def _():
            lat_all[me_z + above] = jnp.zeros(lat_all.shape[1:], bf16)

        return carry

    def stage(turn, carry):
        spot = turn // 2

        @pl.when(turn == 0)
        def _():
            gather_spot(0, 0)

        @pl.when(turn == 1)
        def _():
            pass_y(0, 1)

        @pl.when((turn == 1) & inner)
        def _():
            take_tok(1, 0)
            take_tok(3, 0)

        @pl.when((turn == 2) & inner)
        def _():
            take_tok(1, 1)
            take_tok(3, 1)

        @pl.when((turn == 3) & inner)
        def _():
            take_tok(2, 0)

        @pl.when((turn == 4) & inner)
        def _():
            take_tok(2, 1)

        @pl.when(turn % 2 == 0)
        def _():
            gather_spot(spot, 1)
            share(turn)

            @pl.when(turn > 0)
            def _():
                pass_y(spot, 0)

        @pl.when(turn % 2 == 1)
        def _():
            gather_spot(spot + 1, 0)

            @pl.when(turn > 1)
            def _():
                pass_y(spot, 1)

            share(turn)

        @pl.when(turn == 0)
        def _():
            own_latent()
            lax.fori_loop(1, depth_z, clear, 0)
            pass_y(0, 0)

        @pl.when(turn == 2)
        def _():
            lat_x(far).wait_recv()
            lat_y(0, me_y).start()
            lat_y(1, me_y).start()

        @pl.when(turn == 4)
        def _():
            lat_y(0, 1 - me_y).wait_recv()
            lat_y(1, 1 - me_y).wait_recv()
            raise_lat(me_z)

        @pl.when(turn >= 4)
        def _():
            reduce_pair(turn - 4)

        @pl.when(turn >= 2)
        def _():
            compute(turn - 2)

        @pl.when(turn >= 1)
        def _():
            relay(turn - 1)

        @pl.when(turn == 2)
        def _():
            spread_query()

        @pl.when(turn == 6)
        def _():
            take_lat(1)

        return carry

    lax.fori_loop(0, units - 1, stage, 0)

    pass_y(depth_z - 1, 1)
    share(7)
    reduce_pair(4)
    compute(5)
    relay(6)
    reduce_pair(3)
    reduce_pair(5)
    send_far(5)
    send_far(4)
    take_lat(2)
    compute(6)
    reduce_pair(6)
    relay(7)
    take_lat(3)
    lat_mate(0, tp).start()
    lat_mate(1, tp).start()
    compute(7)
    send_far(3)
    reduce_far(5)
    reduce_pair(7)
    send_far(7)
    send_far(6)
    lat_mate(0, mate).wait_recv()
    lat_mate(1, mate).wait_recv()
    fill_keys()
    attend(0, heads // 2)
    reduce_far(4)

    @pl.when(inner)
    def _():
        join(2)

    @pl.when(jnp.logical_not(inner))
    def _():
        join_pass()

    attend(heads // 2, heads)
    for number, peer in enumerate(peers):
        head_copy(number, peer, tp).start()
    send_far(2)
    send_far(1)
    send_far(0)
    heads_all[tp] = heads_own[tp]
    reduce_far(3)
    reduce_far(7)
    reduce_far(6)

    join(3)
    reduce_far(2)

    @pl.when(inner)
    def _():
        join_passed()

    @pl.when(jnp.logical_not(inner))
    def _():
        join(1)

    loads[6].wait()
    for number, peer in enumerate(peers):
        head_copy(number, peer, peer).wait_recv()
    depth = heads_all.shape[2]
    total = jnp.zeros(mixed.shape, f32)
    for part in range(n_tp):
        total = total + jnp.dot(
            heads_all[part],
            out_proj[part * depth : (part + 1) * depth, :],
            preferred_element_type=f32,
        )
    mixed[...] = total.astype(mixed.dtype)
    reduce_far(1)
    reduce_far(0)
    chosen = [weighted(0, half) for half in range(2)]

    def finish_line(origin, carry):
        for step in (1, -1):

            @pl.when(spread_tok(origin, step))
            def _(step=step):
                for copy in (*tok_step(origin, step, 0), *tok_step(origin, step, 1)):
                    copy.wait_send()

        @pl.when(spread_tok(origin, 1))
        def _():
            for copy in lat_up(origin):
                copy.wait_send()

        passed = jnp.logical_not(inner) & (origin == line_order(me_z, depth_z, 2))

        @pl.when((origin != me_z) & jnp.logical_not(passed))
        def _():
            for half in range(2):
                z_back(origin, me_z, half).wait_send()

        return carry

    lax.fori_loop(0, depth_z, finish_line, 0)

    @pl.when(jnp.logical_not(inner))
    def _():
        for half in range(2):
            z_pass(half).wait_send()

    lat_x(tp).wait_send()
    for part in range(2):
        lat_y(part, me_y).wait_send()
        lat_mate(part, tp).wait_send()
    for number, peer in enumerate(peers):
        head_copy(number, peer, tp).wait_send()

    def all_sent(kind, src, device):
        remote(src, src, (kind, 0), (4, 0), device).wait_send()

    all_sent(4, arrived.at[:, tp], {"tp": far})
    all_sent(5, arrived.at[:, tp], {"tp": mate})
    all_sent(6, arrived.at[:, far], {"tp": mate})
    all_sent(7, away, {"ep": beside})
    all_sent(8, partial.at[:, mate], {"tp": mate})
    all_sent(9, partial.at[:, cross], {"tp": mate})
    all_sent(10, pair_sum, {"tp": far})
    all_sent(11, returned, {"ep": beside})

    none = line_order(me_z, depth_z, 2)
    for half in range(2):
        total = chosen[half]
        for shift in range(1, depth_z):
            sender = (me_z + shift) % depth_z

            @pl.when(jnp.logical_not(inner & (sender == none)))
            def _(sender=sender, half=half):
                z_back(me_z, sender, half).wait_recv()

            total = total + answers[sender, :, columns(half)].astype(f32)
        moe_out[:, columns(half)] = total.astype(moe_out.dtype)


def hand_over(mixed_in, moe_in, mixed_out, moe_out, sem):
    copies = [
        pltpu.make_async_copy(mixed_in, mixed_out, sem.at[0]),
        pltpu.make_async_copy(moe_in, moe_out, sem.at[1]),
    ]
    for copy in copies:
        copy.start()
    for copy in copies:
        copy.wait()


def fused_body(
    query,
    latent,
    rope_key,
    latent_gain,
    key_up,
    value_up,
    out_proj,
    tokens,
    moe_gain,
    routes,
    group_prob,
    expert_prob,
    w_gate,
    w_up,
    w_down,
):
    n_ep = lax.axis_size("ep")
    n_tp = lax.axis_size("tp")
    depth_z = n_ep // 2
    query_rows = query.shape[0]
    own_rows, latent_width = latent.shape
    heads = query.shape[1] // (NOPE + ROPE_DIM)
    rope_room = padded(ROPE_DIM)
    row_count, width = tokens.shape
    capacity = 2 * routes.shape[1] * row_count // n_ep
    bf16 = jnp.bfloat16
    lat_width = latent_width + rope_room
    key_width = key_up.shape[1] + rope_room
    vmem = pl.BlockSpec(memory_space=pltpu.VMEM)
    anywhere = pl.BlockSpec(memory_space=pl.ANY)
    results = pl.pallas_call(
        functools.partial(both_halves, heads, capacity, depth_z),
        out_shape=(
            pltpu.VMEM((own_rows, out_proj.shape[1]), bf16),
            pltpu.VMEM((row_count, width), bf16),
        ),
        in_specs=[anywhere] * 15,
        out_specs=(vmem, vmem),
        scratch_shapes=[
            pltpu.VMEM((depth_z, row_count, width), bf16),
            pltpu.VMEM((depth_z, 8, padded(row_count)), jnp.float32),
            pltpu.VMEM((depth_z, capacity, width), bf16),
            pltpu.VMEM((n_ep, n_tp, capacity, width), bf16),
            pltpu.VMEM((depth_z, 2, n_tp, own_rows, lat_width), bf16),
            pltpu.VMEM((n_ep, n_tp, capacity, width), bf16),
            pltpu.VMEM((n_ep, 2, capacity, width), bf16),
            pltpu.VMEM((n_ep, capacity, width), bf16),
            pltpu.VMEM((n_ep, capacity, width), bf16),
            pltpu.VMEM((n_ep, capacity, width), bf16),
            pltpu.VMEM((depth_z, capacity, width), bf16),
            pltpu.VMEM((depth_z, row_count, width), bf16),
            pltpu.VMEM((depth_z, row_count, width), bf16),
            pltpu.VMEM((row_count, width), bf16),
            pltpu.VMEM((n_ep * n_tp * own_rows, key_width), bf16),
            pltpu.VMEM((n_ep * n_tp * own_rows, value_up.shape[1]), bf16),
            pltpu.VMEM((heads, query_rows, key_width), bf16),
            pltpu.VMEM((n_tp, own_rows, value_up.shape[1]), bf16),
            pltpu.VMEM((n_tp, own_rows, value_up.shape[1]), bf16),
            pltpu.VMEM(tokens.shape, bf16),
            pltpu.VMEM((1, width), jnp.float32),
            pltpu.VMEM((routes.shape[1], row_count), jnp.int32),
            pltpu.VMEM((1, row_count), jnp.float32),
            pltpu.VMEM((routes.shape[1], row_count), jnp.float32),
            pltpu.VMEM(latent.shape, bf16),
            pltpu.VMEM(rope_key.shape, bf16),
            pltpu.VMEM((1, latent_width), jnp.float32),
            pltpu.VMEM(query.shape, bf16),
            pltpu.VMEM(key_up.shape, bf16),
            pltpu.VMEM(value_up.shape, bf16),
            pltpu.VMEM(out_proj.shape, bf16),
            pltpu.VMEM(w_gate.shape[1:], bf16),
            pltpu.VMEM(w_up.shape[1:], bf16),
            pltpu.VMEM(w_down.shape[1:], bf16),
            pltpu.SemaphoreType.DMA((15,)),
            pltpu.SemaphoreType.DMA((sum(send_kinds(depth_z)),)),
            pltpu.SemaphoreType.DMA((sum(recv_kinds(depth_z)),)),
        ],
        compiler_params=pltpu.CompilerParams(
            collective_id=0, has_side_effects=True, vmem_limit_bytes=60 * 1024 * 1024
        ),
        name="both_halves",
    )(
        tokens,
        moe_gain.reshape(1, -1),
        routes.T,
        group_prob.reshape(1, -1),
        expert_prob.T,
        latent,
        rope_key,
        latent_gain.reshape(1, -1),
        query,
        key_up,
        value_up,
        out_proj,
        w_gate[0],
        w_up[0],
        w_down[0],
    )
    return pl.pallas_call(
        hand_over,
        out_shape=tuple(jax.ShapeDtypeStruct(part.shape, part.dtype) for part in results),
        in_specs=[vmem] * 2,
        out_specs=(anywhere, anywhere),
        scratch_shapes=[pltpu.SemaphoreType.DMA((2,))],
        compiler_params=pltpu.CompilerParams(vmem_limit_bytes=4 * 1024 * 1024),
        name="hand_over",
    )(*results)


def fits_kernel(mesh, *arrays):
    n_ep, n_tp = mesh.shape["ep"], mesh.shape["tp"]
    tokens, routes, latent = arrays[7], arrays[9], arrays[1]
    row_count = tokens.shape[0] // (n_ep * n_tp)
    capacity = 2 * routes.shape[1] * row_count // n_ep
    own_rows = latent.shape[0] // (n_ep * n_tp)
    shaped = n_tp == 4 and n_ep == 8 and routes.shape[1] == 2
    aligned = capacity % 16 == 0 and own_rows % 16 == 0 and row_count % 16 == 0
    return shaped and aligned and latent.shape[0] <= 2048


def mapped(mesh, chosen):
    return jax.shard_map(
        chosen,
        mesh=mesh,
        in_specs=(
            P("ep", "tp"),
            P(("ep", "tp"), None),
            P(("ep", "tp"), None),
            P(),
            P(None, "tp"),
            P(None, "tp"),
            P(),
            P(("ep", "tp"), None),
            P(),
            P(("ep", "tp"), None),
            P(("ep", "tp")),
            P(("ep", "tp"), None),
            P("ep", None, "tp"),
            P("ep", None, "tp"),
            P("ep", "tp", None),
        ),
        out_specs=(P(("ep", "tp"), None), P(("ep", "tp"), None)),
        check_vma=False,
    )


def solution(mesh):
    def whole(*arrays):
        chosen = fused_body if fits_kernel(mesh, *arrays) else body
        return mapped(mesh, chosen)(*arrays)

    return whole
```

```python
import functools
import math

import jax
import jax.numpy as jnp
from jax import lax
from jax.experimental import pallas as pl
from jax.experimental.pallas import tpu as pltpu
from jax.sharding import PartitionSpec as P

NOPE = 64
ROPE_DIM = 32
V_DIM = 64


epsilon = 1e-06
rope_base = 10000.0
masked_value = -1e30


def rms_scale(values, gain):
    widened = values.astype(jnp.float32)
    return widened * lax.rsqrt(jnp.mean(widened * widened, axis=-1, keepdims=True) + epsilon) * gain


def tables(positions, rope_width):
    half_width = rope_width // 2
    inverse = rope_base ** (-2.0 * jnp.arange(half_width, dtype=jnp.float32) / rope_width)
    angles = positions.astype(jnp.float32)[:, None] * inverse[None, :]
    return (jnp.cos(angles), jnp.sin(angles))


def rotate(values, cosine, sine):
    half_width = values.shape[-1] // 2
    lower = values[..., :half_width]
    upper = values[..., half_width:]
    return jnp.concatenate([lower * cosine - upper * sine, lower * sine + upper * cosine], axis=-1)


def keep_state(state_in):
    return state_in


def attend_block(running, query_rot, query_pos, key_part, value_part, rope_part):
    amount = key_part.shape[0]
    span_rows = math.gcd(amount, 1024)
    head_count = query_rot.shape[1]
    scale_factor = query_rot.shape[2] ** (-0.5)
    last_query = query_pos[-1]

    def update(state, block_at):
        row_begin = block_at * span_rows
        keys_here = lax.dynamic_slice_in_dim(key_part, row_begin, span_rows, 0).reshape(
            span_rows, head_count, -1
        )
        values_here = lax.dynamic_slice_in_dim(value_part, row_begin, span_rows, 0).reshape(
            span_rows, head_count, -1
        )
        rope_here = lax.dynamic_slice_in_dim(rope_part, row_begin, span_rows, 0)
        key_pos = row_begin + jnp.arange(span_rows, dtype=jnp.int32)

        def advance(state_in):
            top_old, totals, weighted = state_in
            shared = jnp.broadcast_to(
                rope_here[:, None, :], (span_rows, head_count, rope_here.shape[1])
            )
            full_keys = jnp.concatenate([keys_here, shared], axis=-1)
            scores = (
                jnp.einsum("qhd,khd->hqk", query_rot, full_keys, preferred_element_type=jnp.float32)
                * scale_factor
            )
            allowed = key_pos[None, :] <= query_pos[:, None]
            scores = jnp.where(allowed[None], scores, masked_value)
            top_new = jnp.maximum(top_old, jnp.max(scores, axis=-1))
            raised = jnp.where(allowed[None], jnp.exp(scores - top_new[..., None]), 0.0)
            factor = jnp.exp(top_old - top_new)
            totals = totals * factor + jnp.sum(raised, axis=-1)
            weighted = weighted * factor[..., None] + jnp.einsum(
                "hqk,khd->hqd",
                raised.astype(jnp.bfloat16),
                values_here,
                preferred_element_type=jnp.float32,
            )
            return (top_new, totals, weighted)

        return (lax.cond(key_pos[0] <= last_query, advance, keep_state, state), None)

    running, _ = lax.scan(update, running, jnp.arange(amount // span_rows))
    return running


def mixer_half(query, latent, rope_key, latent_gain, key_up, value_up, out_proj):
    query_rows = query.shape[0]
    own_rows = latent.shape[0]
    query_start = lax.axis_index("ep") * query_rows
    key_start = query_start + lax.axis_index("tp") * own_rows
    head_count = query.shape[1] // (NOPE + ROPE_DIM)
    normed = rms_scale(latent, latent_gain).astype(jnp.bfloat16)
    key_cos, key_sin = tables(key_start + jnp.arange(own_rows, dtype=jnp.int32), ROPE_DIM)
    rotated_key = rotate(rope_key.astype(jnp.float32), key_cos, key_sin).astype(jnp.bfloat16)
    query_pos = query_start + jnp.arange(query_rows, dtype=jnp.int32)
    query_cos, query_sin = tables(query_pos, ROPE_DIM)
    query_heads = query.reshape(query_rows, head_count, NOPE + ROPE_DIM)
    turned = rotate(
        query_heads[..., NOPE:].astype(jnp.float32), query_cos[:, None, :], query_sin[:, None, :]
    ).astype(jnp.bfloat16)
    query_rot = jnp.concatenate([query_heads[..., :NOPE], turned], axis=-1)
    last_query = query_start + query_rows - 1
    initial = (
        jnp.full((head_count, query_rows), masked_value, jnp.float32),
        jnp.zeros((head_count, query_rows), jnp.float32),
        jnp.zeros((head_count, query_rows, V_DIM), jnp.float32),
    )
    shard_rows = (
        lax.all_gather(normed, ("ep", "tp"), axis=0, tiled=True),
        lax.all_gather(rotated_key, ("ep", "tp"), axis=0, tiled=True),
    )

    def compute(state_in):
        key_part = jnp.dot(shard_rows[0], key_up, preferred_element_type=jnp.float32).astype(
            jnp.bfloat16
        )
        value_part = jnp.dot(shard_rows[0], value_up, preferred_element_type=jnp.float32).astype(
            jnp.bfloat16
        )
        return attend_block(state_in, query_rot, query_pos, key_part, value_part, shard_rows[1])

    running = lax.cond(jnp.int32(0) <= last_query, compute, keep_state, initial)
    totals = running[1]
    weighted = running[2]
    attention = (
        (weighted / totals[..., None])
        .transpose(1, 0, 2)
        .reshape(query_rows, head_count * V_DIM)
        .astype(jnp.bfloat16)
    )
    own_attention = lax.all_to_all(attention, "tp", split_axis=0, concat_axis=1, tiled=True)
    return jnp.dot(own_attention, out_proj, preferred_element_type=jnp.float32).astype(jnp.bfloat16)


def expert_half(tokens, moe_gain, routes, group_prob, expert_prob, w_gate, w_up, w_down):
    row_count, model_width = tokens.shape
    top_count = routes.shape[1]
    expert_count = lax.axis_size("ep")
    capacity = 2 * top_count * row_count // expert_count
    normed = rms_scale(tokens, moe_gain).astype(jnp.bfloat16)
    flat_routes = routes.reshape(-1)
    onehot = (flat_routes[:, None] == jnp.arange(expert_count, dtype=jnp.int32)[None, :]).astype(
        jnp.int32
    )
    earlier = jnp.cumsum(onehot, axis=0) - onehot
    slot_index = jnp.sum(earlier * onehot, axis=1)
    target = flat_routes * capacity + slot_index
    owner = target[None, :] == jnp.arange(expert_count * capacity, dtype=jnp.int32)[:, None]
    dispatch_table = jnp.any(
        owner.reshape(expert_count * capacity, row_count, top_count), axis=2
    ).astype(jnp.bfloat16)
    outgoing = jnp.dot(dispatch_table, normed, preferred_element_type=jnp.float32).astype(
        jnp.bfloat16
    )
    outgoing = outgoing.reshape(expert_count, capacity, model_width)
    arrived = lax.all_to_all(outgoing, "ep", split_axis=0, concat_axis=0, tiled=True)
    sources, slots, _ = arrived.shape
    flat_rows = arrived.reshape(sources * slots, model_width)
    shard_rows = lax.all_gather(flat_rows, "tp", axis=0, tiled=True)
    gate_values = jnp.dot(shard_rows, w_gate[0], preferred_element_type=jnp.float32)
    up_values = jnp.dot(shard_rows, w_up[0], preferred_element_type=jnp.float32)
    hidden = (jax.nn.silu(gate_values) * up_values).astype(jnp.bfloat16)

    def lower(offset, amount):
        return jnp.dot(hidden, w_down[0], preferred_element_type=jnp.float32)

    summed = lax.psum_scatter(
        lower(jnp.int32(0), sources * slots * lax.axis_size("tp")).astype(jnp.bfloat16),
        "tp",
        scatter_dimension=0,
        tiled=True,
    )
    result = summed.reshape(sources, slots, model_width)
    returned = lax.all_to_all(result, "ep", split_axis=0, concat_axis=0, tiled=True)
    returned_flat = returned.reshape(expert_count * capacity, model_width)
    picked = returned_flat[target].reshape(row_count, top_count, model_width).astype(jnp.float32)
    shares = group_prob[:, None] * expert_prob / jnp.sum(expert_prob, axis=1, keepdims=True)
    return jnp.sum(shares[:, :, None] * picked, axis=1).astype(jnp.bfloat16)


def body(
    query,
    latent,
    rope_key,
    latent_gain,
    key_up,
    value_up,
    out_proj,
    tokens,
    moe_gain,
    routes,
    group_prob,
    expert_prob,
    w_gate,
    w_up,
    w_down,
):
    mixed = mixer_half(query, latent, rope_key, latent_gain, key_up, value_up, out_proj)
    moe_out = expert_half(tokens, moe_gain, routes, group_prob, expert_prob, w_gate, w_up, w_down)
    return (mixed, moe_out)


def padded(amount):
    return -(-amount // 128) * 128


def send_kinds(depth):
    line = 2 * depth
    return (line, line, depth, depth, 1, 1, 1, 1, 1, 1, 1, 1, line, 1, line, 2, 2, 3, 2)


def recv_kinds(depth):
    line = 2 * depth
    wide = 2 * line
    gather = (wide, line, line, line, line, line, wide)
    return (line, 0, depth, 0, *gather, line, line, 1, line, 2, 2, 3, 2)


def line_order(place, depth, spot):
    mirrored = depth - 1 - place
    from_low = (place + spot) % depth
    from_high = depth - 1 - (mirrored + spot) % depth
    return jnp.where(place < depth // 2, from_low, from_high)


def angle_tables(first_row, rows, lanes):
    half_width = ROPE_DIM // 2
    lane = lax.broadcasted_iota(jnp.int32, (rows, lanes), 1) % half_width
    position = first_row + lax.broadcasted_iota(jnp.int32, (rows, lanes), 0)
    inverse = jnp.exp(lane.astype(jnp.float32) * (-2.0 * math.log(rope_base) / ROPE_DIM))
    angles = position.astype(jnp.float32) * inverse
    return (jnp.cos(angles), jnp.sin(angles))


def turn_tables(rows, lanes, first):
    half_width = ROPE_DIM // 2
    row = lax.broadcasted_iota(jnp.int32, (rows, lanes), 0) - first
    lane = lax.broadcasted_iota(jnp.int32, (rows, lanes), 1)
    same = jnp.where((row == lane) & (lane < ROPE_DIM), 1.0, 0.0)
    lower = jnp.where((row == lane + half_width) & (lane < half_width), -1.0, 0.0)
    upper = jnp.where(
        (row == lane - half_width) & (lane >= half_width) & (lane < ROPE_DIM), 1.0, 0.0
    )
    return (same.astype(jnp.bfloat16), (lower + upper).astype(jnp.bfloat16))


def both_halves(
    heads,
    capacity,
    depth_z,
    tokens_hbm,
    moe_gain_hbm,
    routes_hbm,
    group_prob_hbm,
    expert_prob_hbm,
    latent_hbm,
    rope_key_hbm,
    latent_gain_hbm,
    query_hbm,
    key_up_hbm,
    value_up_hbm,
    out_proj_hbm,
    gate_hbm,
    up_hbm,
    down_hbm,
    mixed,
    moe_out,
    tok,
    info,
    away,
    arrived,
    lat_all,
    partial,
    from_pair,
    pair_sum,
    from_far,
    result,
    returned,
    joined,
    answers,
    passing,
    keys,
    values,
    query_big,
    heads_own,
    heads_all,
    tokens,
    moe_gain,
    routes,
    group_prob,
    expert_prob,
    latent,
    rope_key,
    latent_gain,
    query,
    key_up,
    value_up,
    out_proj,
    gate,
    up,
    down,
    load_sem,
    send_sem,
    recv_sem,
):
    row_count, width = tokens.shape
    own_rows, latent_width = latent.shape
    experts = 2 * depth_z
    units = 2 * depth_z
    n_tp = lat_all.shape[2]
    rope_room = lat_all.shape[-1] - latent_width
    bf16 = jnp.bfloat16
    f32 = jnp.float32
    me = lax.axis_index("ep")
    tp = lax.axis_index("tp")
    me_z = me // 2
    me_y = me % 2
    beside = me_z * 2 + 1 - me_y
    inner = (me_z > 0) & (me_z < depth_z - 1)
    inward = jnp.where(me_z < depth_z // 2, me_z + 1, me_z - 1)
    mate = tp + 1 - 2 * (tp % 2)
    far = (tp + 2) % n_tp
    cross = (mate + 2) % n_tp

    barrier = pltpu.get_barrier_semaphore()

    for step in (1, -1):

        @pl.when((me_z + step >= 0) & (me_z + step < depth_z))
        def _(step=step):
            pl.semaphore_signal(
                barrier,
                inc=1,
                device_id={"ep": (me_z + step) * 2 + me_y},
                device_id_type=pl.DeviceIdType.MESH,
            )

    pl.semaphore_signal(
        barrier, inc=1, device_id={"ep": beside}, device_id_type=pl.DeviceIdType.MESH
    )
    for peer in (mate, far, cross):
        pl.semaphore_signal(
            barrier, inc=1, device_id={"tp": peer}, device_id_type=pl.DeviceIdType.MESH
        )

    loads = [
        pltpu.make_async_copy(gate_hbm, gate, load_sem.at[0]),
        pltpu.make_async_copy(up_hbm, up, load_sem.at[1]),
        pltpu.make_async_copy(down_hbm, down, load_sem.at[2]),
        pltpu.make_async_copy(query_hbm, query, load_sem.at[3]),
        pltpu.make_async_copy(key_up_hbm, key_up, load_sem.at[4]),
        pltpu.make_async_copy(value_up_hbm, value_up, load_sem.at[5]),
        pltpu.make_async_copy(out_proj_hbm, out_proj, load_sem.at[6]),
    ]
    small = (
        (routes_hbm, routes),
        (expert_prob_hbm, expert_prob),
        (group_prob_hbm, group_prob),
        (tokens_hbm, tokens),
        (moe_gain_hbm, moe_gain),
        (latent_hbm, latent),
        (rope_key_hbm, rope_key),
        (latent_gain_hbm, latent_gain),
    )
    early = [
        pltpu.make_async_copy(src, dst, load_sem.at[7 + number])
        for number, (src, dst) in enumerate(small)
    ]
    for load in early + loads:
        load.start()

    def remote(src, dst, sent, got, device):
        return pltpu.make_async_remote_copy(
            src_ref=src,
            dst_ref=dst,
            send_sem=send_sem.at[sum(send_kinds(depth_z)[: sent[0]]) + sent[1]],
            recv_sem=recv_sem.at[sum(recv_kinds(depth_z)[: got[0]]) + got[1]],
            device_id=device,
            device_id_type=pl.DeviceIdType.MESH,
        )

    def columns(half):
        return pl.ds(half * (width // 2), width // 2)

    def tok_step(origin, step, half):
        kind = 0 if step > 0 else 1
        target = {"ep": (me_z + step) * 2 + me_y}
        number = origin * 2 + half
        place = tok.at[origin, :, columns(half)]
        copies = [remote(place, place, (kind, number), (0, number), target)]
        if half == 0:
            place = info.at[origin]
            copies.append(remote(place, place, (kind + 2, origin), (2, origin), target))
        return copies

    def spread_tok(origin, step):
        inside = (me_z < depth_z - 1) if step > 0 else (me_z > 0)
        coming = (origin <= me_z) if step > 0 else (origin >= me_z)
        return inside & coming

    def source_of(unit):
        return line_order(me_z, depth_z, unit // 2) * 2 + (me_y + unit) % 2

    def hop_rows(kind, unit, block, peer):
        place = arrived.at[source_of(unit), block]
        return remote(place, place, (kind, 0), (kind, unit), {"tp": peer})

    def far_rows(unit, half, block):
        place = arrived.at[source_of(unit), block, :, columns(half)]
        return remote(place, place, (4, 0), (4, unit * 2 + half), {"tp": far})

    def y_rows(spot, half):
        origin = line_order(me_z, depth_z, spot)
        return remote(
            away.at[origin, :, columns(half)],
            arrived.at[origin * 2 + me_y, tp, :, columns(half)],
            (7, 0),
            (7, spot * 2 + half),
            {"ep": beside},
        )

    def to_mate(kind, unit, block, part):
        source = source_of(unit)
        return remote(
            partial.at[source, block],
            from_pair.at[source, part],
            (kind, 0),
            (kind, unit),
            {"tp": mate},
        )

    def to_far(unit, half):
        source = source_of(unit)
        return remote(
            pair_sum.at[source, :, columns(half)],
            from_far.at[source, :, columns(half)],
            (10, 0),
            (10, unit * 2 + half),
            {"tp": far},
        )

    def send_far(unit):
        for half in range(2):
            to_far(unit, half).start()

    def y_back(spot, half):
        origin = line_order(me_z, depth_z, spot)
        return remote(
            result.at[origin * 2 + 1 - me_y, :, columns(half)],
            returned.at[origin, :, columns(half)],
            (11, 0),
            (11, spot * 2 + half),
            {"ep": beside},
        )

    def z_back(origin, sender, half):
        return remote(
            joined.at[origin, :, columns(half)],
            answers.at[sender, :, columns(half)],
            (12, origin * 2 + half),
            (12, sender * 2 + half),
            {"ep": origin * 2 + me_y},
        )

    def z_pass(half):
        return remote(
            joined.at[line_order(me_z, depth_z, 2), :, columns(half)],
            passing.at[:, columns(half)],
            (18, half),
            (18, half),
            {"ep": inward * 2 + me_y},
        )

    def lat_x(block):
        place = lat_all.at[me_z, me_y, block]
        return remote(place, place, (13, 0), (13, 0), {"tp": far})

    def lat_up(origin):
        copies = []
        for part in range(2):
            place = lat_all.at[origin, :, (tp + 2 * part) % n_tp]
            number = (14, origin * 2 + part)
            copies.append(remote(place, place, number, number, {"ep": (me_z + 1) * 2 + me_y}))
        return copies

    def lat_y(part, side):
        place = lat_all.at[me_z, side, (tp + 2 * part) % n_tp]
        return remote(place, place, (15, part), (15, part), {"ep": beside})

    def lat_mate(part, first):
        place = lat_all.at[:, :, (first + 2 * part) % n_tp]
        return remote(place, place, (16, part), (16, part), {"tp": mate})

    def head_copy(number, peer, slot):
        return remote(
            heads_own.at[peer], heads_all.at[slot], (17, number), (17, number), {"tp": peer}
        )

    for load in early:
        load.wait()
    first_route = routes[0:1, :]
    second_route = routes[1:2, :]
    lane_expert = lax.broadcasted_iota(jnp.int32, (experts, row_count), 0)
    is_first = lane_expert == first_route
    is_second = lane_expert == second_route
    named = jnp.where(is_first | is_second, 1.0, 0.0).astype(bf16)
    ahead = lax.broadcasted_iota(jnp.int32, (row_count, row_count), 0)
    behind = lax.broadcasted_iota(jnp.int32, (row_count, row_count), 1)
    before = jnp.where(ahead < behind, 1.0, 0.0).astype(bf16)
    earlier = jnp.dot(named, before, preferred_element_type=f32)
    first_slot = jnp.sum(jnp.where(is_first, earlier, 0.0), axis=0, keepdims=True)
    second_slot = jnp.sum(jnp.where(is_second, earlier, 0.0), axis=0, keepdims=True)
    both_prob = expert_prob[0:1, :] + expert_prob[1:2, :]
    info[me_z] = jnp.full(info.shape[1:], -1.0, f32)
    info[me_z, 0:1, 0:row_count] = first_route.astype(f32) * capacity + first_slot
    info[me_z, 1:2, 0:row_count] = second_route.astype(f32) * capacity + second_slot
    info[me_z, 2:3, 0:row_count] = group_prob[...] * expert_prob[0:1, :] / both_prob
    info[me_z, 3:4, 0:row_count] = group_prob[...] * expert_prob[1:2, :] / both_prob
    tok[me_z] = rms_scale(tokens[...], moe_gain[...]).astype(bf16)

    pl.semaphore_wait(barrier, jnp.where(inner, 6, 5))

    for step in (1, -1):

        @pl.when(spread_tok(me_z, step))
        def _(step=step):
            for half in range(2):
                for copy in tok_step(me_z, step, half):
                    copy.start()

    def wanted():
        row = lax.broadcasted_iota(jnp.int32, (2 * capacity, info.shape[2]), 0)
        own = me * capacity + row
        other = (beside - 1) * capacity + row
        return jnp.where(row < capacity, own, other).astype(f32)

    def take_tok(spot, half):
        origin = line_order(me_z, depth_z, spot)
        for copy in tok_step(origin, 1, half):
            copy.wait_recv()
        for step in (1, -1):

            @pl.when(spread_tok(origin, step))
            def _(step=step):
                for copy in tok_step(origin, step, half):
                    copy.start()

    def raise_lat(origin):
        @pl.when(spread_tok(origin, 1))
        def _():
            for copy in lat_up(origin):
                copy.start()

    def take_lat(below):
        @pl.when(me_z >= below)
        def _():
            for copy in lat_up(me_z - below):
                copy.wait_recv()
            raise_lat(me_z - below)

    def gather_spot(spot, half):
        origin = line_order(me_z, depth_z, spot)

        @pl.when((spot > 0) & jnp.logical_not(inner))
        def _():
            take_tok(spot, half)

        want = wanted()
        table = jnp.where(
            (want == info[origin, 0:1, :]) | (want == info[origin, 1:2, :]), 1.0, 0.0
        )
        packed = jnp.dot(
            table[:, :row_count].astype(bf16),
            tok[origin, :, columns(half)],
            preferred_element_type=f32,
        ).astype(bf16)
        arrived[origin * 2 + me_y, tp, :, columns(half)] = packed[:capacity]
        away[origin, :, columns(half)] = packed[capacity:]
        y_rows(spot, half).start()
        far_rows(spot * 2, half, tp).start()

    def pass_y(spot, half):
        y_rows(spot, half).wait_recv()
        far_rows(spot * 2 + 1, half, tp).start()

    def share(unit):
        hop_rows(5, unit, tp, mate).start()

    def relay(unit):
        for half in range(2):
            far_rows(unit, half, far).wait_recv()
        hop_rows(6, unit, far, mate).start()

    def compute(unit):
        source = source_of(unit)
        hop_rows(5, unit, mate, mate).wait_recv()
        hop_rows(6, unit, cross, mate).wait_recv()

        @pl.when(unit == 0)
        def _():
            for load in loads[:3]:
                load.wait()

        rows = arrived[source].reshape(n_tp * capacity, width)
        gate_values = jnp.dot(rows, gate[...], preferred_element_type=f32)
        up_values = jnp.dot(rows, up[...], preferred_element_type=f32)
        hidden = (gate_values / (1.0 + jnp.exp(-gate_values)) * up_values).astype(bf16)
        product = jnp.dot(hidden, down[...], preferred_element_type=f32)
        partial[source] = product.astype(bf16).reshape(n_tp, capacity, width)
        to_mate(9, unit, cross, 1).start()
        to_mate(8, unit, mate, 0).start()

    def reduce_pair(unit):
        source = source_of(unit)
        to_mate(9, unit, cross, 1).wait_recv()
        pair_sum[source] = (
            partial[source, far].astype(f32) + from_pair[source, 1].astype(f32)
        ).astype(bf16)

    def reduce_far(unit):
        source = source_of(unit)
        to_mate(8, unit, mate, 0).wait_recv()
        for half in range(2):
            to_far(unit, half).wait_recv()
            result[source, :, columns(half)] = (
                partial[source, tp, :, columns(half)].astype(f32)
                + from_pair[source, 0, :, columns(half)].astype(f32)
                + from_far[source, :, columns(half)].astype(f32)
            ).astype(bf16)
            if unit % 2 == 1:
                y_back(unit // 2, half).start()

    def weighted(spot, half):
        origin = line_order(me_z, depth_z, spot)
        y_back(spot, half).wait_recv()
        want = wanted()
        weights = jnp.where(want == info[origin, 0:1, :], info[origin, 2:3, :], 0.0) + jnp.where(
            want == info[origin, 1:2, :], info[origin, 3:4, :], 0.0
        )
        weights = weights[:, :row_count]
        high = weights.astype(bf16)
        low = (weights - high.astype(f32)).astype(bf16)
        rows = jnp.concatenate(
            [result[origin * 2 + me_y, :, columns(half)], returned[origin, :, columns(half)]],
            axis=0,
        )
        over_slots = (((0,), (0,)), ((), ()))
        return lax.dot_general(
            high, rows, over_slots, preferred_element_type=f32
        ) + lax.dot_general(low, rows, over_slots, preferred_element_type=f32)

    def join(spot):
        origin = line_order(me_z, depth_z, spot)
        for half in range(2):
            joined[origin, :, columns(half)] = weighted(spot, half).astype(bf16)
            z_back(origin, me_z, half).start()

    def join_pass():
        origin = line_order(me_z, depth_z, 2)
        for half in range(2):
            joined[origin, :, columns(half)] = weighted(2, half).astype(bf16)
            z_pass(half).start()

    def join_passed():
        origin = line_order(me_z, depth_z, 1)
        for half in range(2):
            own = weighted(1, half)
            z_pass(half).wait_recv()
            joined[origin, :, columns(half)] = (
                own + passing[:, columns(half)].astype(f32)
            ).astype(bf16)
            z_back(origin, me_z, half).start()

    def own_latent():
        same, swapped = turn_tables(ROPE_DIM, rope_room, 0)
        first_row = (me * n_tp + tp) * own_rows
        cosine, sine = angle_tables(first_row, own_rows, rope_room)
        turned = jnp.dot(rope_key[...], same, preferred_element_type=f32) * cosine + (
            jnp.dot(rope_key[...], swapped, preferred_element_type=f32) * sine
        )
        lat_all[me_z, me_y, tp, :, :latent_width] = rms_scale(
            latent[...], latent_gain[...]
        ).astype(bf16)
        lat_all[me_z, me_y, tp, :, latent_width:] = turned.astype(bf16)
        lat_x(tp).start()

    def spread_query():
        loads[3].wait()
        rows, packed_width = query.shape
        head_width = packed_width // heads
        nope_width = heads * NOPE
        cosine, sine = angle_tables(me * rows, rows, rope_room)
        row = lax.broadcasted_iota(jnp.int32, (packed_width, nope_width), 0)
        lane = lax.broadcasted_iota(jnp.int32, (packed_width, nope_width), 1)
        out_lane = lax.broadcasted_iota(jnp.int32, (rows, nope_width), 1)
        plain = jnp.zeros((packed_width, nope_width), f32)
        for head in range(heads):
            inside = (lane >= head * NOPE) & (lane < (head + 1) * NOPE)
            plain = jnp.where(inside & (row - lane == head * ROPE_DIM), 1.0, plain)
        nope = jnp.dot(query[...], plain.astype(bf16), preferred_element_type=f32)
        for head in range(heads):
            inside = (out_lane >= head * NOPE) & (out_lane < (head + 1) * NOPE)
            query_big[head, :, :nope_width] = jnp.where(inside, nope, 0.0).astype(bf16)
            same, swapped = turn_tables(packed_width, rope_room, head * head_width + NOPE)
            turned = jnp.dot(query[...], same, preferred_element_type=f32) * cosine + (
                jnp.dot(query[...], swapped, preferred_element_type=f32) * sine
            )
            query_big[head, :, nope_width:] = turned.astype(bf16)

    def fill_keys():
        nope_width = key_up.shape[1]
        packed = lat_all[...].reshape(-1, lat_all.shape[-1])
        normed = packed[:, :latent_width]
        loads[4].wait()
        loads[5].wait()
        keys[:, :nope_width] = jnp.dot(normed, key_up[...], preferred_element_type=f32).astype(bf16)
        keys[:, nope_width:] = packed[:, latent_width:]
        values[...] = jnp.dot(normed, value_up[...], preferred_element_type=f32).astype(bf16)

    def attend(first_head, last_head):
        rows = query_big.shape[1]
        seq = keys.shape[0]
        value_width = values.shape[1] // heads
        query_pos = me * rows + lax.broadcasted_iota(jnp.int32, (rows, seq), 0)
        allowed = lax.broadcasted_iota(jnp.int32, (rows, seq), 1) <= query_pos
        lane = lax.broadcasted_iota(jnp.int32, (rows, heads * value_width), 1)
        scale = (NOPE + ROPE_DIM) ** (-0.5)
        gathered = jnp.zeros((rows, heads * value_width), f32)
        if first_head > 0:
            gathered = heads_own[...].reshape(rows, -1).astype(f32)
        for head in range(first_head, last_head):
            scores = (
                lax.dot_general(
                    query_big[head],
                    keys[...],
                    (((1,), (1,)), ((), ())),
                    preferred_element_type=f32,
                )
                * scale
            )
            scores = jnp.where(allowed, scores, masked_value)
            raised = jnp.exp(scores - jnp.max(scores, axis=1, keepdims=True))
            totals = jnp.sum(raised, axis=1, keepdims=True)
            summed = jnp.dot(raised.astype(bf16), values[...], preferred_element_type=f32)
            inside = (lane >= head * value_width) & (lane < (head + 1) * value_width)
            gathered = jnp.where(inside, summed / totals, gathered)
        heads_own[...] = gathered.astype(bf16).reshape(heads_own.shape)

    peers = (mate, far, cross)

    @pl.when(inner)
    def _():
        answers[line_order(me_z, depth_z, 2)] = jnp.zeros(answers.shape[1:], bf16)

    def clear(above, carry):
        @pl.when(me_z + above < depth_z)
        def _():
            lat_all[me_z + above] = jnp.zeros(lat_all.shape[1:], bf16)

        return carry

    def stage(turn, carry):
        spot = turn // 2

        @pl.when(turn == 0)
        def _():
            gather_spot(0, 0)

        @pl.when(turn == 1)
        def _():
            pass_y(0, 1)

        @pl.when((turn == 1) & inner)
        def _():
            take_tok(1, 0)
            take_tok(3, 0)

        @pl.when((turn == 2) & inner)
        def _():
            take_tok(1, 1)
            take_tok(3, 1)

        @pl.when((turn == 3) & inner)
        def _():
            take_tok(2, 0)

        @pl.when((turn == 4) & inner)
        def _():
            take_tok(2, 1)

        @pl.when(turn % 2 == 0)
        def _():
            gather_spot(spot, 1)
            share(turn)

            @pl.when(turn > 0)
            def _():
                pass_y(spot, 0)

        @pl.when(turn % 2 == 1)
        def _():
            gather_spot(spot + 1, 0)

            @pl.when(turn > 1)
            def _():
                pass_y(spot, 1)

            share(turn)

        @pl.when(turn == 0)
        def _():
            own_latent()
            lax.fori_loop(1, depth_z, clear, 0)
            pass_y(0, 0)

        @pl.when(turn == 2)
        def _():
            lat_x(far).wait_recv()
            lat_y(0, me_y).start()
            lat_y(1, me_y).start()

        @pl.when(turn == 4)
        def _():
            lat_y(0, 1 - me_y).wait_recv()
            lat_y(1, 1 - me_y).wait_recv()
            raise_lat(me_z)

        @pl.when(turn >= 4)
        def _():
            reduce_pair(turn - 4)

        @pl.when(turn >= 2)
        def _():
            compute(turn - 2)

        @pl.when(turn >= 1)
        def _():
            relay(turn - 1)

        @pl.when(turn == 2)
        def _():
            spread_query()

        @pl.when(turn == 6)
        def _():
            take_lat(1)

        return carry

    lax.fori_loop(0, units - 1, stage, 0)

    pass_y(depth_z - 1, 1)
    share(7)
    reduce_pair(4)
    compute(5)
    relay(6)
    reduce_pair(3)
    reduce_pair(5)
    send_far(5)
    send_far(4)
    take_lat(2)
    compute(6)
    reduce_pair(6)
    relay(7)
    take_lat(3)
    lat_mate(0, tp).start()
    lat_mate(1, tp).start()
    compute(7)
    send_far(3)
    reduce_far(5)
    reduce_pair(7)
    send_far(7)
    send_far(6)
    send_far(2)
    lat_mate(0, mate).wait_recv()
    lat_mate(1, mate).wait_recv()
    fill_keys()
    attend(0, heads // 2)
    reduce_far(4)

    @pl.when(inner)
    def _():
        join(2)

    @pl.when(jnp.logical_not(inner))
    def _():
        join_pass()

    attend(heads // 2, heads)
    for number, peer in enumerate(peers):
        head_copy(number, peer, tp).start()
    send_far(1)
    send_far(0)
    heads_all[tp] = heads_own[tp]
    reduce_far(3)
    reduce_far(7)
    reduce_far(6)

    join(3)
    reduce_far(2)

    @pl.when(inner)
    def _():
        join_passed()

    @pl.when(jnp.logical_not(inner))
    def _():
        join(1)

    loads[6].wait()
    for number, peer in enumerate(peers):
        head_copy(number, peer, peer).wait_recv()
    depth = heads_all.shape[2]
    total = jnp.zeros(mixed.shape, f32)
    for part in range(n_tp):
        total = total + jnp.dot(
            heads_all[part],
            out_proj[part * depth : (part + 1) * depth, :],
            preferred_element_type=f32,
        )
    mixed[...] = total.astype(mixed.dtype)
    reduce_far(1)
    reduce_far(0)
    chosen = [weighted(0, half) for half in range(2)]

    def finish_line(origin, carry):
        for step in (1, -1):

            @pl.when(spread_tok(origin, step))
            def _(step=step):
                for copy in (*tok_step(origin, step, 0), *tok_step(origin, step, 1)):
                    copy.wait_send()

        @pl.when(spread_tok(origin, 1))
        def _():
            for copy in lat_up(origin):
                copy.wait_send()

        passed = jnp.logical_not(inner) & (origin == line_order(me_z, depth_z, 2))

        @pl.when((origin != me_z) & jnp.logical_not(passed))
        def _():
            for half in range(2):
                z_back(origin, me_z, half).wait_send()

        return carry

    lax.fori_loop(0, depth_z, finish_line, 0)

    @pl.when(jnp.logical_not(inner))
    def _():
        for half in range(2):
            z_pass(half).wait_send()

    lat_x(tp).wait_send()
    for part in range(2):
        lat_y(part, me_y).wait_send()
        lat_mate(part, tp).wait_send()
    for number, peer in enumerate(peers):
        head_copy(number, peer, tp).wait_send()

    def all_sent(kind, src, device):
        remote(src, src, (kind, 0), (4, 0), device).wait_send()

    all_sent(4, arrived.at[:, tp], {"tp": far})
    all_sent(5, arrived.at[:, tp], {"tp": mate})
    all_sent(6, arrived.at[:, far], {"tp": mate})
    all_sent(7, away, {"ep": beside})
    all_sent(8, partial.at[:, mate], {"tp": mate})
    all_sent(9, partial.at[:, cross], {"tp": mate})
    all_sent(10, pair_sum, {"tp": far})
    all_sent(11, returned, {"ep": beside})

    none = line_order(me_z, depth_z, 2)
    for half in range(2):
        total = chosen[half]
        for shift in range(1, depth_z):
            sender = (me_z + shift) % depth_z

            @pl.when(jnp.logical_not(inner & (sender == none)))
            def _(sender=sender, half=half):
                z_back(me_z, sender, half).wait_recv()

            total = total + answers[sender, :, columns(half)].astype(f32)
        moe_out[:, columns(half)] = total.astype(moe_out.dtype)


def hand_over(mixed_in, moe_in, mixed_out, moe_out, sem):
    copies = [
        pltpu.make_async_copy(mixed_in, mixed_out, sem.at[0]),
        pltpu.make_async_copy(moe_in, moe_out, sem.at[1]),
    ]
    for copy in copies:
        copy.start()
    for copy in copies:
        copy.wait()


def fused_body(
    query,
    latent,
    rope_key,
    latent_gain,
    key_up,
    value_up,
    out_proj,
    tokens,
    moe_gain,
    routes,
    group_prob,
    expert_prob,
    w_gate,
    w_up,
    w_down,
):
    n_ep = lax.axis_size("ep")
    n_tp = lax.axis_size("tp")
    depth_z = n_ep // 2
    query_rows = query.shape[0]
    own_rows, latent_width = latent.shape
    heads = query.shape[1] // (NOPE + ROPE_DIM)
    rope_room = padded(ROPE_DIM)
    row_count, width = tokens.shape
    capacity = 2 * routes.shape[1] * row_count // n_ep
    bf16 = jnp.bfloat16
    lat_width = latent_width + rope_room
    key_width = key_up.shape[1] + rope_room
    vmem = pl.BlockSpec(memory_space=pltpu.VMEM)
    anywhere = pl.BlockSpec(memory_space=pl.ANY)
    results = pl.pallas_call(
        functools.partial(both_halves, heads, capacity, depth_z),
        out_shape=(
            pltpu.VMEM((own_rows, out_proj.shape[1]), bf16),
            pltpu.VMEM((row_count, width), bf16),
        ),
        in_specs=[anywhere] * 15,
        out_specs=(vmem, vmem),
        scratch_shapes=[
            pltpu.VMEM((depth_z, row_count, width), bf16),
            pltpu.VMEM((depth_z, 8, padded(row_count)), jnp.float32),
            pltpu.VMEM((depth_z, capacity, width), bf16),
            pltpu.VMEM((n_ep, n_tp, capacity, width), bf16),
            pltpu.VMEM((depth_z, 2, n_tp, own_rows, lat_width), bf16),
            pltpu.VMEM((n_ep, n_tp, capacity, width), bf16),
            pltpu.VMEM((n_ep, 2, capacity, width), bf16),
            pltpu.VMEM((n_ep, capacity, width), bf16),
            pltpu.VMEM((n_ep, capacity, width), bf16),
            pltpu.VMEM((n_ep, capacity, width), bf16),
            pltpu.VMEM((depth_z, capacity, width), bf16),
            pltpu.VMEM((depth_z, row_count, width), bf16),
            pltpu.VMEM((depth_z, row_count, width), bf16),
            pltpu.VMEM((row_count, width), bf16),
            pltpu.VMEM((n_ep * n_tp * own_rows, key_width), bf16),
            pltpu.VMEM((n_ep * n_tp * own_rows, value_up.shape[1]), bf16),
            pltpu.VMEM((heads, query_rows, key_width), bf16),
            pltpu.VMEM((n_tp, own_rows, value_up.shape[1]), bf16),
            pltpu.VMEM((n_tp, own_rows, value_up.shape[1]), bf16),
            pltpu.VMEM(tokens.shape, bf16),
            pltpu.VMEM((1, width), jnp.float32),
            pltpu.VMEM((routes.shape[1], row_count), jnp.int32),
            pltpu.VMEM((1, row_count), jnp.float32),
            pltpu.VMEM((routes.shape[1], row_count), jnp.float32),
            pltpu.VMEM(latent.shape, bf16),
            pltpu.VMEM(rope_key.shape, bf16),
            pltpu.VMEM((1, latent_width), jnp.float32),
            pltpu.VMEM(query.shape, bf16),
            pltpu.VMEM(key_up.shape, bf16),
            pltpu.VMEM(value_up.shape, bf16),
            pltpu.VMEM(out_proj.shape, bf16),
            pltpu.VMEM(w_gate.shape[1:], bf16),
            pltpu.VMEM(w_up.shape[1:], bf16),
            pltpu.VMEM(w_down.shape[1:], bf16),
            pltpu.SemaphoreType.DMA((15,)),
            pltpu.SemaphoreType.DMA((sum(send_kinds(depth_z)),)),
            pltpu.SemaphoreType.DMA((sum(recv_kinds(depth_z)),)),
        ],
        compiler_params=pltpu.CompilerParams(
            collective_id=0, has_side_effects=True, vmem_limit_bytes=60 * 1024 * 1024
        ),
        name="both_halves",
    )(
        tokens,
        moe_gain.reshape(1, -1),
        routes.T,
        group_prob.reshape(1, -1),
        expert_prob.T,
        latent,
        rope_key,
        latent_gain.reshape(1, -1),
        query,
        key_up,
        value_up,
        out_proj,
        w_gate[0],
        w_up[0],
        w_down[0],
    )
    return pl.pallas_call(
        hand_over,
        out_shape=tuple(jax.ShapeDtypeStruct(part.shape, part.dtype) for part in results),
        in_specs=[vmem] * 2,
        out_specs=(anywhere, anywhere),
        scratch_shapes=[pltpu.SemaphoreType.DMA((2,))],
        compiler_params=pltpu.CompilerParams(vmem_limit_bytes=4 * 1024 * 1024),
        name="hand_over",
    )(*results)


def fits_kernel(mesh, *arrays):
    n_ep, n_tp = mesh.shape["ep"], mesh.shape["tp"]
    tokens, routes, latent = arrays[7], arrays[9], arrays[1]
    row_count = tokens.shape[0] // (n_ep * n_tp)
    capacity = 2 * routes.shape[1] * row_count // n_ep
    own_rows = latent.shape[0] // (n_ep * n_tp)
    shaped = n_tp == 4 and n_ep == 8 and routes.shape[1] == 2
    aligned = capacity % 16 == 0 and own_rows % 16 == 0 and row_count % 16 == 0
    return shaped and aligned and latent.shape[0] <= 2048


def mapped(mesh, chosen):
    return jax.shard_map(
        chosen,
        mesh=mesh,
        in_specs=(
            P("ep", "tp"),
            P(("ep", "tp"), None),
            P(("ep", "tp"), None),
            P(),
            P(None, "tp"),
            P(None, "tp"),
            P(),
            P(("ep", "tp"), None),
            P(),
            P(("ep", "tp"), None),
            P(("ep", "tp")),
            P(("ep", "tp"), None),
            P("ep", None, "tp"),
            P("ep", None, "tp"),
            P("ep", "tp", None),
        ),
        out_specs=(P(("ep", "tp"), None), P(("ep", "tp"), None)),
        check_vma=False,
    )


def solution(mesh):
    def whole(*arrays):
        chosen = fused_body if fits_kernel(mesh, *arrays) else body
        return mapped(mesh, chosen)(*arrays)

    return whole
```
